32 devices in a mesh: sp: 8 (over z, y), tp: 4 (over x, core).
Axes of the slice: x: 2, y: 2, z: 4, core: 2. Of those that a mesh axis runs over, the one named last changes fastest.
Arguments:
- activity: bfloat16 [2048, 4096], P('sp', 'tp'), may hold values from -8 to 8
- query_weight: bfloat16 [4096, 3072], P('sp', 'tp'), may hold values from -0.09375 to 0.09375
- key_weight: bfloat16 [4096, 3072], P('sp', 'tp'), may hold values from -0.09375 to 0.09375
- value_weight: bfloat16 [4096, 3072], P('sp', 'tp'), may hold values from -0.09375 to 0.09375
- merge_weight: bfloat16 [1024, 4096], P('tp', 'sp'), may hold values from -1.5 to 1.5
Outputs:
- attended: bfloat16 [2048, 4096], P(('sp', 'tp'))
The draws below stay inside these ranges and needn't reach their ends.
All inputs are finite; a program needn't handle non-finite values.
Results may differ from the reference program's by a relative error of at most 0.013.
Values may be sent and summed in bfloat16 or wider, within the bound.
A program may use at most 128 MiB of HBM per device.

```python
import jax
import jax.numpy as jnp
from jax import lax

D = 4096
HPG = 16
HEAD = 64
HEAD_GROUPS = 3
SPAN = 128
DILATION_MIDDLE = 4
DILATION_WIDEST = 8
TOK_DEV = 256
TOKENS = 2048


def draw_activity(key, part):
    key_base, key_sign = jax.random.split(key, 2)
    drawn = jnp.clip(jax.random.normal(key_base, (TOKENS, D), jnp.float32), -6.0, 6.0)
    return drawn.astype(jnp.bfloat16)


def paired_weights(key):
    key_query = jax.random.fold_in(key, 11)
    key_other = jax.random.fold_in(key, 23)
    col_total = HEAD_GROUPS * HPG * HEAD
    weight_scale = D ** (-0.5)
    query_draw = jnp.clip(jax.random.normal(key_query, (D, col_total), jnp.float32), -6.0, 6.0) * weight_scale
    key_draw = jnp.clip(jax.random.normal(key_other, (D, col_total), jnp.float32), -6.0, 6.0) * weight_scale
    return (query_draw, key_draw)


def draw_query_weight(key, part):
    return paired_weights(key)[0].astype(jnp.bfloat16)


def draw_key_weight(key, part):
    return paired_weights(key)[1].astype(jnp.bfloat16)


def shard_levels(stream_key, extent, cuts, smallest, largest):
    def one(position, parts):
        heights = jax.random.uniform(jax.random.fold_in(jax.random.fold_in(stream_key, 6), position), (parts,), jnp.float32, smallest / len(cuts), largest / len(cuts))
        return jnp.repeat(jnp.exp(heights), extent[position] // parts).reshape((-1,) + (1,) * (len(extent) - position - 1))

    gain = one(*cuts[0])
    for cut in cuts[1:]:
        gain = gain * one(*cut)
    return gain


def noise(key, shape, width, reach, pieces=(), kind=jnp.bfloat16):
    values = jax.random.normal(key, shape, jnp.float32) * width
    if len(pieces) > 0:
        values = shard_levels(key, shape, pieces, -0.22, 0.18) * values
    return jnp.clip(values, min=-reach, max=reach).astype(kind)


def setup_inputs(seed: int = 0) -> dict:
    splits = jax.random.split(jax.random.key(seed), 6)
    activity = draw_activity(jax.random.fold_in(splits[5], 71), 0)
    query_weight = draw_query_weight(jax.random.fold_in(splits[5], 71), 0)
    key_weight = draw_key_weight(jax.random.fold_in(splits[5], 71), 0)
    value_weight = noise(splits[3], (D, HEAD_GROUPS * HPG * HEAD), D ** -0.5, 0.09375, ((0, 8), (1, 4)))
    merge_weight = noise(splits[4], (HPG * HEAD, D), (HEAD // 4) ** -0.5, 1.5, ((0, 4), (1, 8)))
    return dict(activity=activity, query_weight=query_weight, key_weight=key_weight, value_weight=value_weight, merge_weight=merge_weight)


rope_base = 500000.0


def rotate(channels, angle_pos):
    half_width = channels.shape[-1] // 2
    frequency = rope_base ** (-jnp.arange(0, half_width, dtype=jnp.float32) * 2.0 / channels.shape[-1])
    angles = angle_pos[:, None] * frequency[None, :]
    cosine = jnp.cos(angles)[:, None, None, :]
    sine_part = jnp.sin(angles)[:, None, None, :]
    first_half = channels[..., :half_width]
    second_half = channels[..., half_width:]
    return jnp.concatenate([first_half * cosine - second_half * sine_part, second_half * cosine + first_half * sine_part], axis=-1)


def window_mix(queries, key_rows, value_entries, query_pos, key_pos, dilation, reach_rows):
    scores = jnp.einsum('ahc,rhc->har', queries.astype(jnp.float32), key_rows.astype(jnp.float32)) * (queries.shape[-1] ** -0.5)
    distance = query_pos[:, None] - key_pos[None, :]
    allowed = (distance >= 0) & (distance <= reach_rows) & (distance % dilation == 0) & (key_pos[None, :] >= 0)
    scores = jnp.where(allowed[None], scores, -jnp.inf)
    row_max = jnp.max(scores, axis=-1, keepdims=True)
    expo = jnp.where(allowed[None], jnp.exp(scores - row_max), 0.0)
    denominator = jnp.sum(expo, axis=-1)
    rounded = lax.optimization_barrier(expo.astype(jnp.bfloat16)).astype(jnp.float32)
    mixed = jnp.einsum('har,rhc->ahc', rounded, value_entries.astype(jnp.float32))
    mixed = mixed / jnp.transpose(denominator)[:, :, None]
    log_total = jnp.transpose(row_max[..., 0] + jnp.log(denominator))
    return mixed, log_total


def reference(activity, query_weight, key_weight, value_weight, merge_weight):
    tok_total = activity.shape[0]
    local_heads = query_weight.shape[1] // (HEAD_GROUPS * HEAD)
    angle_pos = jnp.arange(tok_total, dtype=jnp.int32).astype(jnp.float32)

    def project(weight):
        return jnp.dot(activity, weight, preferred_element_type=jnp.float32).reshape(tok_total, local_heads, HEAD_GROUPS, HEAD)

    query_all = lax.optimization_barrier(rotate(project(query_weight), angle_pos).astype(jnp.bfloat16))
    key_all = lax.optimization_barrier(rotate(project(key_weight), angle_pos).astype(jnp.bfloat16))
    value_all = lax.optimization_barrier(project(value_weight).astype(jnp.bfloat16))
    group_dilations = (1, DILATION_MIDDLE, DILATION_WIDEST)
    query_groups = []
    padded = []
    for grp_index in range(HEAD_GROUPS):
        reach_rows = SPAN * group_dilations[grp_index]
        query_groups.append(query_all[:, :, grp_index])
        padded.append((jnp.pad(key_all[:, :, grp_index], ((reach_rows, 0), (0, 0), (0, 0))),
                       jnp.pad(value_all[:, :, grp_index], ((reach_rows, 0), (0, 0), (0, 0)))))

    def one_block(block_index):
        start_row = block_index * TOK_DEV
        query_pos = start_row + jnp.arange(TOK_DEV, dtype=jnp.int32)
        mixed_list = []
        total_list = []
        for grp_index in range(HEAD_GROUPS):
            dilation = group_dilations[grp_index]
            reach_rows = SPAN * dilation
            query_blk = lax.dynamic_slice_in_dim(query_groups[grp_index], start_row, TOK_DEV, 0)
            key_blk = lax.dynamic_slice_in_dim(padded[grp_index][0], start_row, reach_rows + TOK_DEV, 0)
            value_blk = lax.dynamic_slice_in_dim(padded[grp_index][1], start_row, reach_rows + TOK_DEV, 0)
            key_pos = start_row - reach_rows + jnp.arange(reach_rows + TOK_DEV, dtype=jnp.int32)
            mixed, log_total = window_mix(query_blk, key_blk, value_blk, query_pos, key_pos, dilation, reach_rows)
            mixed_list.append(mixed)
            total_list.append(log_total)
        total_stack = jnp.stack(total_list)
        peak_total = jnp.max(total_stack, axis=0)
        shifted = jnp.exp(total_stack - peak_total)
        group_weight = shifted / jnp.sum(shifted, axis=0)
        merged = jnp.sum(group_weight[..., None] * jnp.stack(mixed_list), axis=0)
        return merged.astype(jnp.bfloat16).reshape(TOK_DEV, local_heads * HEAD)

    merged_all = lax.map(one_block, jnp.arange(tok_total // TOK_DEV, dtype=jnp.int32))
    merged_all = merged_all.reshape(tok_total, local_heads * HEAD)
    return jnp.dot(merged_all, merge_weight, preferred_element_type=jnp.float32).astype(jnp.bfloat16)
```

```python
import functools
import math

import jax
import jax.numpy as jnp
from jax import lax
from jax.experimental import pallas as pl
from jax.experimental.pallas import tpu as pltpu
from jax.sharding import PartitionSpec as P

HEAD = 64
HEAD_GROUPS = 3
SPAN = 128
DILATIONS = (1, 4, 8)
MESH = pl.DeviceIdType.MESH

rope_base = 500000.0


def project_kernel(
    G, R, act, wq, wk, wv, cos_ref, sin_ref, out,
    a_buf, w_buf, c_buf, r_buf, q_buf, kv_buf, o_buf, m_buf,
    local_sem, swap_send, swap_recv, fan_send, fan_recv,
    w_send, w_recv, c_send, c_recv, kv_send, kv_recv, m_send, m_recv,
):
    s = lax.axis_index("sp")
    t = lax.axis_index("tp")
    g = lax.div(s, R)
    r = lax.rem(s, R)
    tok = act.shape[0]
    krows = wq.shape[0]
    width = wq.shape[1] // G
    pairs = G // 2
    weights = (wq, wk, wv)

    swap_dev = (t * R + r, g)
    barrier = pltpu.get_barrier_semaphore()

    def greet(dev):
        pl.semaphore_signal(barrier, inc=1, device_id=dev, device_id_type=MESH)

    for i in range(1, G):
        greet((s, lax.rem(t + i, G)))
        greet((lax.rem(g + i, G) * R + r, t))
    for i in range(1, R):
        greet((g * R + lax.rem(r + i, R), t))

    @pl.when(g != t)
    def _():
        greet(swap_dev)

    pl.semaphore_wait(barrier, 2 * (G - 1) + (R - 1) + jnp.where(g != t, 1, 0))

    def swap_copy():
        return pltpu.make_async_remote_copy(
            src_ref=act, dst_ref=a_buf.at[g], send_sem=swap_send, recv_sem=swap_recv,
            device_id=swap_dev, device_id_type=MESH)

    def swap_local():
        return pltpu.make_async_copy(act, a_buf.at[t], local_sem)

    @pl.when(g != t)
    def _():
        swap_copy().start()

    @pl.when(g == t)
    def _():
        swap_local().start()

    def pair_at(stage):
        return lax.rem(lax.div(g, 2) + 1 + stage, pairs)

    def pair_cols(stage):
        return pl.ds(pl.multiple_of(pair_at(stage) * (2 * width), 128), 2 * width)

    def w_copy(stage, i, x):
        cols = pair_cols(stage)
        return pltpu.make_async_remote_copy(
            src_ref=weights[x].at[:, cols], dst_ref=w_buf.at[i - 1, x, :, cols],
            send_sem=w_send.at[stage, i - 1, x], recv_sem=w_recv.at[stage, i - 1, x],
            device_id=(g * R + lax.rem(r + R - i, R), t), device_id_type=MESH)

    for stage in range(pairs):
        for i in range(1, R):
            for x in range(3):
                w_copy(stage, i, x).start()

    @pl.when(g != t)
    def _():
        swap_copy().wait_recv()

    @pl.when(g == t)
    def _():
        swap_local().wait()

    def fan_copy(i):
        return pltpu.make_async_remote_copy(
            src_ref=a_buf.at[t], dst_ref=a_buf.at[t], send_sem=fan_send.at[i - 1],
            recv_sem=fan_recv.at[i - 1],
            device_id=(s, lax.rem(t + i, G)), device_id_type=MESH)

    def fan_arrival(i):
        slot = lax.rem(t + G - i, G)
        return pltpu.make_async_remote_copy(
            src_ref=a_buf.at[slot], dst_ref=a_buf.at[slot], send_sem=fan_send.at[i - 1],
            recv_sem=fan_recv.at[i - 1],
            device_id=(s, lax.rem(t + i, G)), device_id_type=MESH)

    for i in range(1, G):
        fan_copy(i).start()
    for i in range(1, G):
        fan_arrival(i).wait_recv()

    def c_copy(stage, j, b):
        dest = pair_at(stage) * 2 + j
        rows = pl.ds(pl.multiple_of(b * tok, tok), tok)
        return pltpu.make_async_remote_copy(
            src_ref=c_buf.at[stage, j, rows], dst_ref=r_buf.at[g, rows],
            send_sem=c_send.at[stage, j, b], recv_sem=c_recv.at[g, b],
            device_id=(dest * R + r, t), device_id_type=MESH)

    for stage in range(pairs):
        for i in range(1, R):
            for x in range(3):
                w_copy(stage, i, x).wait_recv()
        cols = pair_cols(stage)

        @pl.loop(0, G)
        def _(b):
            parts = []
            for x in range(3):
                total = jnp.dot(
                    a_buf[b, :, pl.ds(pl.multiple_of(r * krows, 128), krows)],
                    weights[x][:, cols], preferred_element_type=jnp.float32)
                for i in range(1, R):
                    start = pl.multiple_of(lax.rem(r + i, R) * krows, 128)
                    total = total + jnp.dot(
                        a_buf[b, :, pl.ds(start, krows)], w_buf[i - 1, x, :, cols],
                        preferred_element_type=jnp.float32)
                parts.append(total)
            rows = pl.ds(pl.multiple_of(b * tok, tok), tok)
            for j in range(2):
                c_buf[stage, j, rows, :] = jnp.concatenate(
                    [part[:, j * width:(j + 1) * width] for part in parts], axis=1
                ).astype(jnp.bfloat16)
            for j in range(2):
                @pl.when(pair_at(stage) * 2 + j != g)
                def _():
                    c_copy(stage, j, b).start()

    def c_arrival(source, b):
        rows = pl.ds(pl.multiple_of(b * tok, tok), tok)
        return pltpu.make_async_remote_copy(
            src_ref=r_buf.at[source, rows], dst_ref=r_buf.at[source, rows],
            send_sem=c_send.at[0, 0, b], recv_sem=c_recv.at[source, b],
            device_id=(s, t), device_id_type=MESH)

    mine = lax.rem(g, 2)
    most = SPAN * DILATIONS[-1]
    kv_buf[0:most, :] = jnp.zeros((most, 2 * width), jnp.bfloat16)

    def kv_rows(b, part):
        return pl.ds(pl.multiple_of(most + (b * R + part) * tok, 128), tok)

    def kv_copy(i, b):
        rows = kv_rows(b, r)
        return pltpu.make_async_remote_copy(
            src_ref=kv_buf.at[rows], dst_ref=kv_buf.at[rows],
            send_sem=kv_send.at[i - 1, b], recv_sem=kv_recv.at[i - 1, b],
            device_id=(g * R + lax.rem(r + R - i, R), t), device_id_type=MESH)

    def kv_arrival(i, b):
        rows = kv_rows(b, lax.rem(r + i, R))
        return pltpu.make_async_remote_copy(
            src_ref=kv_buf.at[rows], dst_ref=kv_buf.at[rows],
            send_sem=kv_send.at[i - 1, b], recv_sem=kv_recv.at[i - 1, b],
            device_id=(g * R + lax.rem(r + R - i, R), t), device_id_type=MESH)

    def gather_block(b):
        rows = pl.ds(pl.multiple_of(b * tok, tok), tok)
        total = c_buf[pairs - 1, mine, rows, :].astype(jnp.float32)
        for i in range(1, G):
            source = lax.rem(g + i, G)
            c_arrival(source, b).wait_recv()
            total = total + r_buf[source, rows, :].astype(jnp.float32)
        turn = total[:, :2 * width]
        half = HEAD // 2
        ahead = jnp.concatenate([turn[:, half:], turn[:, :half]], axis=1)
        behind = jnp.concatenate([turn[:, -half:], turn[:, :-half]], axis=1)
        lane = lax.broadcasted_iota(jnp.int32, turn.shape, 1)
        other = jnp.where((lane & (HEAD - 1)) < half, ahead, behind)
        reps = 2 * width // cos_ref.shape[1]
        cosine = jnp.concatenate([cos_ref[rows, :]] * reps, axis=1)
        sine = jnp.concatenate([sin_ref[rows, :]] * reps, axis=1)
        turned = turn * cosine + other * sine
        q_buf[rows, :] = turned[:, :width].astype(jnp.bfloat16)
        kv_buf[kv_rows(b, r), :] = jnp.concatenate(
            [turned[:, width:], total[:, 2 * width:]], axis=1).astype(jnp.bfloat16)
        for i in range(1, R):
            kv_copy(i, b).start()

    def m_copy(b):
        return pltpu.make_async_remote_copy(
            src_ref=o_buf.at[b], dst_ref=m_buf.at[g],
            send_sem=m_send.at[b], recv_sem=m_recv.at[g],
            device_id=(b * R + r, t), device_id_type=MESH)

    def m_arrival(source):
        return pltpu.make_async_remote_copy(
            src_ref=m_buf.at[source], dst_ref=m_buf.at[source],
            send_sem=m_send.at[source], recv_sem=m_recv.at[source],
            device_id=(source * R + r, t), device_id_type=MESH)

    def attend(b):
        for i in range(1, R):
            kv_arrival(i, b).wait_recv()
        rows = pl.ds(pl.multiple_of(b * tok, tok), tok)
        first = (b * R + r) * tok
        mixed_list = []
        total_list = []
        for index, dilation in enumerate(DILATIONS):
            reach = SPAN * dilation
            keys = reach + tok
            near = pl.ds(pl.multiple_of(most - reach + first, 128), keys)
            q = q_buf[rows, index * HEAD:(index + 1) * HEAD]
            k = kv_buf[near, index * HEAD:(index + 1) * HEAD]
            v = kv_buf[near, width + index * HEAD:width + (index + 1) * HEAD]
            scores = lax.dot_general(
                q, k, (((1,), (1,)), ((), ())), preferred_element_type=jnp.float32
            ) * HEAD ** (-0.5)
            col = lax.broadcasted_iota(jnp.int32, (tok, keys), 1)
            gap = reach + lax.broadcasted_iota(jnp.int32, (tok, keys), 0) - col
            allowed = (gap >= 0) & (gap <= reach) & (col >= reach - first)
            if dilation > 1:
                allowed = allowed & ((gap & (dilation - 1)) == 0)
            scores = jnp.where(allowed, scores, -jnp.inf)
            row_max = jnp.max(scores, axis=1, keepdims=True)
            expo = jnp.exp(scores - row_max)
            denominator = jnp.sum(expo, axis=1, keepdims=True)
            mixed = jnp.dot(expo.astype(jnp.bfloat16), v, preferred_element_type=jnp.float32)
            mixed_list.append(mixed / denominator)
            total_list.append(row_max + jnp.log(denominator))
        peak = jnp.maximum(jnp.maximum(total_list[0], total_list[1]), total_list[2])
        shifted = [jnp.exp(one - peak) for one in total_list]
        whole = shifted[0] + shifted[1] + shifted[2]
        merged = sum(a / whole * b_ for a, b_ in zip(shifted, mixed_list)).astype(jnp.bfloat16)

        @pl.when(b != g)
        def _():
            o_buf[b] = merged
            m_copy(b).start()

        @pl.when(b == g)
        def _():
            m_buf[b] = merged

    gather_block(0)

    @pl.loop(1, G)
    def _(b):
        gather_block(b)
        attend(b - 1)

    attend(G - 1)

    for i in range(1, G):
        m_arrival(lax.rem(g + i, G)).wait_recv()
    out[...] = jnp.concatenate(
        [m_buf[h].astype(jnp.float32) for h in range(G)], axis=1).astype(jnp.bfloat16)

    for i in range(1, G):
        m_copy(lax.rem(g + i, G)).wait_send()

    @pl.loop(0, G)
    def _(b):
        for i in range(1, R):
            kv_copy(i, b).wait_send()

    @pl.when(g != t)
    def _():
        swap_copy().wait_send()

    for i in range(1, G):
        fan_copy(i).wait_send()
    for stage in range(pairs):
        for i in range(1, R):
            for x in range(3):
                w_copy(stage, i, x).wait_send()
        for j in range(2):
            @pl.when(pair_at(stage) * 2 + j != g)
            def _():
                @pl.loop(0, G)
                def _(b):
                    c_copy(stage, j, b).wait_send()


def project(activity, wq, wk, wv, cosine, sine, G, R):
    tok, feat = activity.shape
    krows, col_width = wq.shape
    width = 3 * (col_width // G)
    pairs = G // 2
    rows = G * tok
    dma = pltpu.SemaphoreType.DMA
    return pl.pallas_call(
        functools.partial(project_kernel, G, R),
        out_shape=jax.ShapeDtypeStruct((tok, G * HEAD), jnp.bfloat16),
        in_specs=[pl.BlockSpec(memory_space=pltpu.VMEM)] * 6,
        out_specs=pl.BlockSpec(memory_space=pltpu.VMEM),
        scratch_shapes=[
            pltpu.VMEM((G, tok, feat), jnp.bfloat16),
            pltpu.VMEM((R - 1, 3, krows, col_width), jnp.bfloat16),
            pltpu.VMEM((pairs, 2, rows, width), jnp.bfloat16),
            pltpu.VMEM((G, rows, width), jnp.bfloat16),
            pltpu.VMEM((rows, width // 3), jnp.bfloat16),
            pltpu.VMEM((SPAN * DILATIONS[-1] + R * rows, 2 * (width // 3)), jnp.bfloat16),
            pltpu.VMEM((G, tok, HEAD), jnp.bfloat16),
            pltpu.VMEM((G, tok, HEAD), jnp.bfloat16),
            dma, dma, dma, dma((G - 1,)), dma((G - 1,)),
            dma((pairs, R - 1, 3)), dma((pairs, R - 1, 3)),
            dma((pairs, 2, G)), dma((G, G)),
            dma((R - 1, G)), dma((R - 1, G)), dma((G,)), dma((G,)),
        ],
        compiler_params=pltpu.CompilerParams(
            collective_id=0, has_side_effects=True, vmem_limit_bytes=58 * 2**20),
        cost_estimate=pl.CostEstimate(
            flops=2 * rows * feat * 3 * col_width, bytes_accessed=300 * 2**20, transcendentals=0),
    )(activity, wq, wk, wv, cosine, sine)


def finish_kernel(merged, weight, out, near_out, near_in, far_out, far_in, held,
                  near_send, near_recv, far_send, far_recv):
    s = lax.axis_index("sp")
    t = lax.axis_index("tp")
    chunks = near_out.shape[0]
    rows = out.shape[0]
    cols = weight.shape[1] // chunks
    low = lax.rem(t, 2)
    near = t + 1 - 2 * low
    far = lax.rem(t + 2, 4)
    across = lax.rem(near + 2, 4)

    barrier = pltpu.get_barrier_semaphore()
    for peer in (near, far):
        pl.semaphore_signal(barrier, inc=1, device_id=(s, peer), device_id_type=MESH)
    pl.semaphore_wait(barrier, 2)

    def near_copy(c):
        return pltpu.make_async_remote_copy(
            src_ref=near_out.at[c], dst_ref=near_in.at[c], send_sem=near_send.at[c],
            recv_sem=near_recv.at[c], device_id=(s, near), device_id_type=MESH)

    def far_copy(c):
        return pltpu.make_async_remote_copy(
            src_ref=far_out.at[c], dst_ref=far_in.at[c], send_sem=far_send.at[c],
            recv_sem=far_recv.at[c], device_id=(s, far), device_id_type=MESH)

    def part(owner, at):
        picked = merged[pl.ds(pl.multiple_of(owner * rows, rows), rows), :]
        return jnp.dot(picked, weight[:, at], preferred_element_type=jnp.float32)

    @pl.loop(0, chunks)
    def _(c):
        at = pl.ds(pl.multiple_of(c * cols, 128), cols)
        near_out[c, 0] = part(across, at).astype(jnp.bfloat16)
        near_out[c, 1] = part(near, at).astype(jnp.bfloat16)
        near_copy(c).start()
        held[c, 0] = part(far, at)
        held[c, 1] = part(t, at)

    @pl.loop(0, chunks)
    def _(c):
        near_copy(c).wait_recv()
        far_out[c] = (held[c, 0] + near_in[c, 0].astype(jnp.float32)).astype(jnp.bfloat16)
        far_copy(c).start()
        held[c, 1] = held[c, 1] + near_in[c, 1].astype(jnp.float32)

    @pl.loop(0, chunks)
    def _(c):
        at = pl.ds(pl.multiple_of(c * cols, 128), cols)
        far_copy(c).wait_recv()
        out[:, at] = (held[c, 1] + far_in[c].astype(jnp.float32)).astype(jnp.bfloat16)

    @pl.loop(0, chunks)
    def _(c):
        near_copy(c).wait_send()
        far_copy(c).wait_send()


def finish(merged, weight, chunks):
    rows = merged.shape[0] // 4
    cols = weight.shape[1] // chunks
    dma = pltpu.SemaphoreType.DMA
    return pl.pallas_call(
        finish_kernel,
        out_shape=jax.ShapeDtypeStruct((rows, weight.shape[1]), jnp.bfloat16),
        in_specs=[pl.BlockSpec(memory_space=pltpu.VMEM)] * 2,
        out_specs=pl.BlockSpec(memory_space=pltpu.VMEM),
        scratch_shapes=[
            pltpu.VMEM((chunks, 2, rows, cols), jnp.bfloat16),
            pltpu.VMEM((chunks, 2, rows, cols), jnp.bfloat16),
            pltpu.VMEM((chunks, rows, cols), jnp.bfloat16),
            pltpu.VMEM((chunks, rows, cols), jnp.bfloat16),
            pltpu.VMEM((chunks, 2, rows, cols), jnp.float32),
            dma((chunks,)), dma((chunks,)), dma((chunks,)), dma((chunks,)),
        ],
        compiler_params=pltpu.CompilerParams(
            collective_id=1, has_side_effects=True, vmem_limit_bytes=40 * 2**20),
    )(merged, weight)


def halves_kernel(
    act, wq, wk, wv, out,
    x_buf, w_buf, own_buf, c_buf, r_buf, q_buf, kv_buf, o_buf, m_buf, cos_buf, sin_buf,
    local_sem, w_local, x_send, x_recv, w_send, w_recv, c_send, c_recv,
    kv_send, kv_recv, m_send, m_recv,
):
    s = lax.axis_index("sp")
    t = lax.axis_index("tp")
    z = lax.div(s, 2)
    y = lax.rem(s, 2)
    x = lax.div(t, 2)
    c = lax.rem(t, 2)
    zh = lax.div(z, 2)
    zl = lax.rem(z, 2)
    G = 4
    tok, feat = act.shape
    krows = wq.shape[0]
    pair = wq.shape[1] // 2
    width = pair // 2
    part = tok // 2
    weights = (wq, wk, wv)
    z_near = z + 1 - 2 * zl
    z_pair = lax.rem(z + 2, 4)
    y_far = 1 - y
    t_flip = 3 - t
    t_core = t + 1 - 2 * c
    hub = c == zh
    inner = zl != zh
    straight = c == x

    def at_z(other):
        return (other * 2 + y, t)

    barrier = pltpu.get_barrier_semaphore()

    def greet(dev):
        pl.semaphore_signal(barrier, inc=1, device_id=dev, device_id_type=MESH)

    for i in range(1, 4):
        greet(at_z(lax.rem(z + i, 4)))
        greet((s, lax.rem(t + i, 4)))
    greet((z * 2 + y_far, t))
    pl.semaphore_wait(barrier, 7)

    def remote(src, dst, send, recv, dev):
        return pltpu.make_async_remote_copy(
            src_ref=src, dst_ref=dst, send_sem=send, recv_sem=recv,
            device_id=dev, device_id_type=MESH)

    def own_rows(block):
        return pl.ds(pl.multiple_of(block * krows, 128), krows)

    def pair_cols(p):
        return pl.ds(pl.multiple_of(p * pair, 128), pair)

    mine_rows = own_rows(zl * 2 + y)
    near_rows = own_rows((1 - zl) * 2 + y)

    def w_own(i):
        return pltpu.make_async_copy(
            weights[i].at[:, pair_cols(zl)], w_buf.at[i, mine_rows], w_local.at[i])

    def w_over_z(i):
        return remote(weights[i].at[:, pair_cols(1 - zl)], w_buf.at[i, mine_rows],
                      w_send.at[0, i], w_recv.at[0, i], at_z(z_near))

    def w_over_y(i):
        return remote(weights[i].at[:, pair_cols(zl)], w_buf.at[i, mine_rows],
                      w_send.at[1, i], w_recv.at[1, i], (z * 2 + y_far, t))

    def w_relay(i):
        return remote(w_buf.at[i, near_rows], w_buf.at[i, near_rows],
                      w_send.at[2, i], w_recv.at[2, i], (z * 2 + y_far, t))

    hold = 8

    def slot(quarter, block):
        return quarter * 4 + block

    def x_swap():
        there = jnp.where(1 - c == zh, slot(1 - x, z), hold)
        return remote(act, x_buf.at[there], x_send.at[0], x_recv.at[there], (s, t_flip))

    def x_here():
        return jnp.where(hub, slot(x, z), hold)

    def x_move(index, block, dev):
        return remote(x_buf.at[block], x_buf.at[block], x_send.at[index], x_recv.at[block], dev)

    def x_arrived(block):
        remote(x_buf.at[block], x_buf.at[block], x_send.at[0], x_recv.at[block], (s, t)).wait_recv()

    def x_cross():
        dest = jnp.where(c == 0, 1, 2)
        return remote(x_buf.at[hold], x_buf.at[slot(x, z)], x_send.at[1],
                      x_recv.at[slot(x, z)], at_z(dest))

    @pl.when(jnp.logical_not(straight))
    def _():
        x_swap().start()

    @pl.when(straight)
    def _():
        pltpu.make_async_copy(act, x_buf.at[x_here()], local_sem).start()

    for i in range(3):
        w_own(i).start()
    w_over_z(0).start()
    w_over_y(0).start()

    @pl.loop(0, 4)
    def _(b):
        rows = pl.ds(pl.multiple_of(b * tok, tok), tok)
        half = HEAD // 2
        lane = lax.broadcasted_iota(jnp.int32, (tok, 128), 1)
        place = (b * 2 + y) * tok + lax.broadcasted_iota(jnp.int32, (tok, 128), 0)
        exponent = lax.rem(lane, half).astype(jnp.float32) * (2.0 / HEAD)
        angle = place.astype(jnp.float32) * jnp.exp(exponent * (-math.log(rope_base)))
        cos_buf[rows, :] = jnp.cos(angle)
        sine = jnp.sin(angle)
        sin_buf[rows, :] = jnp.where(lax.rem(lane, HEAD) < half, -sine, sine)

    @pl.when(straight)
    def _():
        pltpu.make_async_copy(act, x_buf.at[x_here()], local_sem).wait()

    @pl.when(jnp.logical_not(straight))
    def _():
        x_arrived(x_here())

    order = (z, z_near, jnp.where(inner, 3 - z, z_pair), jnp.where(inner, z_pair, 3 - z))
    mine = jnp.where(hub, x, 1 - x)

    @pl.when(hub)
    def _():
        x_move(1, slot(x, z), at_z(z_near)).start()

    @pl.when(jnp.logical_not(hub))
    def _():
        x_cross().start()

    w_over_z(1).start()
    w_over_y(1).start()
    w_over_z(0).wait_recv()
    w_relay(0).start()
    w_over_z(2).start()
    w_over_y(2).start()

    def c_copy(i, b):
        return remote(c_buf.at[i, b], r_buf.at[i, b], c_send.at[i, b], c_recv.at[i, b], at_z(z_pair))

    def part_sum(i, b):
        total = jnp.dot(x_buf[b], w_buf[i, :feat, :], preferred_element_type=jnp.float32)
        total = total + jnp.dot(x_buf[4 + b], w_buf[i, feat:, :], preferred_element_type=jnp.float32)
        low = total[:, :width]
        high = total[:, width:]
        own_buf[i, b] = jnp.where(zh == 0, low, high)
        give = jnp.where(zh == 0, high, low)
        c_buf[i, b] = jnp.concatenate([give[:part], give[part:]], axis=1).astype(jnp.bfloat16)
        c_copy(i, b).start()

    def w_wait(i):
        w_own(i).wait()
        w_over_y(i).wait_recv()
        w_relay(i).wait_recv()

    for step in range(4):
        b = order[step]

        @pl.when(hub)
        def _():
            if step > 0:
                x_arrived(slot(x, b))
            x_move(2 + 2 * step, slot(x, b), (s, t_flip)).start()
            x_move(3 + 2 * step, slot(x, b), (s, t_core)).start()
            if step > 1:
                @pl.when(inner)
                def _():
                    x_move(8 + step, slot(x, b), at_z(z_near)).start()

        @pl.when(jnp.logical_not(hub))
        def _():
            x_arrived(slot(1 - x, b))
            x_move(3 + 2 * step, slot(1 - x, b), (s, t_core)).start()

        if step == 1:
            w_over_z(1).wait_recv()
            w_relay(1).start()
        if step == 0:
            w_wait(0)
        x_arrived(slot(1 - mine, b))
        part_sum(0, b)

    w_wait(1)

    @pl.loop(0, 4)
    def _(i):
        part_sum(1, lax.rem(zh * 2 + i, 4))

    w_over_z(2).wait_recv()
    w_relay(2).start()

    most = SPAN * DILATIONS[-1]
    kv_buf[0:most, :] = jnp.zeros((most, 2 * width), jnp.bfloat16)

    def kv_rows(b, which):
        return pl.ds(pl.multiple_of(most + (b * 2 + which) * tok, 128), tok)

    def kv_copy(b):
        rows = kv_rows(b, y)
        return remote(kv_buf.at[rows], kv_buf.at[rows], kv_send.at[b], kv_recv.at[b],
                      (z * 2 + y_far, t))

    def kv_arrival(b):
        rows = kv_rows(b, y_far)
        return remote(kv_buf.at[rows], kv_buf.at[rows], kv_send.at[b], kv_recv.at[b],
                      (z * 2 + y_far, t))

    def whole_sum(i, b):
        c_copy(i, b).wait_recv()
        came = r_buf[i, b].astype(jnp.float32)
        return own_buf[i, b] + jnp.concatenate([came[:, :width], came[:, width:]], axis=0)

    def rotate(turn, b):
        rows = pl.ds(pl.multiple_of(b * tok, tok), tok)
        half = HEAD // 2
        ahead = jnp.concatenate([turn[:, half:], turn[:, :half]], axis=1)
        behind = jnp.concatenate([turn[:, -half:], turn[:, :-half]], axis=1)
        lane = lax.broadcasted_iota(jnp.int32, turn.shape, 1)
        other = jnp.where((lane & (HEAD - 1)) < half, ahead, behind)
        cosine = jnp.concatenate([cos_buf[rows, :], cos_buf[rows, :HEAD]], axis=1)
        sine = jnp.concatenate([sin_buf[rows, :], sin_buf[rows, :HEAD]], axis=1)
        return (turn * cosine + other * sine).astype(jnp.bfloat16)

    @pl.loop(0, 4)
    def _(b):
        rows = pl.ds(pl.multiple_of(b * tok, tok), tok)
        q_buf[rows, :] = rotate(whole_sum(0, b), b)

    w_wait(2)

    @pl.loop(0, 4)
    def _(b):
        part_sum(2, b)

    @pl.loop(0, 4)
    def _(b):
        kv_buf[kv_rows(b, y), :width] = rotate(whole_sum(1, b), b)

    def gather_block(b):
        kv_buf[kv_rows(b, y), width:] = whole_sum(2, b).astype(jnp.bfloat16)
        kv_copy(b).start()

    head = 2 * zl + zh

    def m_copy(b):
        return remote(o_buf.at[b], m_buf.at[head], m_send.at[b], m_recv.at[head], at_z(b))

    def m_arrival(source):
        return remote(m_buf.at[source], m_buf.at[source], m_send.at[source], m_recv.at[source], at_z(z))

    def attend(b):
        kv_arrival(b).wait_recv()
        rows = pl.ds(pl.multiple_of(b * tok, tok), tok)
        first = (b * 2 + y) * tok
        mixed_list = []
        total_list = []
        for index, dilation in enumerate(DILATIONS):
            reach = SPAN * dilation
            keys = reach + tok
            near = pl.ds(pl.multiple_of(most - reach + first, 128), keys)
            q = q_buf[rows, index * HEAD:(index + 1) * HEAD]
            k = kv_buf[near, index * HEAD:(index + 1) * HEAD]
            v = kv_buf[near, width + index * HEAD:width + (index + 1) * HEAD]
            scores = lax.dot_general(
                q, k, (((1,), (1,)), ((), ())), preferred_element_type=jnp.float32
            ) * HEAD ** (-0.5)
            col = lax.broadcasted_iota(jnp.int32, (tok, keys), 1)
            gap = reach + lax.broadcasted_iota(jnp.int32, (tok, keys), 0) - col
            allowed = (gap >= 0) & (gap <= reach) & (col >= reach - first)
            if dilation > 1:
                allowed = allowed & ((gap & (dilation - 1)) == 0)
            scores = jnp.where(allowed, scores, -jnp.inf)
            row_max = jnp.max(scores, axis=1, keepdims=True)
            expo = jnp.exp(scores - row_max)
            denominator = jnp.sum(expo, axis=1, keepdims=True)
            mixed = jnp.dot(expo.astype(jnp.bfloat16), v, preferred_element_type=jnp.float32)
            mixed_list.append(mixed / denominator)
            total_list.append(row_max + jnp.log(denominator))
        peak = jnp.maximum(jnp.maximum(total_list[0], total_list[1]), total_list[2])
        shifted = [jnp.exp(one - peak) for one in total_list]
        whole = shifted[0] + shifted[1] + shifted[2]
        merged = sum(a / whole * b_ for a, b_ in zip(shifted, mixed_list)).astype(jnp.bfloat16)

        @pl.when(b != z)
        def _():
            o_buf[b] = merged
            m_copy(b).start()

        @pl.when(b == z)
        def _():
            m_buf[head] = merged

    gather_block(0)

    @pl.loop(1, 4)
    def _(b):
        gather_block(b)
        attend(b - 1)

    attend(3)

    for i in range(1, 4):
        source = lax.rem(z + i, 4)
        m_arrival(2 * lax.rem(source, 2) + lax.div(source, 2)).wait_recv()
    out[...] = jnp.concatenate(
        [m_buf[h].astype(jnp.float32) for h in range(4)], axis=1).astype(jnp.bfloat16)

    for i in range(1, 4):
        m_copy(lax.rem(z + i, 4)).wait_send()

    @pl.loop(0, 4)
    def _(b):
        kv_copy(b).wait_send()
        for i in range(3):
            c_copy(i, b).wait_send()

    for i in range(3):
        w_over_z(i).wait_send()
        w_over_y(i).wait_send()
        w_relay(i).wait_send()

    @pl.when(jnp.logical_not(straight))
    def _():
        x_swap().wait_send()

    @pl.when(jnp.logical_not(hub))
    def _():
        x_cross().wait_send()

    @pl.when(hub)
    def _():
        x_move(1, slot(x, z), at_z(z_near)).wait_send()

    for step in range(4):
        b = order[step]

        @pl.when(hub)
        def _():
            x_move(2 + 2 * step, slot(x, b), (s, t_flip)).wait_send()
            x_move(3 + 2 * step, slot(x, b), (s, t_core)).wait_send()
            if step > 1:
                @pl.when(inner)
                def _():
                    x_move(8 + step, slot(x, b), at_z(z_near)).wait_send()

        @pl.when(jnp.logical_not(hub))
        def _():
            x_move(3 + 2 * step, slot(1 - x, b), (s, t_core)).wait_send()


def halves(activity, wq, wk, wv):
    tok, feat = activity.shape
    krows, col_width = wq.shape
    width = col_width // 4
    rows = 4 * tok
    dma = pltpu.SemaphoreType.DMA
    return pl.pallas_call(
        halves_kernel,
        out_shape=jax.ShapeDtypeStruct((tok, 4 * HEAD), jnp.bfloat16),
        in_specs=[pl.BlockSpec(memory_space=pl.ANY)] * 4,
        out_specs=pl.BlockSpec(memory_space=pltpu.VMEM),
        scratch_shapes=[
            pltpu.VMEM((9, tok, feat), jnp.bfloat16),
            pltpu.VMEM((3, 4 * krows, 2 * width), jnp.bfloat16),
            pltpu.VMEM((3, 4, tok, width), jnp.float32),
            pltpu.VMEM((3, 4, tok // 2, 2 * width), jnp.bfloat16),
            pltpu.VMEM((3, 4, tok // 2, 2 * width), jnp.bfloat16),
            pltpu.VMEM((rows, width), jnp.bfloat16),
            pltpu.VMEM((SPAN * DILATIONS[-1] + 2 * rows, 2 * width), jnp.bfloat16),
            pltpu.VMEM((4, tok, HEAD), jnp.bfloat16),
            pltpu.VMEM((4, tok, HEAD), jnp.bfloat16),
            pltpu.VMEM((rows, 128), jnp.float32),
            pltpu.VMEM((rows, 128), jnp.float32),
            dma, dma((3,)), dma((12,)), dma((9,)), dma((3, 3)), dma((3, 3)),
            dma((3, 4)), dma((3, 4)), dma((4,)), dma((4,)), dma((4,)), dma((4,)),
        ],
        compiler_params=pltpu.CompilerParams(
            collective_id=2, has_side_effects=True, vmem_limit_bytes=58 * 2**20),
        cost_estimate=pl.CostEstimate(
            flops=2 * rows * feat * 3 * col_width, bytes_accessed=300 * 2**20, transcendentals=0),
    )(activity, wq, wk, wv)


def per_device(activity, query_weight, key_weight, value_weight, merge_weight):
    G = lax.axis_size("tp")
    R = lax.axis_size("sp") // G
    r = lax.axis_index("sp") % R
    tok = activity.shape[0]
    merge_full = lax.all_gather(merge_weight, "sp", axis=1, tiled=True)
    if G == 4 and R == 2:
        merged = halves(activity, query_weight, key_weight, value_weight)
        return finish(merged, merge_full, 8)
    block_start = (jnp.arange(G, dtype=jnp.int32) * R + r) * tok
    pos = (block_start[:, None] + jnp.arange(tok, dtype=jnp.int32)[None, :]).reshape(G * tok)
    half = HEAD // 2
    frequency = rope_base ** (-jnp.arange(0, half, dtype=jnp.float32) * 2.0 / HEAD)
    angles = pos.astype(jnp.float32)[:, None] * frequency[None, :]
    cosine = jnp.tile(jnp.cos(angles), (1, 4))
    sine = jnp.sin(angles)
    sine = jnp.tile(jnp.concatenate([-sine, sine], axis=1), (1, 2))
    merged = project(activity, query_weight, key_weight, value_weight, cosine, sine, G, R)
    return finish(merged, merge_full, 8)


def solution(mesh):
    placed = (P("sp", "tp"), P("sp", "tp"), P("sp", "tp"), P("sp", "tp"), P("tp", "sp"))
    return jax.shard_map(
        per_device, mesh=mesh, in_specs=placed, out_specs=P(("sp", "tp"), None), check_vma=False
    )
```

```python
import functools
import math

import jax
import jax.numpy as jnp
from jax import lax
from jax.experimental import pallas as pl
from jax.experimental.pallas import tpu as pltpu
from jax.sharding import PartitionSpec as P

HEAD = 64
HEAD_GROUPS = 3
SPAN = 128
DILATIONS = (1, 4, 8)
MESH = pl.DeviceIdType.MESH

rope_base = 500000.0


def project_kernel(
    G, R, act, wq, wk, wv, cos_ref, sin_ref, out,
    a_buf, w_buf, c_buf, r_buf, q_buf, kv_buf, o_buf, m_buf,
    local_sem, swap_send, swap_recv, fan_send, fan_recv,
    w_send, w_recv, c_send, c_recv, kv_send, kv_recv, m_send, m_recv,
):
    s = lax.axis_index("sp")
    t = lax.axis_index("tp")
    g = lax.div(s, R)
    r = lax.rem(s, R)
    tok = act.shape[0]
    krows = wq.shape[0]
    width = wq.shape[1] // G
    pairs = G // 2
    weights = (wq, wk, wv)

    swap_dev = (t * R + r, g)
    barrier = pltpu.get_barrier_semaphore()

    def greet(dev):
        pl.semaphore_signal(barrier, inc=1, device_id=dev, device_id_type=MESH)

    for i in range(1, G):
        greet((s, lax.rem(t + i, G)))
        greet((lax.rem(g + i, G) * R + r, t))
    for i in range(1, R):
        greet((g * R + lax.rem(r + i, R), t))

    @pl.when(g != t)
    def _():
        greet(swap_dev)

    pl.semaphore_wait(barrier, 2 * (G - 1) + (R - 1) + jnp.where(g != t, 1, 0))

    def swap_copy():
        return pltpu.make_async_remote_copy(
            src_ref=act, dst_ref=a_buf.at[g], send_sem=swap_send, recv_sem=swap_recv,
            device_id=swap_dev, device_id_type=MESH)

    def swap_local():
        return pltpu.make_async_copy(act, a_buf.at[t], local_sem)

    @pl.when(g != t)
    def _():
        swap_copy().start()

    @pl.when(g == t)
    def _():
        swap_local().start()

    def pair_at(stage):
        return lax.rem(lax.div(g, 2) + 1 + stage, pairs)

    def pair_cols(stage):
        return pl.ds(pl.multiple_of(pair_at(stage) * (2 * width), 128), 2 * width)

    def w_copy(stage, i, x):
        cols = pair_cols(stage)
        return pltpu.make_async_remote_copy(
            src_ref=weights[x].at[:, cols], dst_ref=w_buf.at[i - 1, x, :, cols],
            send_sem=w_send.at[stage, i - 1, x], recv_sem=w_recv.at[stage, i - 1, x],
            device_id=(g * R + lax.rem(r + R - i, R), t), device_id_type=MESH)

    for stage in range(pairs):
        for i in range(1, R):
            for x in range(3):
                w_copy(stage, i, x).start()

    @pl.when(g != t)
    def _():
        swap_copy().wait_recv()

    @pl.when(g == t)
    def _():
        swap_local().wait()

    def fan_copy(i):
        return pltpu.make_async_remote_copy(
            src_ref=a_buf.at[t], dst_ref=a_buf.at[t], send_sem=fan_send.at[i - 1],
            recv_sem=fan_recv.at[i - 1],
            device_id=(s, lax.rem(t + i, G)), device_id_type=MESH)

    def fan_arrival(i):
        slot = lax.rem(t + G - i, G)
        return pltpu.make_async_remote_copy(
            src_ref=a_buf.at[slot], dst_ref=a_buf.at[slot], send_sem=fan_send.at[i - 1],
            recv_sem=fan_recv.at[i - 1],
            device_id=(s, lax.rem(t + i, G)), device_id_type=MESH)

    for i in range(1, G):
        fan_copy(i).start()
    for i in range(1, G):
        fan_arrival(i).wait_recv()

    def c_copy(stage, j, b):
        dest = pair_at(stage) * 2 + j
        rows = pl.ds(pl.multiple_of(b * tok, tok), tok)
        return pltpu.make_async_remote_copy(
            src_ref=c_buf.at[stage, j, rows], dst_ref=r_buf.at[g, rows],
            send_sem=c_send.at[stage, j, b], recv_sem=c_recv.at[g, b],
            device_id=(dest * R + r, t), device_id_type=MESH)

    for stage in range(pairs):
        for i in range(1, R):
            for x in range(3):
                w_copy(stage, i, x).wait_recv()
        cols = pair_cols(stage)

        @pl.loop(0, G)
        def _(b):
            parts = []
            for x in range(3):
                total = jnp.dot(
                    a_buf[b, :, pl.ds(pl.multiple_of(r * krows, 128), krows)],
                    weights[x][:, cols], preferred_element_type=jnp.float32)
                for i in range(1, R):
                    start = pl.multiple_of(lax.rem(r + i, R) * krows, 128)
                    total = total + jnp.dot(
                        a_buf[b, :, pl.ds(start, krows)], w_buf[i - 1, x, :, cols],
                        preferred_element_type=jnp.float32)
                parts.append(total)
            rows = pl.ds(pl.multiple_of(b * tok, tok), tok)
            for j in range(2):
                c_buf[stage, j, rows, :] = jnp.concatenate(
                    [part[:, j * width:(j + 1) * width] for part in parts], axis=1
                ).astype(jnp.bfloat16)
            for j in range(2):
                @pl.when(pair_at(stage) * 2 + j != g)
                def _():
                    c_copy(stage, j, b).start()

    def c_arrival(source, b):
        rows = pl.ds(pl.multiple_of(b * tok, tok), tok)
        return pltpu.make_async_remote_copy(
            src_ref=r_buf.at[source, rows], dst_ref=r_buf.at[source, rows],
            send_sem=c_send.at[0, 0, b], recv_sem=c_recv.at[source, b],
            device_id=(s, t), device_id_type=MESH)

    mine = lax.rem(g, 2)
    most = SPAN * DILATIONS[-1]
    kv_buf[0:most, :] = jnp.zeros((most, 2 * width), jnp.bfloat16)

    def kv_rows(b, part):
        return pl.ds(pl.multiple_of(most + (b * R + part) * tok, 128), tok)

    def kv_copy(i, b):
        rows = kv_rows(b, r)
        return pltpu.make_async_remote_copy(
            src_ref=kv_buf.at[rows], dst_ref=kv_buf.at[rows],
            send_sem=kv_send.at[i - 1, b], recv_sem=kv_recv.at[i - 1, b],
            device_id=(g * R + lax.rem(r + R - i, R), t), device_id_type=MESH)

    def kv_arrival(i, b):
        rows = kv_rows(b, lax.rem(r + i, R))
        return pltpu.make_async_remote_copy(
            src_ref=kv_buf.at[rows], dst_ref=kv_buf.at[rows],
            send_sem=kv_send.at[i - 1, b], recv_sem=kv_recv.at[i - 1, b],
            device_id=(g * R + lax.rem(r + R - i, R), t), device_id_type=MESH)

    def gather_block(b):
        rows = pl.ds(pl.multiple_of(b * tok, tok), tok)
        total = c_buf[pairs - 1, mine, rows, :].astype(jnp.float32)
        for i in range(1, G):
            source = lax.rem(g + i, G)
            c_arrival(source, b).wait_recv()
            total = total + r_buf[source, rows, :].astype(jnp.float32)
        turn = total[:, :2 * width]
        half = HEAD // 2
        ahead = jnp.concatenate([turn[:, half:], turn[:, :half]], axis=1)
        behind = jnp.concatenate([turn[:, -half:], turn[:, :-half]], axis=1)
        lane = lax.broadcasted_iota(jnp.int32, turn.shape, 1)
        other = jnp.where((lane & (HEAD - 1)) < half, ahead, behind)
        reps = 2 * width // cos_ref.shape[1]
        cosine = jnp.concatenate([cos_ref[rows, :]] * reps, axis=1)
        sine = jnp.concatenate([sin_ref[rows, :]] * reps, axis=1)
        turned = turn * cosine + other * sine
        q_buf[rows, :] = turned[:, :width].astype(jnp.bfloat16)
        kv_buf[kv_rows(b, r), :] = jnp.concatenate(
            [turned[:, width:], total[:, 2 * width:]], axis=1).astype(jnp.bfloat16)
        for i in range(1, R):
            kv_copy(i, b).start()

    def m_copy(b):
        return pltpu.make_async_remote_copy(
            src_ref=o_buf.at[b], dst_ref=m_buf.at[g],
            send_sem=m_send.at[b], recv_sem=m_recv.at[g],
            device_id=(b * R + r, t), device_id_type=MESH)

    def m_arrival(source):
        return pltpu.make_async_remote_copy(
            src_ref=m_buf.at[source], dst_ref=m_buf.at[source],
            send_sem=m_send.at[source], recv_sem=m_recv.at[source],
            device_id=(source * R + r, t), device_id_type=MESH)

    def attend(b):
        for i in range(1, R):
            kv_arrival(i, b).wait_recv()
        rows = pl.ds(pl.multiple_of(b * tok, tok), tok)
        first = (b * R + r) * tok
        mixed_list = []
        total_list = []
        for index, dilation in enumerate(DILATIONS):
            reach = SPAN * dilation
            keys = reach + tok
            near = pl.ds(pl.multiple_of(most - reach + first, 128), keys)
            q = q_buf[rows, index * HEAD:(index + 1) * HEAD]
            k = kv_buf[near, index * HEAD:(index + 1) * HEAD]
            v = kv_buf[near, width + index * HEAD:width + (index + 1) * HEAD]
            scores = lax.dot_general(
                q, k, (((1,), (1,)), ((), ())), preferred_element_type=jnp.float32
            ) * HEAD ** (-0.5)
            col = lax.broadcasted_iota(jnp.int32, (tok, keys), 1)
            gap = reach + lax.broadcasted_iota(jnp.int32, (tok, keys), 0) - col
            allowed = (gap >= 0) & (gap <= reach) & (col >= reach - first)
            if dilation > 1:
                allowed = allowed & ((gap & (dilation - 1)) == 0)
            scores = jnp.where(allowed, scores, -jnp.inf)
            row_max = jnp.max(scores, axis=1, keepdims=True)
            expo = jnp.exp(scores - row_max)
            denominator = jnp.sum(expo, axis=1, keepdims=True)
            mixed = jnp.dot(expo.astype(jnp.bfloat16), v, preferred_element_type=jnp.float32)
            mixed_list.append(mixed / denominator)
            total_list.append(row_max + jnp.log(denominator))
        peak = jnp.maximum(jnp.maximum(total_list[0], total_list[1]), total_list[2])
        shifted = [jnp.exp(one - peak) for one in total_list]
        whole = shifted[0] + shifted[1] + shifted[2]
        merged = sum(a / whole * b_ for a, b_ in zip(shifted, mixed_list)).astype(jnp.bfloat16)

        @pl.when(b != g)
        def _():
            o_buf[b] = merged
            m_copy(b).start()

        @pl.when(b == g)
        def _():
            m_buf[b] = merged

    gather_block(0)

    @pl.loop(1, G)
    def _(b):
        gather_block(b)
        attend(b - 1)

    attend(G - 1)

    for i in range(1, G):
        m_arrival(lax.rem(g + i, G)).wait_recv()
    out[...] = jnp.concatenate(
        [m_buf[h].astype(jnp.float32) for h in range(G)], axis=1).astype(jnp.bfloat16)

    for i in range(1, G):
        m_copy(lax.rem(g + i, G)).wait_send()

    @pl.loop(0, G)
    def _(b):
        for i in range(1, R):
            kv_copy(i, b).wait_send()

    @pl.when(g != t)
    def _():
        swap_copy().wait_send()

    for i in range(1, G):
        fan_copy(i).wait_send()
    for stage in range(pairs):
        for i in range(1, R):
            for x in range(3):
                w_copy(stage, i, x).wait_send()
        for j in range(2):
            @pl.when(pair_at(stage) * 2 + j != g)
            def _():
                @pl.loop(0, G)
                def _(b):
                    c_copy(stage, j, b).wait_send()


def project(activity, wq, wk, wv, cosine, sine, G, R):
    tok, feat = activity.shape
    krows, col_width = wq.shape
    width = 3 * (col_width // G)
    pairs = G // 2
    rows = G * tok
    dma = pltpu.SemaphoreType.DMA
    return pl.pallas_call(
        functools.partial(project_kernel, G, R),
        out_shape=jax.ShapeDtypeStruct((tok, G * HEAD), jnp.bfloat16),
        in_specs=[pl.BlockSpec(memory_space=pltpu.VMEM)] * 6,
        out_specs=pl.BlockSpec(memory_space=pltpu.VMEM),
        scratch_shapes=[
            pltpu.VMEM((G, tok, feat), jnp.bfloat16),
            pltpu.VMEM((R - 1, 3, krows, col_width), jnp.bfloat16),
            pltpu.VMEM((pairs, 2, rows, width), jnp.bfloat16),
            pltpu.VMEM((G, rows, width), jnp.bfloat16),
            pltpu.VMEM((rows, width // 3), jnp.bfloat16),
            pltpu.VMEM((SPAN * DILATIONS[-1] + R * rows, 2 * (width // 3)), jnp.bfloat16),
            pltpu.VMEM((G, tok, HEAD), jnp.bfloat16),
            pltpu.VMEM((G, tok, HEAD), jnp.bfloat16),
            dma, dma, dma, dma((G - 1,)), dma((G - 1,)),
            dma((pairs, R - 1, 3)), dma((pairs, R - 1, 3)),
            dma((pairs, 2, G)), dma((G, G)),
            dma((R - 1, G)), dma((R - 1, G)), dma((G,)), dma((G,)),
        ],
        compiler_params=pltpu.CompilerParams(
            collective_id=0, has_side_effects=True, vmem_limit_bytes=58 * 2**20),
        cost_estimate=pl.CostEstimate(
            flops=2 * rows * feat * 3 * col_width, bytes_accessed=300 * 2**20, transcendentals=0),
    )(activity, wq, wk, wv, cosine, sine)


def finish_kernel(merged, weight, out, near_out, near_in, far_out, far_in, held,
                  near_send, near_recv, far_send, far_recv):
    s = lax.axis_index("sp")
    t = lax.axis_index("tp")
    chunks = near_out.shape[0]
    rows = out.shape[0]
    cols = weight.shape[1] // chunks
    low = lax.rem(t, 2)
    near = t + 1 - 2 * low
    far = lax.rem(t + 2, 4)
    across = lax.rem(near + 2, 4)

    barrier = pltpu.get_barrier_semaphore()
    for peer in (near, far):
        pl.semaphore_signal(barrier, inc=1, device_id=(s, peer), device_id_type=MESH)
    pl.semaphore_wait(barrier, 2)

    def near_copy(c):
        return pltpu.make_async_remote_copy(
            src_ref=near_out.at[c], dst_ref=near_in.at[c], send_sem=near_send.at[c],
            recv_sem=near_recv.at[c], device_id=(s, near), device_id_type=MESH)

    def far_copy(c):
        return pltpu.make_async_remote_copy(
            src_ref=far_out.at[c], dst_ref=far_in.at[c], send_sem=far_send.at[c],
            recv_sem=far_recv.at[c], device_id=(s, far), device_id_type=MESH)

    def part(owner, at):
        picked = merged[pl.ds(pl.multiple_of(owner * rows, rows), rows), :]
        return jnp.dot(picked, weight[:, at], preferred_element_type=jnp.float32)

    @pl.loop(0, chunks)
    def _(c):
        at = pl.ds(pl.multiple_of(c * cols, 128), cols)
        near_out[c, 0] = part(across, at).astype(jnp.bfloat16)
        near_out[c, 1] = part(near, at).astype(jnp.bfloat16)
        near_copy(c).start()
        held[c, 0] = part(far, at)
        held[c, 1] = part(t, at)

    @pl.loop(0, chunks)
    def _(c):
        near_copy(c).wait_recv()
        far_out[c] = (held[c, 0] + near_in[c, 0].astype(jnp.float32)).astype(jnp.bfloat16)
        far_copy(c).start()
        held[c, 1] = held[c, 1] + near_in[c, 1].astype(jnp.float32)

    @pl.loop(0, chunks)
    def _(c):
        at = pl.ds(pl.multiple_of(c * cols, 128), cols)
        far_copy(c).wait_recv()
        out[:, at] = (held[c, 1] + far_in[c].astype(jnp.float32)).astype(jnp.bfloat16)

    @pl.loop(0, chunks)
    def _(c):
        near_copy(c).wait_send()
        far_copy(c).wait_send()


def finish(merged, weight, chunks):
    rows = merged.shape[0] // 4
    cols = weight.shape[1] // chunks
    dma = pltpu.SemaphoreType.DMA
    return pl.pallas_call(
        finish_kernel,
        out_shape=jax.ShapeDtypeStruct((rows, weight.shape[1]), jnp.bfloat16),
        in_specs=[pl.BlockSpec(memory_space=pltpu.VMEM)] * 2,
        out_specs=pl.BlockSpec(memory_space=pltpu.VMEM),
        scratch_shapes=[
            pltpu.VMEM((chunks, 2, rows, cols), jnp.bfloat16),
            pltpu.VMEM((chunks, 2, rows, cols), jnp.bfloat16),
            pltpu.VMEM((chunks, rows, cols), jnp.bfloat16),
            pltpu.VMEM((chunks, rows, cols), jnp.bfloat16),
            pltpu.VMEM((chunks, 2, rows, cols), jnp.float32),
            dma((chunks,)), dma((chunks,)), dma((chunks,)), dma((chunks,)),
        ],
        compiler_params=pltpu.CompilerParams(
            collective_id=1, has_side_effects=True, vmem_limit_bytes=40 * 2**20),
    )(merged, weight)


def halves_kernel(
    act, wq, wk, wv, wm, out,
    x_buf, w_buf, own_buf, c_buf, r_buf, q_buf, kv_buf, o_buf, m_buf, cos_buf, sin_buf,
    wm_buf, merged_buf, near_out, near_in, far_out, far_in, held,
    local_sem, w_local, x_send, x_recv, w_send, w_recv, c_send, c_recv,
    kv_send, kv_recv, m_send, m_recv, wm_local, wm_send, wm_recv,
    near_send, near_recv, far_send, far_recv,
):
    s = lax.axis_index("sp")
    t = lax.axis_index("tp")
    z = lax.div(s, 2)
    y = lax.rem(s, 2)
    x = lax.div(t, 2)
    c = lax.rem(t, 2)
    zh = lax.div(z, 2)
    zl = lax.rem(z, 2)
    G = 4
    tok, feat = act.shape
    krows = wq.shape[0]
    pair = wq.shape[1] // 2
    width = pair // 2
    part = tok // 2
    weights = (wq, wk, wv)
    z_near = z + 1 - 2 * zl
    z_pair = lax.rem(z + 2, 4)
    y_far = 1 - y
    t_flip = 3 - t
    t_core = t + 1 - 2 * c
    hub = c == zh
    inner = zl != zh
    straight = c == x

    def at_z(other):
        return (other * 2 + y, t)

    barrier = pltpu.get_barrier_semaphore()

    def greet(dev):
        pl.semaphore_signal(barrier, inc=1, device_id=dev, device_id_type=MESH)

    for i in range(1, 4):
        greet(at_z(lax.rem(z + i, 4)))
        greet((s, lax.rem(t + i, 4)))
    greet((z * 2 + y_far, t))
    pl.semaphore_wait(barrier, 7)

    def remote(src, dst, send, recv, dev):
        return pltpu.make_async_remote_copy(
            src_ref=src, dst_ref=dst, send_sem=send, recv_sem=recv,
            device_id=dev, device_id_type=MESH)

    def own_rows(block):
        return pl.ds(pl.multiple_of(block * krows, 128), krows)

    def pair_cols(p):
        return pl.ds(pl.multiple_of(p * pair, 128), pair)

    mine_rows = own_rows(zl * 2 + y)
    near_rows = own_rows((1 - zl) * 2 + y)

    def w_own(i):
        return pltpu.make_async_copy(
            weights[i].at[:, pair_cols(zl)], w_buf.at[i, mine_rows], w_local.at[i])

    def w_over_z(i):
        return remote(weights[i].at[:, pair_cols(1 - zl)], w_buf.at[i, mine_rows],
                      w_send.at[0, i], w_recv.at[0, i], at_z(z_near))

    def w_over_y(i):
        return remote(weights[i].at[:, pair_cols(zl)], w_buf.at[i, mine_rows],
                      w_send.at[1, i], w_recv.at[1, i], (z * 2 + y_far, t))

    def w_relay(i):
        return remote(w_buf.at[i, near_rows], w_buf.at[i, near_rows],
                      w_send.at[2, i], w_recv.at[2, i], (z * 2 + y_far, t))

    hold = 8

    def slot(quarter, block):
        return quarter * 4 + block

    def x_swap():
        there = jnp.where(1 - c == zh, slot(1 - x, z), hold)
        return remote(act, x_buf.at[there], x_send.at[0], x_recv.at[there], (s, t_flip))

    def x_here():
        return jnp.where(hub, slot(x, z), hold)

    def x_move(index, block, dev):
        return remote(x_buf.at[block], x_buf.at[block], x_send.at[index], x_recv.at[block], dev)

    def x_arrived(block):
        remote(x_buf.at[block], x_buf.at[block], x_send.at[0], x_recv.at[block], (s, t)).wait_recv()

    def x_cross():
        dest = jnp.where(c == 0, 1, 2)
        return remote(x_buf.at[hold], x_buf.at[slot(x, z)], x_send.at[1],
                      x_recv.at[slot(x, z)], at_z(dest))

    def wm_move(index, block, dev):
        return remote(wm_buf.at[block], wm_buf.at[block], wm_send.at[index], wm_recv.at[block], dev)

    def wm_first():
        return remote(wm, wm_buf.at[s], wm_send.at[0], wm_recv.at[s], at_z(z_pair))

    def wm_here():
        return pltpu.make_async_copy(wm, wm_buf.at[s], wm_local)

    y_dev = (z * 2 + y_far, t)
    mate = z_pair * 2 + y
    wm_pairs = (
        (1, s, y_dev), (2, s, at_z(z_near)), (3, mate, y_dev), (4, mate, at_z(z_near)))
    wm_last = ((5, z_near * 2 + y, y_dev), (6, z_pair * 2 + y_far, at_z(z_near)))

    @pl.when(jnp.logical_not(straight))
    def _():
        x_swap().start()

    @pl.when(straight)
    def _():
        pltpu.make_async_copy(act, x_buf.at[x_here()], local_sem).start()

    for i in range(3):
        w_own(i).start()
    wm_here().start()
    wm_first().start()
    w_over_z(0).start()
    w_over_y(0).start()

    @pl.loop(0, 4)
    def _(b):
        rows = pl.ds(pl.multiple_of(b * tok, tok), tok)
        half = HEAD // 2
        lane = lax.broadcasted_iota(jnp.int32, (tok, 128), 1)
        place = (b * 2 + y) * tok + lax.broadcasted_iota(jnp.int32, (tok, 128), 0)
        exponent = lax.rem(lane, half).astype(jnp.float32) * (2.0 / HEAD)
        angle = place.astype(jnp.float32) * jnp.exp(exponent * (-math.log(rope_base)))
        cos_buf[rows, :] = jnp.cos(angle)
        sine = jnp.sin(angle)
        sin_buf[rows, :] = jnp.where(lax.rem(lane, HEAD) < half, -sine, sine)

    @pl.when(straight)
    def _():
        pltpu.make_async_copy(act, x_buf.at[x_here()], local_sem).wait()

    @pl.when(jnp.logical_not(straight))
    def _():
        x_arrived(x_here())

    order = (z, z_near, jnp.where(inner, 3 - z, z_pair), jnp.where(inner, z_pair, 3 - z))
    mine = jnp.where(hub, x, 1 - x)

    def x_hand_on(step):
        block = slot(x, order[step])
        x_move(2 + 2 * step, block, (s, t_flip)).start()
        x_move(3 + 2 * step, block, (s, t_core)).start()
        if step > 1:
            @pl.when(inner)
            def _():
                x_move(8 + step, block, at_z(z_near)).start()

    def hub_step(step):
        x_arrived(slot(x, order[step]))
        x_hand_on(step)

    def spoke_step(step):
        block = slot(1 - x, order[step])
        x_arrived(block)
        x_move(3 + 2 * step, block, (s, t_core)).start()

    @pl.when(hub)
    def _():
        x_move(1, slot(x, z), at_z(z_near)).start()
        x_hand_on(0)

    @pl.when(jnp.logical_not(hub))
    def _():
        x_cross().start()

    w_over_z(1).start()
    w_over_z(0).wait_recv()
    w_relay(0).start()
    w_over_y(1).start()

    def c_copy(i, b):
        return remote(c_buf.at[i, b], r_buf.at[i, b], c_send.at[i, b], c_recv.at[i, b], at_z(z_pair))

    def part_sum(i, b):
        total = jnp.dot(x_buf[b], w_buf[i, :feat, :], preferred_element_type=jnp.float32)
        total = total + jnp.dot(x_buf[4 + b], w_buf[i, feat:, :], preferred_element_type=jnp.float32)
        low = total[:, :width]
        high = total[:, width:]
        own_buf[i, b] = jnp.where(zh == 0, low, high)
        give = jnp.where(zh == 0, high, low)
        c_buf[i, b] = jnp.concatenate([give[:part], give[part:]], axis=1).astype(jnp.bfloat16)
        c_copy(i, b).start()

    def w_wait(i):
        w_own(i).wait()
        w_over_y(i).wait_recv()
        w_relay(i).wait_recv()

    def other_arrived(step):
        x_arrived(slot(1 - mine, order[step]))

    spoke = jnp.logical_not(hub)
    inner_hub = hub & inner
    outer_hub = hub & jnp.logical_not(inner)

    @pl.when(spoke)
    def _():
        spoke_step(0)

    @pl.when(hub)
    def _():
        hub_step(1)

    @pl.when(inner_hub)
    def _():
        hub_step(2)

    w_wait(0)
    other_arrived(0)
    part_sum(0, order[0])

    w_over_z(1).wait_recv()
    w_relay(1).start()
    w_over_y(2).start()

    @pl.when(inner_hub)
    def _():
        hub_step(3)

    w_over_z(2).start()

    @pl.when(spoke)
    def _():
        spoke_step(1)

    other_arrived(1)
    part_sum(0, order[1])

    @pl.when(spoke)
    def _():
        spoke_step(2)

    @pl.when(outer_hub)
    def _():
        hub_step(2)
        hub_step(3)

    w_wait(1)
    part_sum(1, order[0])
    part_sum(1, order[1])
    w_over_z(2).wait_recv()
    w_relay(2).start()
    other_arrived(2)
    part_sum(0, order[2])
    part_sum(1, order[2])

    @pl.when(spoke)
    def _():
        spoke_step(3)

    other_arrived(3)
    part_sum(0, order[3])
    part_sum(1, order[3])

    most = SPAN * DILATIONS[-1]
    kv_buf[0:most, :] = jnp.zeros((most, 2 * width), jnp.bfloat16)

    def kv_rows(b, which):
        return pl.ds(pl.multiple_of(most + (b * 2 + which) * tok, 128), tok)

    def kv_copy(b):
        rows = kv_rows(b, y)
        return remote(kv_buf.at[rows], kv_buf.at[rows], kv_send.at[b], kv_recv.at[b],
                      (z * 2 + y_far, t))

    def kv_arrival(b):
        rows = kv_rows(b, y_far)
        return remote(kv_buf.at[rows], kv_buf.at[rows], kv_send.at[b], kv_recv.at[b],
                      (z * 2 + y_far, t))

    def whole_sum(i, b):
        c_copy(i, b).wait_recv()
        came = r_buf[i, b].astype(jnp.float32)
        return own_buf[i, b] + jnp.concatenate([came[:, :width], came[:, width:]], axis=0)

    def rotate(turn, b):
        rows = pl.ds(pl.multiple_of(b * tok, tok), tok)
        half = HEAD // 2
        ahead = jnp.concatenate([turn[:, half:], turn[:, :half]], axis=1)
        behind = jnp.concatenate([turn[:, -half:], turn[:, :-half]], axis=1)
        lane = lax.broadcasted_iota(jnp.int32, turn.shape, 1)
        other = jnp.where((lane & (HEAD - 1)) < half, ahead, behind)
        cosine = jnp.concatenate([cos_buf[rows, :], cos_buf[rows, :HEAD]], axis=1)
        sine = jnp.concatenate([sin_buf[rows, :], sin_buf[rows, :HEAD]], axis=1)
        return (turn * cosine + other * sine).astype(jnp.bfloat16)

    @pl.loop(0, 4)
    def _(b):
        rows = pl.ds(pl.multiple_of(b * tok, tok), tok)
        q_buf[rows, :] = rotate(whole_sum(0, b), b)

    w_wait(2)
    wm_here().wait()
    wm_move(0, mate, y_dev).wait_recv()
    for index, block, dev in wm_pairs:
        wm_move(index, block, dev).start()

    @pl.loop(0, 4)
    def _(b):
        part_sum(2, b)

    @pl.loop(0, 4)
    def _(b):
        kv_buf[kv_rows(b, y), :width] = rotate(whole_sum(1, b), b)

    def gather_block(b):
        kv_buf[kv_rows(b, y), width:] = whole_sum(2, b).astype(jnp.bfloat16)
        kv_copy(b).start()

    head = 2 * zl + zh

    def m_copy(b):
        return remote(o_buf.at[b], m_buf.at[head], m_send.at[b], m_recv.at[head], at_z(b))

    def m_arrival(source):
        return remote(m_buf.at[source], m_buf.at[source], m_send.at[source], m_recv.at[source], at_z(z))

    def attend(b):
        kv_arrival(b).wait_recv()
        rows = pl.ds(pl.multiple_of(b * tok, tok), tok)
        first = (b * 2 + y) * tok
        mixed_list = []
        total_list = []
        for index, dilation in enumerate(DILATIONS):
            reach = SPAN * dilation
            keys = reach + tok
            near = pl.ds(pl.multiple_of(most - reach + first, 128), keys)
            q = q_buf[rows, index * HEAD:(index + 1) * HEAD]
            k = kv_buf[near, index * HEAD:(index + 1) * HEAD]
            v = kv_buf[near, width + index * HEAD:width + (index + 1) * HEAD]
            scores = lax.dot_general(
                q, k, (((1,), (1,)), ((), ())), preferred_element_type=jnp.float32
            ) * HEAD ** (-0.5)
            col = lax.broadcasted_iota(jnp.int32, (tok, keys), 1)
            gap = reach + lax.broadcasted_iota(jnp.int32, (tok, keys), 0) - col
            allowed = (gap >= 0) & (gap <= reach) & (col >= reach - first)
            if dilation > 1:
                allowed = allowed & ((gap & (dilation - 1)) == 0)
            scores = jnp.where(allowed, scores, -jnp.inf)
            row_max = jnp.max(scores, axis=1, keepdims=True)
            expo = jnp.exp(scores - row_max)
            denominator = jnp.sum(expo, axis=1, keepdims=True)
            mixed = jnp.dot(expo.astype(jnp.bfloat16), v, preferred_element_type=jnp.float32)
            mixed_list.append(mixed / denominator)
            total_list.append(row_max + jnp.log(denominator))
        peak = jnp.maximum(jnp.maximum(total_list[0], total_list[1]), total_list[2])
        shifted = [jnp.exp(one - peak) for one in total_list]
        whole = shifted[0] + shifted[1] + shifted[2]
        merged = sum(a / whole * b_ for a, b_ in zip(shifted, mixed_list)).astype(jnp.bfloat16)

        @pl.when(b != z)
        def _():
            o_buf[b] = merged
            m_copy(b).start()

        @pl.when(b == z)
        def _():
            m_buf[head] = merged

    gather_block(0)

    @pl.loop(1, 4)
    def _(b):
        gather_block(b)
        attend(b - 1)

    attend(3)

    def wm_came(block):
        wm_move(0, block, y_dev).wait_recv()

    wm_came(z_near * 2 + y)
    wm_came(z_pair * 2 + y_far)
    for index, block, dev in wm_last:
        wm_move(index, block, dev).start()

    for i in range(1, 4):
        source = lax.rem(z + i, 4)
        m_arrival(2 * lax.rem(source, 2) + lax.div(source, 2)).wait_recv()
    merged_buf[...] = jnp.concatenate(
        [m_buf[h].astype(jnp.float32) for h in range(4)], axis=1).astype(jnp.bfloat16)

    far = lax.rem(t + 2, 4)
    across = 3 - t
    piece = out.shape[0]
    cols = wm.shape[1]

    def near_copy(n):
        return remote(near_out.at[n], near_in.at[n], near_send.at[n], near_recv.at[n], (s, t_core))

    def far_copy(n):
        return remote(far_out.at[n], far_in.at[n], far_send.at[n], far_recv.at[n], (s, far))

    chunks = (s, mate, z * 2 + y_far, z_near * 2 + y, z_pair * 2 + y_far,
              lax.rem(z_near + 2, 4) * 2 + y,
              z_near * 2 + y_far, lax.rem(z_near + 2, 4) * 2 + y_far)

    def product(n):
        def rows_of(owner):
            picked = merged_buf[pl.ds(pl.multiple_of(owner * piece, piece), piece), :]
            return jnp.dot(picked, wm_buf[chunks[n]], preferred_element_type=jnp.float32)
        near_out[n, 0] = rows_of(across).astype(jnp.bfloat16)
        near_out[n, 1] = rows_of(t_core).astype(jnp.bfloat16)
        near_copy(n).start()
        held[n, 0] = rows_of(far)
        held[n, 1] = rows_of(t)

    def pass_on(n):
        near_copy(n).wait_recv()
        far_out[n] = (held[n, 0] + near_in[n, 0].astype(jnp.float32)).astype(jnp.bfloat16)
        far_copy(n).start()
        held[n, 1] = held[n, 1] + near_in[n, 1].astype(jnp.float32)

    for n in range(8):
        if n == 2:
            wm_came(chunks[2])
        if n > 4:
            wm_came(chunks[n])
        product(n)
        if n > 0:
            pass_on(n - 1)
    pass_on(7)

    for n in range(8):
        far_copy(n).wait_recv()
        at = pl.ds(pl.multiple_of(chunks[n] * cols, 128), cols)
        out[:, at] = (held[n, 1] + far_in[n].astype(jnp.float32)).astype(jnp.bfloat16)

    for n in range(8):
        near_copy(n).wait_send()
        far_copy(n).wait_send()
    wm_first().wait_send()
    for index, block, dev in wm_pairs + wm_last:
        wm_move(index, block, dev).wait_send()

    for i in range(1, 4):
        m_copy(lax.rem(z + i, 4)).wait_send()

    @pl.loop(0, 4)
    def _(b):
        kv_copy(b).wait_send()
        for i in range(3):
            c_copy(i, b).wait_send()

    for i in range(3):
        w_over_z(i).wait_send()
        w_over_y(i).wait_send()
        w_relay(i).wait_send()

    @pl.when(jnp.logical_not(straight))
    def _():
        x_swap().wait_send()

    @pl.when(jnp.logical_not(hub))
    def _():
        x_cross().wait_send()

    @pl.when(hub)
    def _():
        x_move(1, slot(x, z), at_z(z_near)).wait_send()

    for step in range(4):
        b = order[step]

        @pl.when(hub)
        def _():
            x_move(2 + 2 * step, slot(x, b), (s, t_flip)).wait_send()
            x_move(3 + 2 * step, slot(x, b), (s, t_core)).wait_send()
            if step > 1:
                @pl.when(inner)
                def _():
                    x_move(8 + step, slot(x, b), at_z(z_near)).wait_send()

        @pl.when(jnp.logical_not(hub))
        def _():
            x_move(3 + 2 * step, slot(1 - x, b), (s, t_core)).wait_send()


def halves(activity, wq, wk, wv, wm):
    tok, feat = activity.shape
    krows, col_width = wq.shape
    width = col_width // 4
    rows = 4 * tok
    piece = tok // 4
    cols = wm.shape[1]
    dma = pltpu.SemaphoreType.DMA
    return pl.pallas_call(
        halves_kernel,
        out_shape=jax.ShapeDtypeStruct((piece, 8 * cols), jnp.bfloat16),
        in_specs=[pl.BlockSpec(memory_space=pl.ANY)] * 5,
        out_specs=pl.BlockSpec(memory_space=pltpu.VMEM),
        scratch_shapes=[
            pltpu.VMEM((9, tok, feat), jnp.bfloat16),
            pltpu.VMEM((3, 4 * krows, 2 * width), jnp.bfloat16),
            pltpu.VMEM((3, 4, tok, width), jnp.float32),
            pltpu.VMEM((3, 4, tok // 2, 2 * width), jnp.bfloat16),
            pltpu.VMEM((3, 4, tok // 2, 2 * width), jnp.bfloat16),
            pltpu.VMEM((rows, width), jnp.bfloat16),
            pltpu.VMEM((SPAN * DILATIONS[-1] + 2 * rows, 2 * width), jnp.bfloat16),
            pltpu.VMEM((4, tok, HEAD), jnp.bfloat16),
            pltpu.VMEM((4, tok, HEAD), jnp.bfloat16),
            pltpu.VMEM((rows, 128), jnp.float32),
            pltpu.VMEM((rows, 128), jnp.float32),
            pltpu.VMEM((8, tok, cols), jnp.bfloat16),
            pltpu.VMEM((tok, 4 * HEAD), jnp.bfloat16),
            pltpu.VMEM((8, 2, piece, cols), jnp.bfloat16),
            pltpu.VMEM((8, 2, piece, cols), jnp.bfloat16),
            pltpu.VMEM((8, piece, cols), jnp.bfloat16),
            pltpu.VMEM((8, piece, cols), jnp.bfloat16),
            pltpu.VMEM((8, 2, piece, cols), jnp.float32),
            dma, dma((3,)), dma((12,)), dma((9,)), dma((3, 3)), dma((3, 3)),
            dma((3, 4)), dma((3, 4)), dma((4,)), dma((4,)), dma((4,)), dma((4,)),
            dma, dma((7,)), dma((8,)), dma((8,)), dma((8,)), dma((8,)), dma((8,)),
        ],
        compiler_params=pltpu.CompilerParams(
            collective_id=2, has_side_effects=True, vmem_limit_bytes=58 * 2**20),
        cost_estimate=pl.CostEstimate(
            flops=2 * rows * feat * 3 * col_width, bytes_accessed=300 * 2**20, transcendentals=0),
    )(activity, wq, wk, wv, wm)


def per_device(activity, query_weight, key_weight, value_weight, merge_weight):
    G = lax.axis_size("tp")
    R = lax.axis_size("sp") // G
    r = lax.axis_index("sp") % R
    tok = activity.shape[0]
    if G == 4 and R == 2:
        return halves(activity, query_weight, key_weight, value_weight, merge_weight)
    merge_full = lax.all_gather(merge_weight, "sp", axis=1, tiled=True)
    block_start = (jnp.arange(G, dtype=jnp.int32) * R + r) * tok
    pos = (block_start[:, None] + jnp.arange(tok, dtype=jnp.int32)[None, :]).reshape(G * tok)
    half = HEAD // 2
    frequency = rope_base ** (-jnp.arange(0, half, dtype=jnp.float32) * 2.0 / HEAD)
    angles = pos.astype(jnp.float32)[:, None] * frequency[None, :]
    cosine = jnp.tile(jnp.cos(angles), (1, 4))
    sine = jnp.sin(angles)
    sine = jnp.tile(jnp.concatenate([-sine, sine], axis=1), (1, 2))
    merged = project(activity, query_weight, key_weight, value_weight, cosine, sine, G, R)
    return finish(merged, merge_full, 8)


def solution(mesh):
    placed = (P("sp", "tp"), P("sp", "tp"), P("sp", "tp"), P("sp", "tp"), P("tp", "sp"))
    return jax.shard_map(
        per_device, mesh=mesh, in_specs=placed, out_specs=P(("sp", "tp"), None), check_vma=False
    )
```

```python
import functools
import math

import jax
import jax.numpy as jnp
from jax import lax
from jax.experimental import pallas as pl
from jax.experimental.pallas import tpu as pltpu
from jax.sharding import PartitionSpec as P

HEAD = 64
HEAD_GROUPS = 3
SPAN = 128
DILATIONS = (1, 4, 8)
MESH = pl.DeviceIdType.MESH

rope_base = 500000.0


def project_kernel(
    G, R, act, wq, wk, wv, cos_ref, sin_ref, out,
    a_buf, w_buf, c_buf, r_buf, q_buf, kv_buf, o_buf, m_buf,
    local_sem, swap_send, swap_recv, fan_send, fan_recv,
    w_send, w_recv, c_send, c_recv, kv_send, kv_recv, m_send, m_recv,
):
    s = lax.axis_index("sp")
    t = lax.axis_index("tp")
    g = lax.div(s, R)
    r = lax.rem(s, R)
    tok = act.shape[0]
    krows = wq.shape[0]
    width = wq.shape[1] // G
    pairs = G // 2
    weights = (wq, wk, wv)

    swap_dev = (t * R + r, g)
    barrier = pltpu.get_barrier_semaphore()

    def greet(dev):
        pl.semaphore_signal(barrier, inc=1, device_id=dev, device_id_type=MESH)

    for i in range(1, G):
        greet((s, lax.rem(t + i, G)))
        greet((lax.rem(g + i, G) * R + r, t))
    for i in range(1, R):
        greet((g * R + lax.rem(r + i, R), t))

    @pl.when(g != t)
    def _():
        greet(swap_dev)

    pl.semaphore_wait(barrier, 2 * (G - 1) + (R - 1) + jnp.where(g != t, 1, 0))

    def swap_copy():
        return pltpu.make_async_remote_copy(
            src_ref=act, dst_ref=a_buf.at[g], send_sem=swap_send, recv_sem=swap_recv,
            device_id=swap_dev, device_id_type=MESH)

    def swap_local():
        return pltpu.make_async_copy(act, a_buf.at[t], local_sem)

    @pl.when(g != t)
    def _():
        swap_copy().start()

    @pl.when(g == t)
    def _():
        swap_local().start()

    def pair_at(stage):
        return lax.rem(lax.div(g, 2) + 1 + stage, pairs)

    def pair_cols(stage):
        return pl.ds(pl.multiple_of(pair_at(stage) * (2 * width), 128), 2 * width)

    def w_copy(stage, i, x):
        cols = pair_cols(stage)
        return pltpu.make_async_remote_copy(
            src_ref=weights[x].at[:, cols], dst_ref=w_buf.at[i - 1, x, :, cols],
            send_sem=w_send.at[stage, i - 1, x], recv_sem=w_recv.at[stage, i - 1, x],
            device_id=(g * R + lax.rem(r + R - i, R), t), device_id_type=MESH)

    for stage in range(pairs):
        for i in range(1, R):
            for x in range(3):
                w_copy(stage, i, x).start()

    @pl.when(g != t)
    def _():
        swap_copy().wait_recv()

    @pl.when(g == t)
    def _():
        swap_local().wait()

    def fan_copy(i):
        return pltpu.make_async_remote_copy(
            src_ref=a_buf.at[t], dst_ref=a_buf.at[t], send_sem=fan_send.at[i - 1],
            recv_sem=fan_recv.at[i - 1],
            device_id=(s, lax.rem(t + i, G)), device_id_type=MESH)

    def fan_arrival(i):
        slot = lax.rem(t + G - i, G)
        return pltpu.make_async_remote_copy(
            src_ref=a_buf.at[slot], dst_ref=a_buf.at[slot], send_sem=fan_send.at[i - 1],
            recv_sem=fan_recv.at[i - 1],
            device_id=(s, lax.rem(t + i, G)), device_id_type=MESH)

    for i in range(1, G):
        fan_copy(i).start()
    for i in range(1, G):
        fan_arrival(i).wait_recv()

    def c_copy(stage, j, b):
        dest = pair_at(stage) * 2 + j
        rows = pl.ds(pl.multiple_of(b * tok, tok), tok)
        return pltpu.make_async_remote_copy(
            src_ref=c_buf.at[stage, j, rows], dst_ref=r_buf.at[g, rows],
            send_sem=c_send.at[stage, j, b], recv_sem=c_recv.at[g, b],
            device_id=(dest * R + r, t), device_id_type=MESH)

    for stage in range(pairs):
        for i in range(1, R):
            for x in range(3):
                w_copy(stage, i, x).wait_recv()
        cols = pair_cols(stage)

        @pl.loop(0, G)
        def _(b):
            parts = []
            for x in range(3):
                total = jnp.dot(
                    a_buf[b, :, pl.ds(pl.multiple_of(r * krows, 128), krows)],
                    weights[x][:, cols], preferred_element_type=jnp.float32)
                for i in range(1, R):
                    start = pl.multiple_of(lax.rem(r + i, R) * krows, 128)
                    total = total + jnp.dot(
                        a_buf[b, :, pl.ds(start, krows)], w_buf[i - 1, x, :, cols],
                        preferred_element_type=jnp.float32)
                parts.append(total)
            rows = pl.ds(pl.multiple_of(b * tok, tok), tok)
            for j in range(2):
                c_buf[stage, j, rows, :] = jnp.concatenate(
                    [part[:, j * width:(j + 1) * width] for part in parts], axis=1
                ).astype(jnp.bfloat16)
            for j in range(2):
                @pl.when(pair_at(stage) * 2 + j != g)
                def _():
                    c_copy(stage, j, b).start()

    def c_arrival(source, b):
        rows = pl.ds(pl.multiple_of(b * tok, tok), tok)
        return pltpu.make_async_remote_copy(
            src_ref=r_buf.at[source, rows], dst_ref=r_buf.at[source, rows],
            send_sem=c_send.at[0, 0, b], recv_sem=c_recv.at[source, b],
            device_id=(s, t), device_id_type=MESH)

    mine = lax.rem(g, 2)
    most = SPAN * DILATIONS[-1]
    kv_buf[0:most, :] = jnp.zeros((most, 2 * width), jnp.bfloat16)

    def kv_rows(b, part):
        return pl.ds(pl.multiple_of(most + (b * R + part) * tok, 128), tok)

    def kv_copy(i, b):
        rows = kv_rows(b, r)
        return pltpu.make_async_remote_copy(
            src_ref=kv_buf.at[rows], dst_ref=kv_buf.at[rows],
            send_sem=kv_send.at[i - 1, b], recv_sem=kv_recv.at[i - 1, b],
            device_id=(g * R + lax.rem(r + R - i, R), t), device_id_type=MESH)

    def kv_arrival(i, b):
        rows = kv_rows(b, lax.rem(r + i, R))
        return pltpu.make_async_remote_copy(
            src_ref=kv_buf.at[rows], dst_ref=kv_buf.at[rows],
            send_sem=kv_send.at[i - 1, b], recv_sem=kv_recv.at[i - 1, b],
            device_id=(g * R + lax.rem(r + R - i, R), t), device_id_type=MESH)

    def gather_block(b):
        rows = pl.ds(pl.multiple_of(b * tok, tok), tok)
        total = c_buf[pairs - 1, mine, rows, :].astype(jnp.float32)
        for i in range(1, G):
            source = lax.rem(g + i, G)
            c_arrival(source, b).wait_recv()
            total = total + r_buf[source, rows, :].astype(jnp.float32)
        turn = total[:, :2 * width]
        half = HEAD // 2
        ahead = jnp.concatenate([turn[:, half:], turn[:, :half]], axis=1)
        behind = jnp.concatenate([turn[:, -half:], turn[:, :-half]], axis=1)
        lane = lax.broadcasted_iota(jnp.int32, turn.shape, 1)
        other = jnp.where((lane & (HEAD - 1)) < half, ahead, behind)
        reps = 2 * width // cos_ref.shape[1]
        cosine = jnp.concatenate([cos_ref[rows, :]] * reps, axis=1)
        sine = jnp.concatenate([sin_ref[rows, :]] * reps, axis=1)
        turned = turn * cosine + other * sine
        q_buf[rows, :] = turned[:, :width].astype(jnp.bfloat16)
        kv_buf[kv_rows(b, r), :] = jnp.concatenate(
            [turned[:, width:], total[:, 2 * width:]], axis=1).astype(jnp.bfloat16)
        for i in range(1, R):
            kv_copy(i, b).start()

    def m_copy(b):
        return pltpu.make_async_remote_copy(
            src_ref=o_buf.at[b], dst_ref=m_buf.at[g],
            send_sem=m_send.at[b], recv_sem=m_recv.at[g],
            device_id=(b * R + r, t), device_id_type=MESH)

    def m_arrival(source):
        return pltpu.make_async_remote_copy(
            src_ref=m_buf.at[source], dst_ref=m_buf.at[source],
            send_sem=m_send.at[source], recv_sem=m_recv.at[source],
            device_id=(source * R + r, t), device_id_type=MESH)

    def attend(b):
        for i in range(1, R):
            kv_arrival(i, b).wait_recv()
        rows = pl.ds(pl.multiple_of(b * tok, tok), tok)
        first = (b * R + r) * tok
        mixed_list = []
        total_list = []
        for index, dilation in enumerate(DILATIONS):
            reach = SPAN * dilation
            keys = reach + tok
            near = pl.ds(pl.multiple_of(most - reach + first, 128), keys)
            q = q_buf[rows, index * HEAD:(index + 1) * HEAD]
            k = kv_buf[near, index * HEAD:(index + 1) * HEAD]
            v = kv_buf[near, width + index * HEAD:width + (index + 1) * HEAD]
            scores = lax.dot_general(
                q, k, (((1,), (1,)), ((), ())), preferred_element_type=jnp.float32
            ) * HEAD ** (-0.5)
            col = lax.broadcasted_iota(jnp.int32, (tok, keys), 1)
            gap = reach + lax.broadcasted_iota(jnp.int32, (tok, keys), 0) - col
            allowed = (gap >= 0) & (gap <= reach) & (col >= reach - first)
            if dilation > 1:
                allowed = allowed & ((gap & (dilation - 1)) == 0)
            scores = jnp.where(allowed, scores, -jnp.inf)
            row_max = jnp.max(scores, axis=1, keepdims=True)
            expo = jnp.exp(scores - row_max)
            denominator = jnp.sum(expo, axis=1, keepdims=True)
            mixed = jnp.dot(expo.astype(jnp.bfloat16), v, preferred_element_type=jnp.float32)
            mixed_list.append(mixed / denominator)
            total_list.append(row_max + jnp.log(denominator))
        peak = jnp.maximum(jnp.maximum(total_list[0], total_list[1]), total_list[2])
        shifted = [jnp.exp(one - peak) for one in total_list]
        whole = shifted[0] + shifted[1] + shifted[2]
        merged = sum(a / whole * b_ for a, b_ in zip(shifted, mixed_list)).astype(jnp.bfloat16)

        @pl.when(b != g)
        def _():
            o_buf[b] = merged
            m_copy(b).start()

        @pl.when(b == g)
        def _():
            m_buf[b] = merged

    gather_block(0)

    @pl.loop(1, G)
    def _(b):
        gather_block(b)
        attend(b - 1)

    attend(G - 1)

    for i in range(1, G):
        m_arrival(lax.rem(g + i, G)).wait_recv()
    out[...] = jnp.concatenate(
        [m_buf[h].astype(jnp.float32) for h in range(G)], axis=1).astype(jnp.bfloat16)

    for i in range(1, G):
        m_copy(lax.rem(g + i, G)).wait_send()

    @pl.loop(0, G)
    def _(b):
        for i in range(1, R):
            kv_copy(i, b).wait_send()

    @pl.when(g != t)
    def _():
        swap_copy().wait_send()

    for i in range(1, G):
        fan_copy(i).wait_send()
    for stage in range(pairs):
        for i in range(1, R):
            for x in range(3):
                w_copy(stage, i, x).wait_send()
        for j in range(2):
            @pl.when(pair_at(stage) * 2 + j != g)
            def _():
                @pl.loop(0, G)
                def _(b):
                    c_copy(stage, j, b).wait_send()


def project(activity, wq, wk, wv, cosine, sine, G, R):
    tok, feat = activity.shape
    krows, col_width = wq.shape
    width = 3 * (col_width // G)
    pairs = G // 2
    rows = G * tok
    dma = pltpu.SemaphoreType.DMA
    return pl.pallas_call(
        functools.partial(project_kernel, G, R),
        out_shape=jax.ShapeDtypeStruct((tok, G * HEAD), jnp.bfloat16),
        in_specs=[pl.BlockSpec(memory_space=pltpu.VMEM)] * 6,
        out_specs=pl.BlockSpec(memory_space=pltpu.VMEM),
        scratch_shapes=[
            pltpu.VMEM((G, tok, feat), jnp.bfloat16),
            pltpu.VMEM((R - 1, 3, krows, col_width), jnp.bfloat16),
            pltpu.VMEM((pairs, 2, rows, width), jnp.bfloat16),
            pltpu.VMEM((G, rows, width), jnp.bfloat16),
            pltpu.VMEM((rows, width // 3), jnp.bfloat16),
            pltpu.VMEM((SPAN * DILATIONS[-1] + R * rows, 2 * (width // 3)), jnp.bfloat16),
            pltpu.VMEM((G, tok, HEAD), jnp.bfloat16),
            pltpu.VMEM((G, tok, HEAD), jnp.bfloat16),
            dma, dma, dma, dma((G - 1,)), dma((G - 1,)),
            dma((pairs, R - 1, 3)), dma((pairs, R - 1, 3)),
            dma((pairs, 2, G)), dma((G, G)),
            dma((R - 1, G)), dma((R - 1, G)), dma((G,)), dma((G,)),
        ],
        compiler_params=pltpu.CompilerParams(
            collective_id=0, has_side_effects=True, vmem_limit_bytes=58 * 2**20),
        cost_estimate=pl.CostEstimate(
            flops=2 * rows * feat * 3 * col_width, bytes_accessed=300 * 2**20, transcendentals=0),
    )(activity, wq, wk, wv, cosine, sine)


def finish_kernel(merged, weight, out, near_out, near_in, far_out, far_in, held,
                  near_send, near_recv, far_send, far_recv):
    s = lax.axis_index("sp")
    t = lax.axis_index("tp")
    chunks = near_out.shape[0]
    rows = out.shape[0]
    cols = weight.shape[1] // chunks
    low = lax.rem(t, 2)
    near = t + 1 - 2 * low
    far = lax.rem(t + 2, 4)
    across = lax.rem(near + 2, 4)

    barrier = pltpu.get_barrier_semaphore()
    for peer in (near, far):
        pl.semaphore_signal(barrier, inc=1, device_id=(s, peer), device_id_type=MESH)
    pl.semaphore_wait(barrier, 2)

    def near_copy(c):
        return pltpu.make_async_remote_copy(
            src_ref=near_out.at[c], dst_ref=near_in.at[c], send_sem=near_send.at[c],
            recv_sem=near_recv.at[c], device_id=(s, near), device_id_type=MESH)

    def far_copy(c):
        return pltpu.make_async_remote_copy(
            src_ref=far_out.at[c], dst_ref=far_in.at[c], send_sem=far_send.at[c],
            recv_sem=far_recv.at[c], device_id=(s, far), device_id_type=MESH)

    def part(owner, at):
        picked = merged[pl.ds(pl.multiple_of(owner * rows, rows), rows), :]
        return jnp.dot(picked, weight[:, at], preferred_element_type=jnp.float32)

    @pl.loop(0, chunks)
    def _(c):
        at = pl.ds(pl.multiple_of(c * cols, 128), cols)
        near_out[c, 0] = part(across, at).astype(jnp.bfloat16)
        near_out[c, 1] = part(near, at).astype(jnp.bfloat16)
        near_copy(c).start()
        held[c, 0] = part(far, at)
        held[c, 1] = part(t, at)

    @pl.loop(0, chunks)
    def _(c):
        near_copy(c).wait_recv()
        far_out[c] = (held[c, 0] + near_in[c, 0].astype(jnp.float32)).astype(jnp.bfloat16)
        far_copy(c).start()
        held[c, 1] = held[c, 1] + near_in[c, 1].astype(jnp.float32)

    @pl.loop(0, chunks)
    def _(c):
        at = pl.ds(pl.multiple_of(c * cols, 128), cols)
        far_copy(c).wait_recv()
        out[:, at] = (held[c, 1] + far_in[c].astype(jnp.float32)).astype(jnp.bfloat16)

    @pl.loop(0, chunks)
    def _(c):
        near_copy(c).wait_send()
        far_copy(c).wait_send()


def finish(merged, weight, chunks):
    rows = merged.shape[0] // 4
    cols = weight.shape[1] // chunks
    dma = pltpu.SemaphoreType.DMA
    return pl.pallas_call(
        finish_kernel,
        out_shape=jax.ShapeDtypeStruct((rows, weight.shape[1]), jnp.bfloat16),
        in_specs=[pl.BlockSpec(memory_space=pltpu.VMEM)] * 2,
        out_specs=pl.BlockSpec(memory_space=pltpu.VMEM),
        scratch_shapes=[
            pltpu.VMEM((chunks, 2, rows, cols), jnp.bfloat16),
            pltpu.VMEM((chunks, 2, rows, cols), jnp.bfloat16),
            pltpu.VMEM((chunks, rows, cols), jnp.bfloat16),
            pltpu.VMEM((chunks, rows, cols), jnp.bfloat16),
            pltpu.VMEM((chunks, 2, rows, cols), jnp.float32),
            dma((chunks,)), dma((chunks,)), dma((chunks,)), dma((chunks,)),
        ],
        compiler_params=pltpu.CompilerParams(
            collective_id=1, has_side_effects=True, vmem_limit_bytes=40 * 2**20),
    )(merged, weight)


def halves_kernel(
    act, wq, wk, wv, wm, out,
    x_buf, w_buf, own_buf, c_buf, r_buf, q_buf, kv_buf, ky_out, ky_in, o_buf, m_buf,
    cos_buf, sin_buf, wm_buf, merged_buf, near_out, near_in, far_out, far_in, held,
    done_out,
    local_sem, w_local, x_send, x_recv, w_send, w_recv, c_send, c_recv,
    ky_send, ky_recv, m_send, m_recv, wm_local, wm_send, wm_recv,
    near_send, near_recv, far_send, far_recv, done_send, done_recv,
):
    s = lax.axis_index("sp")
    t = lax.axis_index("tp")
    z = lax.div(s, 2)
    y = lax.rem(s, 2)
    x = lax.div(t, 2)
    c = lax.rem(t, 2)
    zh = lax.div(z, 2)
    zl = lax.rem(z, 2)
    tok, feat = act.shape
    krows = wq.shape[0]
    pair = wq.shape[1] // 2
    width = pair // 2
    part = tok // 2
    weights = (wk, wq, wv)
    z_near = z + 1 - 2 * zl
    z_pair = lax.rem(z + 2, 4)
    y_far = 1 - y
    y_dev = (z * 2 + y_far, t)
    t_flip = 3 - t
    t_core = t + 1 - 2 * c
    hub = c == zh
    spoke = jnp.logical_not(hub)
    inner = zl != zh
    outer = jnp.logical_not(inner)
    straight = c == x
    bent = jnp.logical_not(straight)

    def at_z(other):
        return (other * 2 + y, t)

    barrier = pltpu.get_barrier_semaphore()

    def greet(dev):
        pl.semaphore_signal(barrier, inc=1, device_id=dev, device_id_type=MESH)

    for i in range(1, 4):
        greet(at_z(lax.rem(z + i, 4)))
        greet((s, lax.rem(t + i, 4)))
    greet(y_dev)
    cross_z = jnp.where(c == 0, 1, 2)
    cross_dev = (cross_z * 2 + y, t_core)

    for i in range(1, 4):
        greet((lax.rem(z + i, 4) * 2 + y, t_core))
    pl.semaphore_wait(barrier, 10)

    def remote(src, dst, send, recv, dev):
        return pltpu.make_async_remote_copy(
            src_ref=src, dst_ref=dst, send_sem=send, recv_sem=recv,
            device_id=dev, device_id_type=MESH)

    def own_rows(block):
        return pl.ds(pl.multiple_of(block * krows, 128), krows)

    def pair_cols(p):
        return pl.ds(pl.multiple_of(p * pair, 128), pair)

    mine_rows = own_rows(zl * 2 + y)
    near_rows = own_rows((1 - zl) * 2 + y)

    def w_own(i):
        return pltpu.make_async_copy(
            weights[i].at[:, pair_cols(zl)], w_buf.at[i, mine_rows], w_local.at[i])

    def w_over_z(i):
        return remote(weights[i].at[:, pair_cols(1 - zl)], w_buf.at[i, mine_rows],
                      w_send.at[0, i], w_recv.at[0, i], at_z(z_near))

    def w_over_y(i):
        return remote(weights[i].at[:, pair_cols(zl)], w_buf.at[i, mine_rows],
                      w_send.at[1, i], w_recv.at[1, i], y_dev)

    def w_relay(i):
        return remote(w_buf.at[i, near_rows], w_buf.at[i, near_rows],
                      w_send.at[2, i], w_recv.at[2, i], y_dev)

    def w_wait(i):
        w_own(i).wait()
        w_over_y(i).wait_recv()
        w_relay(i).wait_recv()

    wm_slot = zl * 2 + y
    wm_near_slot = (1 - zl) * 2 + y

    def wm_here():
        return pltpu.make_async_copy(wm, wm_buf.at[wm_slot], wm_local)

    def wm_over_z():
        return remote(wm, wm_buf.at[wm_slot], wm_send.at[0], wm_recv.at[wm_slot], at_z(z_near))

    def wm_over_y():
        return remote(wm, wm_buf.at[wm_slot], wm_send.at[1], wm_recv.at[wm_slot], y_dev)

    def wm_relay():
        return remote(wm_buf.at[wm_near_slot], wm_buf.at[wm_near_slot],
                      wm_send.at[2], wm_recv.at[wm_near_slot], y_dev)

    def wm_came(block):
        remote(wm_buf.at[block], wm_buf.at[block], wm_send.at[0], wm_recv.at[block], y_dev).wait_recv()

    hold = 8
    order = (z, z_near, jnp.where(inner, 3 - z, z_pair), jnp.where(inner, z_pair, 3 - z))

    def slot(quarter, block):
        return quarter * 4 + block

    def x_swap():
        there = jnp.where(1 - c == zh, slot(1 - x, z), hold)
        return remote(act, x_buf.at[there], x_send.at[0], x_recv.at[there], (s, t_flip))

    def x_here():
        return jnp.where(hub, slot(x, z), hold)

    def x_local():
        return pltpu.make_async_copy(act, x_buf.at[x_here()], local_sem)

    def x_move(index, block, dev):
        return remote(x_buf.at[block], x_buf.at[block], x_send.at[index], x_recv.at[block], dev)

    def x_arrived(block):
        remote(x_buf.at[block], x_buf.at[block], x_send.at[0], x_recv.at[block], (s, t)).wait_recv()

    def x_near():
        return x_move(1, slot(x, z), at_z(z_near))

    def x_cross():
        return remote(x_buf.at[hold], x_buf.at[slot(x, z)], x_send.at[1],
                      x_recv.at[slot(x, z)], cross_dev)

    def x_sideways(step):
        return x_move(2 + 2 * step, slot(x, order[step]), (s, t_flip))

    def x_inside(step):
        return x_move(3 + 2 * step, slot(x, order[step]), (s, t_core))

    def x_back(step):
        return x_move(3 + 2 * step, slot(1 - x, order[step]), (s, t_core))

    def x_outward(step):
        return x_move(8 + step, slot(x, order[step]), at_z(z_near))

    def lead(step):
        if step > 0:
            x_arrived(slot(x, order[step]))
        if step > 1:
            @pl.when(inner)
            def _():
                x_outward(step).start()
        x_sideways(step).start()
        x_inside(step).start()

    def follow(step):
        x_arrived(slot(1 - x, order[step]))
        x_back(step).start()

    def other_arrived(step):
        leads = hub if step < 2 else spoke
        x_arrived(slot(jnp.where(leads, 1 - x, x), order[step]))

    def packed(rows):
        return jnp.concatenate([rows[:part], rows[part:]], axis=1)

    def c_copy(i, b):
        return remote(c_buf.at[i, b], r_buf.at[i, b], c_send.at[i, b], c_recv.at[i, b], at_z(z_pair))

    def part_sum(i, b, held_back):
        total = jnp.dot(x_buf[b], w_buf[i, :feat, :], preferred_element_type=jnp.float32)
        total = total + jnp.dot(x_buf[4 + b], w_buf[i, feat:, :], preferred_element_type=jnp.float32)
        low = packed(total[:, :width])
        high = packed(total[:, width:])
        own_buf[i, b] = jnp.where(zh == 0, low, high)
        c_buf[i, b] = jnp.where(zh == 0, high, low).astype(jnp.bfloat16)
        if not held_back:
            c_copy(i, b).start()
        else:
            @pl.when(outer)
            def _():
                c_copy(i, b).start()

    w_over_z(0).start()
    w_over_y(0).start()

    @pl.when(bent)
    def _():
        x_swap().start()

    @pl.when(straight)
    def _():
        x_local().start()

    for i in range(3):
        w_own(i).start()
    wm_here().start()

    def x_first():
        @pl.when(hub)
        def _():
            x_near().start()
            lead(0)
            w_over_z(1).start()
            w_over_z(2).start()

        @pl.when(spoke)
        def _():
            x_cross().start()
            w_over_z(1).start()

    @pl.when(straight)
    def _():
        x_local().wait()
        x_first()

    @pl.loop(0, 4)
    def _(b):
        half = HEAD // 2
        shape = (part, pair)
        lane = lax.broadcasted_iota(jnp.int32, shape, 1)
        place = (b * 2 + y) * tok + lax.broadcasted_iota(jnp.int32, shape, 0)
        place = place + jnp.where(lane < width, 0, part)
        exponent = (lane & (half - 1)).astype(jnp.float32) * (2.0 / HEAD)
        angle = place.astype(jnp.float32) * jnp.exp(exponent * (-math.log(rope_base)))
        cos_buf[b] = jnp.cos(angle)
        sine = jnp.sin(angle)
        sin_buf[b] = jnp.where((lane & (HEAD - 1)) < half, -sine, sine)

    @pl.when(bent)
    def _():
        x_arrived(x_here())
        x_first()

    w_over_z(0).wait_recv()
    w_relay(0).start()
    w_over_y(1).start()

    @pl.when(spoke)
    def _():
        follow(0)

        @pl.when(inner)
        def _():
            lead(2)

    @pl.when(hub)
    def _():
        lead(1)

    w_wait(0)
    other_arrived(0)
    part_sum(0, order[0], False)

    w_over_z(1).wait_recv()
    w_relay(1).start()
    w_over_y(2).start()

    @pl.when(spoke)
    def _():
        @pl.when(inner)
        def _():
            lead(3)

        w_over_z(2).start()
        follow(1)

    @pl.when(hub & inner)
    def _():
        follow(2)

    other_arrived(1)
    part_sum(0, order[1], False)

    @pl.when(spoke & outer)
    def _():
        lead(2)

    @pl.when(hub & inner)
    def _():
        follow(3)

    w_wait(1)
    part_sum(1, order[0], True)
    part_sum(1, order[1], True)

    @pl.when(spoke & outer)
    def _():
        lead(3)

    @pl.when(hub & outer)
    def _():
        follow(2)

    w_over_z(2).wait_recv()
    w_relay(2).start()
    other_arrived(2)
    part_sum(0, order[2], True)
    part_sum(1, order[2], True)

    @pl.when(hub & outer)
    def _():
        follow(3)

    other_arrived(3)
    part_sum(0, order[3], True)
    part_sum(1, order[3], True)

    w_over_z(2).wait_send()
    wm_over_z().start()
    wm_over_y().start()

    @pl.when(inner)
    def _():
        for i in range(2):
            for step in range(4):
                if i == 1 or step > 1:
                    c_copy(i, order[step]).start()

    most = SPAN * DILATIONS[-1]
    kv_buf[0:most, :] = jnp.zeros((most, 2 * width), jnp.bfloat16)

    w_wait(2)

    @pl.loop(0, 4)
    def _(b):
        part_sum(2, b, False)

    def kv_rows(b, which):
        return pl.ds(pl.multiple_of(most + (b * 2 + which) * tok, 128), tok)

    def ky_copy(i, b):
        return remote(ky_out.at[i, b], ky_in.at[i, b], ky_send.at[i, b], ky_recv.at[i, b], y_dev)

    def whole_sum(i, b):
        c_copy(i, b).wait_recv()
        return own_buf[i, b] + r_buf[i, b].astype(jnp.float32)

    def unpacked(both):
        return jnp.concatenate([both[:, :width], both[:, width:]], axis=0)

    def rotate(turn, b):
        half = HEAD // 2
        ahead = jnp.concatenate([turn[:, half:], turn[:, :half]], axis=1)
        behind = jnp.concatenate([turn[:, -half:], turn[:, :-half]], axis=1)
        lane = lax.broadcasted_iota(jnp.int32, turn.shape, 1)
        other = jnp.where((lane & (HEAD - 1)) < half, ahead, behind)
        return (turn * cos_buf[b] + other * sin_buf[b]).astype(jnp.bfloat16)

    theirs = (z_pair, lax.rem(z_near + 2, 4), jnp.where(outer, 3 - z_pair, z), jnp.where(outer, z, 3 - z_pair))

    for step in range(4):
        b = theirs[step]
        turned = rotate(whole_sum(0, b), b)
        ky_out[0, b] = turned
        ky_copy(0, b).start()
        kv_buf[kv_rows(b, y), :width] = unpacked(turned)

    wm_came(wm_near_slot)
    wm_relay().start()

    for step in range(4):
        b = theirs[step]
        rows = pl.ds(pl.multiple_of(b * tok, tok), tok)
        q_buf[rows, :] = unpacked(rotate(whole_sum(1, b), b))

    def gather_values(b):
        value = whole_sum(2, b).astype(jnp.bfloat16)
        ky_out[1, b] = value
        ky_copy(1, b).start()
        kv_buf[kv_rows(b, y), width:] = unpacked(value)

    def values_arrived(b):
        ky_copy(0, b).wait_recv()
        kv_buf[kv_rows(b, y_far), :width] = unpacked(ky_in[0, b])
        ky_copy(1, b).wait_recv()
        kv_buf[kv_rows(b, y_far), width:] = unpacked(ky_in[1, b])

    head = 2 * zl + zh

    def m_copy(b, there):
        where = lax.rem(b + 2 * there, 4)
        return remote(o_buf.at[b], m_buf.at[there, head], m_send.at[there, b],
                      m_recv.at[there, head], at_z(where))

    def m_arrival(there, source):
        return remote(m_buf.at[there, source], m_buf.at[there, source], m_send.at[there, source],
                      m_recv.at[there, source], at_z(z))

    def attend(b):
        values_arrived(b)
        rows = pl.ds(pl.multiple_of(b * tok, tok), tok)
        first = (b * 2 + y) * tok
        mixed_list = []
        total_list = []
        for index, dilation in enumerate(DILATIONS):
            reach = SPAN * dilation
            keys = reach + tok
            near = pl.ds(pl.multiple_of(most - reach + first, 128), keys)
            q = q_buf[rows, index * HEAD:(index + 1) * HEAD]
            k = kv_buf[near, index * HEAD:(index + 1) * HEAD]
            v = kv_buf[near, width + index * HEAD:width + (index + 1) * HEAD]
            scores = lax.dot_general(
                q, k, (((1,), (1,)), ((), ())), preferred_element_type=jnp.float32
            ) * HEAD ** (-0.5)
            col = lax.broadcasted_iota(jnp.int32, (tok, keys), 1)
            gap = reach + lax.broadcasted_iota(jnp.int32, (tok, keys), 0) - col
            allowed = (gap >= 0) & (gap <= reach) & (col >= reach - first)
            if dilation > 1:
                allowed = allowed & ((gap & (dilation - 1)) == 0)
            scores = jnp.where(allowed, scores, -jnp.inf)
            row_max = jnp.max(scores, axis=1, keepdims=True)
            expo = jnp.exp(scores - row_max)
            denominator = jnp.sum(expo, axis=1, keepdims=True)
            mixed = jnp.dot(expo.astype(jnp.bfloat16), v, preferred_element_type=jnp.float32)
            mixed_list.append(mixed / denominator)
            total_list.append(row_max + jnp.log(denominator))
        peak = jnp.maximum(jnp.maximum(total_list[0], total_list[1]), total_list[2])
        shifted = [jnp.exp(one - peak) for one in total_list]
        whole = shifted[0] + shifted[1] + shifted[2]
        merged = sum(a / whole * b_ for a, b_ in zip(shifted, mixed_list)).astype(jnp.bfloat16)
        o_buf[b] = merged
        for there in range(2):
            mine = lax.rem(b + 2 * there, 4) == z

            @pl.when(jnp.logical_not(mine))
            def _():
                m_copy(b, there).start()

            @pl.when(mine)
            def _():
                m_buf[there, head] = merged

    gather_values(0)

    gather_values(1)

    @pl.loop(2, 4)
    def _(b):
        gather_values(b)
        attend(b - 2)

    wm_here().wait()

    far = lax.rem(t + 2, 4)
    across = 3 - t
    piece = out.shape[0]
    cols = wm.shape[1]

    def near_copy(n):
        return remote(near_out.at[n], near_in.at[n], near_send.at[n], near_recv.at[n], (s, t_core))

    def far_copy(n):
        return remote(far_out.at[n], far_in.at[n], far_send.at[n], far_recv.at[n], (s, far))

    blocks = (wm_slot, wm_near_slot, zl * 2 + y_far, (1 - zl) * 2 + y_far)

    def goes_over(n):
        return zh == 1 - n // 4

    def product(n):
        there = zh if n < 4 else 1 - zh
        block = blocks[n % 4]

        def rows_of(owner):
            picked = merged_buf[there, pl.ds(pl.multiple_of(owner * piece, piece), piece), :]
            return jnp.dot(picked, wm_buf[block], preferred_element_type=jnp.float32)
        near_out[n, 0] = rows_of(across).astype(jnp.bfloat16)
        near_out[n, 1] = rows_of(t_core).astype(jnp.bfloat16)
        near_copy(n).start()
        held[n, 0] = rows_of(far)
        held[n, 1] = rows_of(t)

    def pass_on(n):
        near_copy(n).wait_recv()
        far_out[n] = (held[n, 0] + near_in[n, 0].astype(jnp.float32)).astype(jnp.bfloat16)
        far_copy(n).start()
        held[n, 1] = held[n, 1] + near_in[n, 1].astype(jnp.float32)

    def total_of(n):
        far_copy(n).wait_recv()
        return (held[n, 1] + far_in[n].astype(jnp.float32)).astype(jnp.bfloat16)

    def block_at(half, n):
        return pl.ds(pl.multiple_of((half * 4 + blocks[n]) * cols, 128), cols)

    def done_copy(n):
        return remote(done_out.at[n], out.at[:, block_at(zh, n)], done_send.at[n],
                      done_recv.at[n], at_z(z_pair))

    def collect(group):
        there = zh if group == 0 else 1 - zh
        for i in range(1, 4):
            source = lax.rem(z + i, 4)
            m_arrival(there, 2 * lax.rem(source, 2) + lax.div(source, 2)).wait_recv()
        merged_buf[there] = jnp.concatenate(
            [m_buf[there, h].astype(jnp.float32) for h in range(4)], axis=1).astype(jnp.bfloat16)

    def project_out(group):
        collect(group)
        for n in range(4 * group, 4 * group + 4):
            if n == 2:
                wm_came(blocks[2])
            if n == 3:
                wm_came(blocks[3])
            product(n)
            if n > 4 * group:
                pass_on(n - 1)
        pass_on(4 * group + 3)

    def settle(group):
        for n in range(4):
            total = total_of(4 * group + n)

            @pl.when(goes_over(4 * group))
            def _():
                done_out[n] = total
                done_copy(n).start()

            @pl.when(jnp.logical_not(goes_over(4 * group)))
            def _():
                out[:, block_at(zh, n)] = total

    attend(2)
    attend(3)
    project_out(0)
    project_out(1)
    settle(0)
    settle(1)
    for n in range(4):
        done_copy(n).wait_recv()

    for n in range(8):
        near_copy(n).wait_send()
        far_copy(n).wait_send()
    for n in range(4):
        done_copy(n).wait_send()
    wm_over_z().wait_send()
    wm_over_y().wait_send()
    wm_relay().wait_send()

    @pl.loop(0, 4)
    def _(b):
        for there in range(2):
            @pl.when(lax.rem(b + 2 * there, 4) != z)
            def _():
                m_copy(b, there).wait_send()
        for i in range(2):
            ky_copy(i, b).wait_send()
        for i in range(3):
            c_copy(i, b).wait_send()

    for i in range(3):
        if i < 2:
            w_over_z(i).wait_send()
        w_over_y(i).wait_send()
        w_relay(i).wait_send()

    @pl.when(bent)
    def _():
        x_swap().wait_send()

    @pl.when(hub)
    def _():
        x_near().wait_send()

    @pl.when(spoke)
    def _():
        x_cross().wait_send()

    for step in range(4):
        leads = hub if step < 2 else spoke

        @pl.when(leads)
        def _():
            x_sideways(step).wait_send()
            x_inside(step).wait_send()
            if step > 1:
                @pl.when(inner)
                def _():
                    x_outward(step).wait_send()

        @pl.when(jnp.logical_not(leads))
        def _():
            x_back(step).wait_send()


def halves(activity, wq, wk, wv, wm):
    tok, feat = activity.shape
    krows, col_width = wq.shape
    width = col_width // 4
    rows = 4 * tok
    piece = tok // 4
    cols = wm.shape[1]
    dma = pltpu.SemaphoreType.DMA
    return pl.pallas_call(
        halves_kernel,
        out_shape=jax.ShapeDtypeStruct((piece, 8 * cols), jnp.bfloat16),
        in_specs=[pl.BlockSpec(memory_space=pltpu.HBM)] * 5,
        out_specs=pl.BlockSpec(memory_space=pltpu.VMEM),
        scratch_shapes=[
            pltpu.VMEM((9, tok, feat), jnp.bfloat16),
            pltpu.VMEM((3, 4 * krows, 2 * width), jnp.bfloat16),
            pltpu.VMEM((3, 4, tok // 2, 2 * width), jnp.float32),
            pltpu.VMEM((3, 4, tok // 2, 2 * width), jnp.bfloat16),
            pltpu.VMEM((3, 4, tok // 2, 2 * width), jnp.bfloat16),
            pltpu.VMEM((rows, width), jnp.bfloat16),
            pltpu.VMEM((SPAN * DILATIONS[-1] + 2 * rows, 2 * width), jnp.bfloat16),
            pltpu.VMEM((2, 4, tok // 2, 2 * width), jnp.bfloat16),
            pltpu.VMEM((2, 4, tok // 2, 2 * width), jnp.bfloat16),
            pltpu.VMEM((4, tok, HEAD), jnp.bfloat16),
            pltpu.VMEM((2, 4, tok, HEAD), jnp.bfloat16),
            pltpu.VMEM((4, tok // 2, 2 * width), jnp.float32),
            pltpu.VMEM((4, tok // 2, 2 * width), jnp.float32),
            pltpu.VMEM((4, tok, cols), jnp.bfloat16),
            pltpu.VMEM((2, tok, 4 * HEAD), jnp.bfloat16),
            pltpu.VMEM((8, 2, piece, cols), jnp.bfloat16),
            pltpu.VMEM((8, 2, piece, cols), jnp.bfloat16),
            pltpu.VMEM((8, piece, cols), jnp.bfloat16),
            pltpu.VMEM((8, piece, cols), jnp.bfloat16),
            pltpu.VMEM((8, 2, piece, cols), jnp.float32),
            pltpu.VMEM((4, piece, cols), jnp.bfloat16),
            dma, dma((3,)), dma((12,)), dma((9,)), dma((3, 3)), dma((3, 3)),
            dma((3, 4)), dma((3, 4)), dma((2, 4)), dma((2, 4)), dma((2, 4)), dma((2, 4)),
            dma, dma((3,)), dma((4,)), dma((8,)), dma((8,)), dma((8,)), dma((8,)),
            dma((4,)), dma((4,)),
        ],
        compiler_params=pltpu.CompilerParams(
            collective_id=2, has_side_effects=True, vmem_limit_bytes=66400000),
        cost_estimate=pl.CostEstimate(
            flops=2 * rows * feat * 3 * col_width, bytes_accessed=300 * 2**20, transcendentals=0),
    )(activity, wq, wk, wv, wm)


def per_device(activity, query_weight, key_weight, value_weight, merge_weight):
    G = lax.axis_size("tp")
    R = lax.axis_size("sp") // G
    r = lax.axis_index("sp") % R
    tok = activity.shape[0]
    if G == 4 and R == 2:
        return halves(activity, query_weight, key_weight, value_weight, merge_weight)
    merge_full = lax.all_gather(merge_weight, "sp", axis=1, tiled=True)
    block_start = (jnp.arange(G, dtype=jnp.int32) * R + r) * tok
    pos = (block_start[:, None] + jnp.arange(tok, dtype=jnp.int32)[None, :]).reshape(G * tok)
    half = HEAD // 2
    frequency = rope_base ** (-jnp.arange(0, half, dtype=jnp.float32) * 2.0 / HEAD)
    angles = pos.astype(jnp.float32)[:, None] * frequency[None, :]
    cosine = jnp.tile(jnp.cos(angles), (1, 4))
    sine = jnp.sin(angles)
    sine = jnp.tile(jnp.concatenate([-sine, sine], axis=1), (1, 2))
    merged = project(activity, query_weight, key_weight, value_weight, cosine, sine, G, R)
    return finish(merged, merge_full, 8)


def solution(mesh):
    placed = (P("sp", "tp"), P("sp", "tp"), P("sp", "tp"), P("sp", "tp"), P("tp", "sp"))
    return jax.shard_map(
        per_device, mesh=mesh, in_specs=placed, out_specs=P(("sp", "tp"), None), check_vma=False
    )
```

```python
import functools
import math

import jax
import jax.numpy as jnp
from jax import lax
from jax.experimental import pallas as pl
from jax.experimental.pallas import tpu as pltpu
from jax.sharding import PartitionSpec as P

HEAD = 64
HEAD_GROUPS = 3
SPAN = 128
DILATIONS = (1, 4, 8)
MESH = pl.DeviceIdType.MESH

rope_base = 500000.0


def project_kernel(
    G, R, act, wq, wk, wv, cos_ref, sin_ref, out,
    a_buf, w_buf, c_buf, r_buf, q_buf, kv_buf, o_buf, m_buf,
    local_sem, swap_send, swap_recv, fan_send, fan_recv,
    w_send, w_recv, c_send, c_recv, kv_send, kv_recv, m_send, m_recv,
):
    s = lax.axis_index("sp")
    t = lax.axis_index("tp")
    g = lax.div(s, R)
    r = lax.rem(s, R)
    tok = act.shape[0]
    krows = wq.shape[0]
    width = wq.shape[1] // G
    pairs = G // 2
    weights = (wq, wk, wv)

    swap_dev = (t * R + r, g)
    barrier = pltpu.get_barrier_semaphore()

    def greet(dev):
        pl.semaphore_signal(barrier, inc=1, device_id=dev, device_id_type=MESH)

    for i in range(1, G):
        greet((s, lax.rem(t + i, G)))
        greet((lax.rem(g + i, G) * R + r, t))
    for i in range(1, R):
        greet((g * R + lax.rem(r + i, R), t))

    @pl.when(g != t)
    def _():
        greet(swap_dev)

    pl.semaphore_wait(barrier, 2 * (G - 1) + (R - 1) + jnp.where(g != t, 1, 0))

    def swap_copy():
        return pltpu.make_async_remote_copy(
            src_ref=act, dst_ref=a_buf.at[g], send_sem=swap_send, recv_sem=swap_recv,
            device_id=swap_dev, device_id_type=MESH)

    def swap_local():
        return pltpu.make_async_copy(act, a_buf.at[t], local_sem)

    @pl.when(g != t)
    def _():
        swap_copy().start()

    @pl.when(g == t)
    def _():
        swap_local().start()

    def pair_at(stage):
        return lax.rem(lax.div(g, 2) + 1 + stage, pairs)

    def pair_cols(stage):
        return pl.ds(pl.multiple_of(pair_at(stage) * (2 * width), 128), 2 * width)

    def w_copy(stage, i, x):
        cols = pair_cols(stage)
        return pltpu.make_async_remote_copy(
            src_ref=weights[x].at[:, cols], dst_ref=w_buf.at[i - 1, x, :, cols],
            send_sem=w_send.at[stage, i - 1, x], recv_sem=w_recv.at[stage, i - 1, x],
            device_id=(g * R + lax.rem(r + R - i, R), t), device_id_type=MESH)

    for stage in range(pairs):
        for i in range(1, R):
            for x in range(3):
                w_copy(stage, i, x).start()

    @pl.when(g != t)
    def _():
        swap_copy().wait_recv()

    @pl.when(g == t)
    def _():
        swap_local().wait()

    def fan_copy(i):
        return pltpu.make_async_remote_copy(
            src_ref=a_buf.at[t], dst_ref=a_buf.at[t], send_sem=fan_send.at[i - 1],
            recv_sem=fan_recv.at[i - 1],
            device_id=(s, lax.rem(t + i, G)), device_id_type=MESH)

    def fan_arrival(i):
        slot = lax.rem(t + G - i, G)
        return pltpu.make_async_remote_copy(
            src_ref=a_buf.at[slot], dst_ref=a_buf.at[slot], send_sem=fan_send.at[i - 1],
            recv_sem=fan_recv.at[i - 1],
            device_id=(s, lax.rem(t + i, G)), device_id_type=MESH)

    for i in range(1, G):
        fan_copy(i).start()
    for i in range(1, G):
        fan_arrival(i).wait_recv()

    def c_copy(stage, j, b):
        dest = pair_at(stage) * 2 + j
        rows = pl.ds(pl.multiple_of(b * tok, tok), tok)
        return pltpu.make_async_remote_copy(
            src_ref=c_buf.at[stage, j, rows], dst_ref=r_buf.at[g, rows],
            send_sem=c_send.at[stage, j, b], recv_sem=c_recv.at[g, b],
            device_id=(dest * R + r, t), device_id_type=MESH)

    for stage in range(pairs):
        for i in range(1, R):
            for x in range(3):
                w_copy(stage, i, x).wait_recv()
        cols = pair_cols(stage)

        @pl.loop(0, G)
        def _(b):
            parts = []
            for x in range(3):
                total = jnp.dot(
                    a_buf[b, :, pl.ds(pl.multiple_of(r * krows, 128), krows)],
                    weights[x][:, cols], preferred_element_type=jnp.float32)
                for i in range(1, R):
                    start = pl.multiple_of(lax.rem(r + i, R) * krows, 128)
                    total = total + jnp.dot(
                        a_buf[b, :, pl.ds(start, krows)], w_buf[i - 1, x, :, cols],
                        preferred_element_type=jnp.float32)
                parts.append(total)
            rows = pl.ds(pl.multiple_of(b * tok, tok), tok)
            for j in range(2):
                c_buf[stage, j, rows, :] = jnp.concatenate(
                    [part[:, j * width:(j + 1) * width] for part in parts], axis=1
                ).astype(jnp.bfloat16)
            for j in range(2):
                @pl.when(pair_at(stage) * 2 + j != g)
                def _():
                    c_copy(stage, j, b).start()

    def c_arrival(source, b):
        rows = pl.ds(pl.multiple_of(b * tok, tok), tok)
        return pltpu.make_async_remote_copy(
            src_ref=r_buf.at[source, rows], dst_ref=r_buf.at[source, rows],
            send_sem=c_send.at[0, 0, b], recv_sem=c_recv.at[source, b],
            device_id=(s, t), device_id_type=MESH)

    mine = lax.rem(g, 2)
    most = SPAN * DILATIONS[-1]
    kv_buf[0:most, :] = jnp.zeros((most, 2 * width), jnp.bfloat16)

    def kv_rows(b, part):
        return pl.ds(pl.multiple_of(most + (b * R + part) * tok, 128), tok)

    def kv_copy(i, b):
        rows = kv_rows(b, r)
        return pltpu.make_async_remote_copy(
            src_ref=kv_buf.at[rows], dst_ref=kv_buf.at[rows],
            send_sem=kv_send.at[i - 1, b], recv_sem=kv_recv.at[i - 1, b],
            device_id=(g * R + lax.rem(r + R - i, R), t), device_id_type=MESH)

    def kv_arrival(i, b):
        rows = kv_rows(b, lax.rem(r + i, R))
        return pltpu.make_async_remote_copy(
            src_ref=kv_buf.at[rows], dst_ref=kv_buf.at[rows],
            send_sem=kv_send.at[i - 1, b], recv_sem=kv_recv.at[i - 1, b],
            device_id=(g * R + lax.rem(r + R - i, R), t), device_id_type=MESH)

    def gather_block(b):
        rows = pl.ds(pl.multiple_of(b * tok, tok), tok)
        total = c_buf[pairs - 1, mine, rows, :].astype(jnp.float32)
        for i in range(1, G):
            source = lax.rem(g + i, G)
            c_arrival(source, b).wait_recv()
            total = total + r_buf[source, rows, :].astype(jnp.float32)
        turn = total[:, :2 * width]
        half = HEAD // 2
        ahead = jnp.concatenate([turn[:, half:], turn[:, :half]], axis=1)
        behind = jnp.concatenate([turn[:, -half:], turn[:, :-half]], axis=1)
        lane = lax.broadcasted_iota(jnp.int32, turn.shape, 1)
        other = jnp.where((lane & (HEAD - 1)) < half, ahead, behind)
        reps = 2 * width // cos_ref.shape[1]
        cosine = jnp.concatenate([cos_ref[rows, :]] * reps, axis=1)
        sine = jnp.concatenate([sin_ref[rows, :]] * reps, axis=1)
        turned = turn * cosine + other * sine
        q_buf[rows, :] = turned[:, :width].astype(jnp.bfloat16)
        kv_buf[kv_rows(b, r), :] = jnp.concatenate(
            [turned[:, width:], total[:, 2 * width:]], axis=1).astype(jnp.bfloat16)
        for i in range(1, R):
            kv_copy(i, b).start()

    def m_copy(b):
        return pltpu.make_async_remote_copy(
            src_ref=o_buf.at[b], dst_ref=m_buf.at[g],
            send_sem=m_send.at[b], recv_sem=m_recv.at[g],
            device_id=(b * R + r, t), device_id_type=MESH)

    def m_arrival(source):
        return pltpu.make_async_remote_copy(
            src_ref=m_buf.at[source], dst_ref=m_buf.at[source],
            send_sem=m_send.at[source], recv_sem=m_recv.at[source],
            device_id=(source * R + r, t), device_id_type=MESH)

    def attend(b):
        for i in range(1, R):
            kv_arrival(i, b).wait_recv()
        rows = pl.ds(pl.multiple_of(b * tok, tok), tok)
        first = (b * R + r) * tok
        mixed_list = []
        total_list = []
        for index, dilation in enumerate(DILATIONS):
            reach = SPAN * dilation
            keys = reach + tok
            near = pl.ds(pl.multiple_of(most - reach + first, 128), keys)
            q = q_buf[rows, index * HEAD:(index + 1) * HEAD]
            k = kv_buf[near, index * HEAD:(index + 1) * HEAD]
            v = kv_buf[near, width + index * HEAD:width + (index + 1) * HEAD]
            scores = lax.dot_general(
                q, k, (((1,), (1,)), ((), ())), preferred_element_type=jnp.float32
            ) * HEAD ** (-0.5)
            col = lax.broadcasted_iota(jnp.int32, (tok, keys), 1)
            gap = reach + lax.broadcasted_iota(jnp.int32, (tok, keys), 0) - col
            allowed = (gap >= 0) & (gap <= reach) & (col >= reach - first)
            if dilation > 1:
                allowed = allowed & ((gap & (dilation - 1)) == 0)
            scores = jnp.where(allowed, scores, -jnp.inf)
            row_max = jnp.max(scores, axis=1, keepdims=True)
            expo = jnp.exp(scores - row_max)
            denominator = jnp.sum(expo, axis=1, keepdims=True)
            mixed = jnp.dot(expo.astype(jnp.bfloat16), v, preferred_element_type=jnp.float32)
            mixed_list.append(mixed / denominator)
            total_list.append(row_max + jnp.log(denominator))
        peak = jnp.maximum(jnp.maximum(total_list[0], total_list[1]), total_list[2])
        shifted = [jnp.exp(one - peak) for one in total_list]
        whole = shifted[0] + shifted[1] + shifted[2]
        merged = sum(a / whole * b_ for a, b_ in zip(shifted, mixed_list)).astype(jnp.bfloat16)

        @pl.when(b != g)
        def _():
            o_buf[b] = merged
            m_copy(b).start()

        @pl.when(b == g)
        def _():
            m_buf[b] = merged

    gather_block(0)

    @pl.loop(1, G)
    def _(b):
        gather_block(b)
        attend(b - 1)

    attend(G - 1)

    for i in range(1, G):
        m_arrival(lax.rem(g + i, G)).wait_recv()
    out[...] = jnp.concatenate(
        [m_buf[h].astype(jnp.float32) for h in range(G)], axis=1).astype(jnp.bfloat16)

    for i in range(1, G):
        m_copy(lax.rem(g + i, G)).wait_send()

    @pl.loop(0, G)
    def _(b):
        for i in range(1, R):
            kv_copy(i, b).wait_send()

    @pl.when(g != t)
    def _():
        swap_copy().wait_send()

    for i in range(1, G):
        fan_copy(i).wait_send()
    for stage in range(pairs):
        for i in range(1, R):
            for x in range(3):
                w_copy(stage, i, x).wait_send()
        for j in range(2):
            @pl.when(pair_at(stage) * 2 + j != g)
            def _():
                @pl.loop(0, G)
                def _(b):
                    c_copy(stage, j, b).wait_send()


def project(activity, wq, wk, wv, cosine, sine, G, R):
    tok, feat = activity.shape
    krows, col_width = wq.shape
    width = 3 * (col_width // G)
    pairs = G // 2
    rows = G * tok
    dma = pltpu.SemaphoreType.DMA
    return pl.pallas_call(
        functools.partial(project_kernel, G, R),
        out_shape=jax.ShapeDtypeStruct((tok, G * HEAD), jnp.bfloat16),
        in_specs=[pl.BlockSpec(memory_space=pltpu.VMEM)] * 6,
        out_specs=pl.BlockSpec(memory_space=pltpu.VMEM),
        scratch_shapes=[
            pltpu.VMEM((G, tok, feat), jnp.bfloat16),
            pltpu.VMEM((R - 1, 3, krows, col_width), jnp.bfloat16),
            pltpu.VMEM((pairs, 2, rows, width), jnp.bfloat16),
            pltpu.VMEM((G, rows, width), jnp.bfloat16),
            pltpu.VMEM((rows, width // 3), jnp.bfloat16),
            pltpu.VMEM((SPAN * DILATIONS[-1] + R * rows, 2 * (width // 3)), jnp.bfloat16),
            pltpu.VMEM((G, tok, HEAD), jnp.bfloat16),
            pltpu.VMEM((G, tok, HEAD), jnp.bfloat16),
            dma, dma, dma, dma((G - 1,)), dma((G - 1,)),
            dma((pairs, R - 1, 3)), dma((pairs, R - 1, 3)),
            dma((pairs, 2, G)), dma((G, G)),
            dma((R - 1, G)), dma((R - 1, G)), dma((G,)), dma((G,)),
        ],
        compiler_params=pltpu.CompilerParams(
            collective_id=0, has_side_effects=True, vmem_limit_bytes=58 * 2**20),
        cost_estimate=pl.CostEstimate(
            flops=2 * rows * feat * 3 * col_width, bytes_accessed=300 * 2**20, transcendentals=0),
    )(activity, wq, wk, wv, cosine, sine)


def finish_kernel(merged, weight, out, near_out, near_in, far_out, far_in, held,
                  near_send, near_recv, far_send, far_recv):
    s = lax.axis_index("sp")
    t = lax.axis_index("tp")
    chunks = near_out.shape[0]
    rows = out.shape[0]
    cols = weight.shape[1] // chunks
    low = lax.rem(t, 2)
    near = t + 1 - 2 * low
    far = lax.rem(t + 2, 4)
    across = lax.rem(near + 2, 4)

    barrier = pltpu.get_barrier_semaphore()
    for peer in (near, far):
        pl.semaphore_signal(barrier, inc=1, device_id=(s, peer), device_id_type=MESH)
    pl.semaphore_wait(barrier, 2)

    def near_copy(c):
        return pltpu.make_async_remote_copy(
            src_ref=near_out.at[c], dst_ref=near_in.at[c], send_sem=near_send.at[c],
            recv_sem=near_recv.at[c], device_id=(s, near), device_id_type=MESH)

    def far_copy(c):
        return pltpu.make_async_remote_copy(
            src_ref=far_out.at[c], dst_ref=far_in.at[c], send_sem=far_send.at[c],
            recv_sem=far_recv.at[c], device_id=(s, far), device_id_type=MESH)

    def part(owner, at):
        picked = merged[pl.ds(pl.multiple_of(owner * rows, rows), rows), :]
        return jnp.dot(picked, weight[:, at], preferred_element_type=jnp.float32)

    @pl.loop(0, chunks)
    def _(c):
        at = pl.ds(pl.multiple_of(c * cols, 128), cols)
        near_out[c, 0] = part(across, at).astype(jnp.bfloat16)
        near_out[c, 1] = part(near, at).astype(jnp.bfloat16)
        near_copy(c).start()
        held[c, 0] = part(far, at)
        held[c, 1] = part(t, at)

    @pl.loop(0, chunks)
    def _(c):
        near_copy(c).wait_recv()
        far_out[c] = (held[c, 0] + near_in[c, 0].astype(jnp.float32)).astype(jnp.bfloat16)
        far_copy(c).start()
        held[c, 1] = held[c, 1] + near_in[c, 1].astype(jnp.float32)

    @pl.loop(0, chunks)
    def _(c):
        at = pl.ds(pl.multiple_of(c * cols, 128), cols)
        far_copy(c).wait_recv()
        out[:, at] = (held[c, 1] + far_in[c].astype(jnp.float32)).astype(jnp.bfloat16)

    @pl.loop(0, chunks)
    def _(c):
        near_copy(c).wait_send()
        far_copy(c).wait_send()


def finish(merged, weight, chunks):
    rows = merged.shape[0] // 4
    cols = weight.shape[1] // chunks
    dma = pltpu.SemaphoreType.DMA
    return pl.pallas_call(
        finish_kernel,
        out_shape=jax.ShapeDtypeStruct((rows, weight.shape[1]), jnp.bfloat16),
        in_specs=[pl.BlockSpec(memory_space=pltpu.VMEM)] * 2,
        out_specs=pl.BlockSpec(memory_space=pltpu.VMEM),
        scratch_shapes=[
            pltpu.VMEM((chunks, 2, rows, cols), jnp.bfloat16),
            pltpu.VMEM((chunks, 2, rows, cols), jnp.bfloat16),
            pltpu.VMEM((chunks, rows, cols), jnp.bfloat16),
            pltpu.VMEM((chunks, rows, cols), jnp.bfloat16),
            pltpu.VMEM((chunks, 2, rows, cols), jnp.float32),
            dma((chunks,)), dma((chunks,)), dma((chunks,)), dma((chunks,)),
        ],
        compiler_params=pltpu.CompilerParams(
            collective_id=1, has_side_effects=True, vmem_limit_bytes=40 * 2**20),
    )(merged, weight)


def halves_kernel(
    act, wq, wk, wv, wm, out,
    x_buf, w_buf, own_buf, c_buf, r_buf, q_buf, kv_buf, ky_out, ky_in, o_buf, m_buf,
    cos_buf, sin_buf, wm_buf, merged_buf, near_out, near_in, far_out, far_in, held,
    done_out, prob_buf, gain_buf,
    local_sem, w_local, x_send, x_recv, w_send, w_recv, c_send, c_recv,
    ky_send, ky_recv, m_send, m_recv, wm_local, wm_send, wm_recv,
    near_send, near_recv, far_send, far_recv, done_send, done_recv,
):
    s = lax.axis_index("sp")
    t = lax.axis_index("tp")
    z = lax.div(s, 2)
    y = lax.rem(s, 2)
    x = lax.div(t, 2)
    c = lax.rem(t, 2)
    zh = lax.div(z, 2)
    zl = lax.rem(z, 2)
    tok, feat = act.shape
    krows = wq.shape[0]
    pair = wq.shape[1] // 2
    width = pair // 2
    part = tok // 2
    weights = (wk, wv, wq)
    z_near = z + 1 - 2 * zl
    z_pair = lax.rem(z + 2, 4)
    y_far = 1 - y
    y_dev = (z * 2 + y_far, t)
    t_flip = 3 - t
    t_core = t + 1 - 2 * c
    hub = c == zh
    spoke = jnp.logical_not(hub)
    inner = zl != zh
    outer = jnp.logical_not(inner)
    straight = c == x
    bent = jnp.logical_not(straight)

    def at_z(other):
        return (other * 2 + y, t)

    barrier = pltpu.get_barrier_semaphore()

    def greet(dev):
        pl.semaphore_signal(barrier, inc=1, device_id=dev, device_id_type=MESH)

    for i in range(1, 4):
        greet(at_z(lax.rem(z + i, 4)))
        greet((s, lax.rem(t + i, 4)))
    greet(y_dev)
    cross_z = jnp.where(c == 0, 1, 2)
    cross_dev = (cross_z * 2 + y, t_core)

    for i in range(1, 4):
        greet((lax.rem(z + i, 4) * 2 + y, t_core))
    pl.semaphore_wait(barrier, 10)

    def remote(src, dst, send, recv, dev):
        return pltpu.make_async_remote_copy(
            src_ref=src, dst_ref=dst, send_sem=send, recv_sem=recv,
            device_id=dev, device_id_type=MESH)

    def own_rows(block):
        return pl.ds(pl.multiple_of(block * krows, 128), krows)

    def pair_cols(p):
        return pl.ds(pl.multiple_of(p * pair, 128), pair)

    mine_rows = own_rows(zl * 2 + y)
    near_rows = own_rows((1 - zl) * 2 + y)

    def w_own(i):
        return pltpu.make_async_copy(
            weights[i].at[:, pair_cols(zl)], w_buf.at[i, mine_rows], w_local.at[i])

    def w_over_z(i):
        return remote(weights[i].at[:, pair_cols(1 - zl)], w_buf.at[i, mine_rows],
                      w_send.at[0, i], w_recv.at[0, i], at_z(z_near))

    def w_over_y(i):
        return remote(weights[i].at[:, pair_cols(zl)], w_buf.at[i, mine_rows],
                      w_send.at[1, i], w_recv.at[1, i], y_dev)

    def w_relay(i):
        return remote(w_buf.at[i, near_rows], w_buf.at[i, near_rows],
                      w_send.at[2, i], w_recv.at[2, i], y_dev)

    def w_wait(i):
        w_own(i).wait()
        w_over_y(i).wait_recv()
        w_relay(i).wait_recv()

    wm_slot = zl * 2 + y
    wm_near_slot = (1 - zl) * 2 + y

    def wm_here():
        return pltpu.make_async_copy(wm, wm_buf.at[wm_slot], wm_local)

    def wm_over_z():
        return remote(wm, wm_buf.at[wm_slot], wm_send.at[0], wm_recv.at[wm_slot], at_z(z_near))

    def wm_over_y():
        return remote(wm, wm_buf.at[wm_slot], wm_send.at[1], wm_recv.at[wm_slot], y_dev)

    def wm_relay():
        return remote(wm_buf.at[wm_near_slot], wm_buf.at[wm_near_slot],
                      wm_send.at[2], wm_recv.at[wm_near_slot], y_dev)

    def wm_came(block):
        remote(wm_buf.at[block], wm_buf.at[block], wm_send.at[0], wm_recv.at[block], y_dev).wait_recv()

    hold = 8
    order = (z, z_near, jnp.where(inner, 3 - z, z_pair), jnp.where(inner, z_pair, 3 - z))

    def slot(quarter, block):
        return quarter * 4 + block

    def x_swap():
        there = jnp.where(1 - c == zh, slot(1 - x, z), hold)
        return remote(act, x_buf.at[there], x_send.at[0], x_recv.at[there], (s, t_flip))

    def x_here():
        return jnp.where(hub, slot(x, z), hold)

    def x_local():
        return pltpu.make_async_copy(act, x_buf.at[x_here()], local_sem)

    def x_move(index, block, dev):
        return remote(x_buf.at[block], x_buf.at[block], x_send.at[index], x_recv.at[block], dev)

    def x_arrived(block):
        remote(x_buf.at[block], x_buf.at[block], x_send.at[0], x_recv.at[block], (s, t)).wait_recv()

    def x_near():
        return x_move(1, slot(x, z), at_z(z_near))

    def x_cross():
        return remote(x_buf.at[hold], x_buf.at[slot(x, z)], x_send.at[1],
                      x_recv.at[slot(x, z)], cross_dev)

    def x_sideways(step):
        return x_move(2 + 2 * step, slot(x, order[step]), (s, t_flip))

    def x_inside(step):
        return x_move(3 + 2 * step, slot(x, order[step]), (s, t_core))

    def x_back(step):
        return x_move(3 + 2 * step, slot(1 - x, order[step]), (s, t_core))

    def x_outward(step):
        return x_move(8 + step, slot(x, order[step]), at_z(z_near))

    def lead(step):
        if step > 0:
            x_arrived(slot(x, order[step]))
        if step > 1:
            @pl.when(inner)
            def _():
                x_outward(step).start()
        if step > 0:
            x_sideways(step).start()
        x_inside(step).start()

    def follow(step):
        x_arrived(slot(1 - x, order[step]))
        x_back(step).start()

    def other_arrived(step):
        leads = hub if step < 2 else spoke
        x_arrived(slot(jnp.where(leads, 1 - x, x), order[step]))

    def packed(rows):
        return jnp.concatenate([rows[:part], rows[part:]], axis=1)

    def c_copy(i, b):
        return remote(c_buf.at[i, b], r_buf.at[i, b], c_send.at[i, b], c_recv.at[i, b], at_z(z_pair))

    def part_sum(i, b, held_back):
        total = jnp.dot(x_buf[b], w_buf[i, :feat, :], preferred_element_type=jnp.float32)
        total = total + jnp.dot(x_buf[4 + b], w_buf[i, feat:, :], preferred_element_type=jnp.float32)
        low = packed(total[:, :width])
        high = packed(total[:, width:])
        own_buf[i, b] = jnp.where(zh == 0, low, high)
        c_buf[i, b] = jnp.where(zh == 0, high, low).astype(jnp.bfloat16)
        if not held_back:
            c_copy(i, b).start()
        else:
            @pl.when(outer)
            def _():
                c_copy(i, b).start()

    w_over_z(0).start()
    w_over_y(0).start()

    @pl.when(bent)
    def _():
        x_swap().start()

    @pl.when(straight)
    def _():
        x_local().start()

    for i in range(3):
        w_own(i).start()
    wm_here().start()

    def x_first():
        @pl.when(hub)
        def _():
            x_near().start()
            lead(0)
            w_over_z(1).start()

        @pl.when(spoke)
        def _():
            x_cross().start()
            w_over_z(1).start()

    @pl.when(straight)
    def _():
        x_local().wait()
        x_first()

    @pl.loop(0, 4)
    def _(b):
        half = HEAD // 2
        shape = (part, pair)
        lane = lax.broadcasted_iota(jnp.int32, shape, 1)
        place = (b * 2 + y) * tok + lax.broadcasted_iota(jnp.int32, shape, 0)
        place = place + jnp.where(lane < width, 0, part)
        exponent = (lane & (half - 1)).astype(jnp.float32) * (2.0 / HEAD)
        angle = place.astype(jnp.float32) * jnp.exp(exponent * (-math.log(rope_base)))
        cos_buf[b] = jnp.cos(angle)
        sine = jnp.sin(angle)
        sin_buf[b] = jnp.where((lane & (HEAD - 1)) < half, -sine, sine)

    @pl.when(bent)
    def _():
        x_arrived(x_here())
        x_first()

    w_over_z(0).wait_recv()
    w_relay(0).start()
    w_over_y(1).start()

    @pl.when(hub)
    def _():
        x_sideways(0).start()

    @pl.when(spoke)
    def _():
        follow(0)

        @pl.when(inner)
        def _():
            lead(2)

    @pl.when(hub)
    def _():
        lead(1)

    w_wait(0)
    other_arrived(0)
    part_sum(0, order[0], False)

    @pl.when(spoke & inner)
    def _():
        lead(3)

    w_over_z(1).wait_recv()
    w_relay(1).start()
    w_over_y(2).start()
    w_over_z(2).start()

    @pl.when(spoke)
    def _():
        follow(1)

    @pl.when(hub & inner)
    def _():
        follow(2)

    other_arrived(1)
    part_sum(0, order[1], False)

    @pl.when(spoke & outer)
    def _():
        lead(2)

    @pl.when(hub & inner)
    def _():
        follow(3)

    w_wait(1)
    part_sum(1, order[0], True)
    part_sum(1, order[1], True)

    @pl.when(spoke & outer)
    def _():
        lead(3)

    @pl.when(hub & outer)
    def _():
        follow(2)

    w_over_z(2).wait_recv()
    w_relay(2).start()
    other_arrived(2)
    part_sum(0, order[2], False)
    part_sum(1, order[2], True)

    @pl.when(hub & outer)
    def _():
        follow(3)

    other_arrived(3)
    part_sum(0, order[3], False)
    part_sum(1, order[3], True)

    w_over_z(2).wait_send()
    wm_over_z().start()

    @pl.when(inner)
    def _():
        for b in range(2):
            c_copy(1, b).start()

    most = SPAN * DILATIONS[-1]
    kv_buf[0:most, :] = jnp.zeros((most, 2 * width), jnp.bfloat16)

    w_wait(2)

    @pl.loop(0, 4)
    def _(b):
        @pl.when(inner & (b > 0) & (b < 3))
        def _():
            c_copy(1, b + 1).start()

        part_sum(2, b, False)

    def kv_rows(b, which):
        return pl.ds(pl.multiple_of(most + (b * 2 + which) * tok, 128), tok)

    def ky_copy(i, b):
        return remote(ky_out.at[i, b], ky_in.at[i, b], ky_send.at[i, b], ky_recv.at[i, b], y_dev)

    def whole_sum(i, b):
        c_copy(i, b).wait_recv()
        return own_buf[i, b] + r_buf[i, b].astype(jnp.float32)

    def unpacked(both):
        return jnp.concatenate([both[:, :width], both[:, width:]], axis=0)

    def rotate(turn, b):
        half = HEAD // 2
        ahead = jnp.concatenate([turn[:, half:], turn[:, :half]], axis=1)
        behind = jnp.concatenate([turn[:, -half:], turn[:, :-half]], axis=1)
        lane = lax.broadcasted_iota(jnp.int32, turn.shape, 1)
        other = jnp.where((lane & (HEAD - 1)) < half, ahead, behind)
        return (turn * cos_buf[b] + other * sin_buf[b]).astype(jnp.bfloat16)

    theirs = (z_pair, lax.rem(z_near + 2, 4), jnp.where(outer, 3 - z_pair, z), jnp.where(outer, z, 3 - z_pair))

    for step in range(4):
        b = theirs[step]
        turned = rotate(whole_sum(0, b), b)
        ky_out[0, b] = turned
        ky_copy(0, b).start()
        kv_buf[kv_rows(b, y), :width] = unpacked(turned)


    def gather_values(b):
        value = whole_sum(1, b).astype(jnp.bfloat16)
        ky_out[1, b] = value
        ky_copy(1, b).start()
        kv_buf[kv_rows(b, y), width:] = unpacked(value)

    def gather_queries(b):
        rows = pl.ds(pl.multiple_of(b * tok, tok), tok)
        q_buf[rows, :] = unpacked(rotate(whole_sum(2, b), b))

    def keys_arrived(b):
        ky_copy(0, b).wait_recv()
        kv_buf[kv_rows(b, y_far), :width] = unpacked(ky_in[0, b])

    def values_arrived(b):
        ky_copy(1, b).wait_recv()
        kv_buf[kv_rows(b, y_far), width:] = unpacked(ky_in[1, b])

    head = 2 * zl + zh

    def m_copy(b, there):
        where = lax.rem(b + 2 * there, 4)
        return remote(o_buf.at[b], m_buf.at[there, head], m_send.at[there, b],
                      m_recv.at[there, head], at_z(where))

    def m_arrival(there, source):
        return remote(m_buf.at[there, source], m_buf.at[there, source], m_send.at[there, source],
                      m_recv.at[there, source], at_z(z))

    spans = [SPAN * dilation + tok for dilation in DILATIONS]
    places = [sum(spans[:index]) for index in range(HEAD_GROUPS)]

    def near_keys(index, b):
        first = (b * 2 + y) * tok
        return pl.ds(pl.multiple_of(most - SPAN * DILATIONS[index] + first, 128), spans[index])

    def weigh(b):
        rows = pl.ds(pl.multiple_of(b * tok, tok), tok)
        first = (b * 2 + y) * tok
        sum_list = []
        total_list = []
        for index, dilation in enumerate(DILATIONS):
            reach = SPAN * dilation
            keys = spans[index]
            q = q_buf[rows, index * HEAD:(index + 1) * HEAD]
            k = kv_buf[near_keys(index, b), index * HEAD:(index + 1) * HEAD]
            scores = lax.dot_general(
                q, k, (((1,), (1,)), ((), ())), preferred_element_type=jnp.float32
            ) * HEAD ** (-0.5)
            col = lax.broadcasted_iota(jnp.int32, (tok, keys), 1)
            gap = reach + lax.broadcasted_iota(jnp.int32, (tok, keys), 0) - col
            allowed = (gap >= 0) & (gap <= reach) & (col >= reach - first)
            if dilation > 1:
                allowed = allowed & ((gap & (dilation - 1)) == 0)
            scores = jnp.where(allowed, scores, -jnp.inf)
            row_max = jnp.max(scores, axis=1, keepdims=True)
            expo = jnp.exp(scores - row_max)
            denominator = jnp.sum(expo, axis=1, keepdims=True)
            prob_buf[b, :, places[index]:places[index] + keys] = expo.astype(jnp.bfloat16)
            sum_list.append(denominator)
            total_list.append(row_max + jnp.log(denominator))
        peak = jnp.maximum(jnp.maximum(total_list[0], total_list[1]), total_list[2])
        shifted = [jnp.exp(one - peak) for one in total_list]
        whole = shifted[0] + shifted[1] + shifted[2]
        for index in range(HEAD_GROUPS):
            gain_buf[b, index] = shifted[index] / whole / sum_list[index]

    def attend(b):
        merged = jnp.zeros((tok, HEAD), jnp.float32)
        for index in range(HEAD_GROUPS):
            v = kv_buf[near_keys(index, b), width + index * HEAD:width + (index + 1) * HEAD]
            prob = prob_buf[b, :, places[index]:places[index] + spans[index]]
            mixed = jnp.dot(prob, v, preferred_element_type=jnp.float32)
            merged = merged + gain_buf[b, index] * mixed
        merged = packed(merged).astype(jnp.bfloat16)
        o_buf[b] = merged
        for there in range(2):
            mine = lax.rem(b + 2 * there, 4) == z

            @pl.when(jnp.logical_not(mine))
            def _():
                m_copy(b, there).start()

            @pl.when(mine)
            def _():
                m_buf[there, head] = merged

    far = lax.rem(t + 2, 4)
    across = 3 - t
    piece = out.shape[0]
    cols = wm.shape[1]

    def near_copy(n):
        return remote(near_out.at[n], near_in.at[n], near_send.at[n], near_recv.at[n], (s, t_core))

    def far_copy(n):
        return remote(far_out.at[n], far_in.at[n], far_send.at[n], far_recv.at[n], (s, far))

    blocks = (wm_slot, wm_near_slot, zl * 2 + y_far, (1 - zl) * 2 + y_far)

    def product(n):
        there = 1 - n // 4
        block = blocks[n % 4]

        def rows_of(owner):
            picked = merged_buf[there, pl.ds(pl.multiple_of(owner * piece, piece), piece), :]
            return jnp.dot(picked, wm_buf[block], preferred_element_type=jnp.float32)
        near_out[n, 0] = rows_of(across).astype(jnp.bfloat16)
        near_out[n, 1] = rows_of(t_core).astype(jnp.bfloat16)
        near_copy(n).start()
        held[n, 0] = rows_of(far)
        held[n, 1] = rows_of(t)

    def pass_on(n):
        near_copy(n).wait_recv()
        far_out[n] = (held[n, 0] + near_in[n, 0].astype(jnp.float32)).astype(jnp.bfloat16)
        far_copy(n).start()
        held[n, 1] = held[n, 1] + near_in[n, 1].astype(jnp.float32)

    def total_of(n):
        far_copy(n).wait_recv()
        return (held[n, 1] + far_in[n].astype(jnp.float32)).astype(jnp.bfloat16)

    def block_at(half, n):
        return pl.ds(pl.multiple_of((half * 4 + blocks[n]) * cols, 128), cols)

    def done_copy(n):
        return remote(done_out.at[n], out.at[:, block_at(zh, n)], done_send.at[n],
                      done_recv.at[n], at_z(z_pair))

    def collect(group):
        there = 1 - group
        for i in range(1, 4):
            source = lax.rem(z + i, 4)
            m_arrival(there, 2 * lax.rem(source, 2) + lax.div(source, 2)).wait_recv()
        heads = [m_buf[there, h].astype(jnp.float32) for h in range(4)]
        for half in range(2):
            merged_buf[there, half * part:(half + 1) * part] = jnp.concatenate(
                [one[:, half * HEAD:(half + 1) * HEAD] for one in heads], axis=1).astype(jnp.bfloat16)

    def hand_over(n):
        done_out[n] = total_of(n)
        done_copy(n).start()

    def finish_block(b):
        gather_queries(b)
        keys_arrived(b)
        values_arrived(b)
        weigh(b)
        attend(b)

    wm_over_y().start()
    gather_values(0)
    gather_values(1)

    @pl.when(inner)
    def _():
        gather_values(2)
        gather_values(3)

    wm_here().wait()
    wm_came(wm_near_slot)
    wm_relay().start()

    for b in range(2):
        finish_block(b)

        @pl.when(outer)
        def _():
            gather_values(b + 2)

    finish_block(2)
    finish_block(3)
    collect(0)
    for n in range(4):
        if n == 2:
            wm_came(blocks[2])
        if n == 3:
            wm_came(blocks[3])
        product(n)
        if n > 0:
            pass_on(n - 1)
    pass_on(3)
    hand_over(0)
    collect(1)
    for n in range(4, 8):
        product(n)
        if n > 4:
            pass_on(n - 1)
            hand_over(n - 4)
    pass_on(7)
    for n in range(4, 8):
        out[:, block_at(zh, n - 4)] = total_of(n)
    for n in range(4):
        done_copy(n).wait_recv()

    for n in range(8):
        near_copy(n).wait_send()
        far_copy(n).wait_send()
    for n in range(4):
        done_copy(n).wait_send()
    wm_over_z().wait_send()
    wm_over_y().wait_send()
    wm_relay().wait_send()

    @pl.loop(0, 4)
    def _(b):
        for there in range(2):
            @pl.when(lax.rem(b + 2 * there, 4) != z)
            def _():
                m_copy(b, there).wait_send()
        for i in range(2):
            ky_copy(i, b).wait_send()
        for i in range(3):
            c_copy(i, b).wait_send()

    for i in range(3):
        if i < 2:
            w_over_z(i).wait_send()
        w_over_y(i).wait_send()
        w_relay(i).wait_send()

    @pl.when(bent)
    def _():
        x_swap().wait_send()

    @pl.when(hub)
    def _():
        x_near().wait_send()

    @pl.when(spoke)
    def _():
        x_cross().wait_send()

    for step in range(4):
        leads = hub if step < 2 else spoke

        @pl.when(leads)
        def _():
            x_sideways(step).wait_send()
            x_inside(step).wait_send()
            if step > 1:
                @pl.when(inner)
                def _():
                    x_outward(step).wait_send()

        @pl.when(jnp.logical_not(leads))
        def _():
            x_back(step).wait_send()


def halves(activity, wq, wk, wv, wm):
    tok, feat = activity.shape
    krows, col_width = wq.shape
    width = col_width // 4
    rows = 4 * tok
    piece = tok // 4
    cols = wm.shape[1]
    dma = pltpu.SemaphoreType.DMA
    return pl.pallas_call(
        halves_kernel,
        out_shape=jax.ShapeDtypeStruct((piece, 8 * cols), jnp.bfloat16),
        in_specs=[pl.BlockSpec(memory_space=pltpu.HBM)] * 5,
        out_specs=pl.BlockSpec(memory_space=pltpu.VMEM),
        scratch_shapes=[
            pltpu.VMEM((9, tok, feat), jnp.bfloat16),
            pltpu.VMEM((3, 4 * krows, 2 * width), jnp.bfloat16),
            pltpu.VMEM((3, 4, tok // 2, 2 * width), jnp.float32),
            pltpu.VMEM((3, 4, tok // 2, 2 * width), jnp.bfloat16),
            pltpu.VMEM((3, 4, tok // 2, 2 * width), jnp.bfloat16),
            pltpu.VMEM((rows, width), jnp.bfloat16),
            pltpu.VMEM((SPAN * DILATIONS[-1] + 2 * rows, 2 * width), jnp.bfloat16),
            pltpu.VMEM((2, 4, tok // 2, 2 * width), jnp.bfloat16),
            pltpu.VMEM((2, 4, tok // 2, 2 * width), jnp.bfloat16),
            pltpu.VMEM((4, tok // 2, 2 * HEAD), jnp.bfloat16),
            pltpu.VMEM((2, 4, tok // 2, 2 * HEAD), jnp.bfloat16),
            pltpu.VMEM((4, tok // 2, 2 * width), jnp.float32),
            pltpu.VMEM((4, tok // 2, 2 * width), jnp.float32),
            pltpu.VMEM((4, tok, cols), jnp.bfloat16),
            pltpu.VMEM((2, tok, 4 * HEAD), jnp.bfloat16),
            pltpu.VMEM((8, 2, piece, cols), jnp.bfloat16),
            pltpu.VMEM((8, 2, piece, cols), jnp.bfloat16),
            pltpu.VMEM((8, piece, cols), jnp.bfloat16),
            pltpu.VMEM((8, piece, cols), jnp.bfloat16),
            pltpu.VMEM((8, 2, piece, cols), jnp.float32),
            pltpu.VMEM((4, piece, cols), jnp.bfloat16),
            pltpu.VMEM((4, tok, sum(SPAN * one + tok for one in DILATIONS)), jnp.bfloat16),
            pltpu.VMEM((4, HEAD_GROUPS, tok, 1), jnp.float32),
            dma, dma((3,)), dma((12,)), dma((9,)), dma((3, 3)), dma((3, 3)),
            dma((3, 4)), dma((3, 4)), dma((2, 4)), dma((2, 4)), dma((2, 4)), dma((2, 4)),
            dma, dma((3,)), dma((4,)), dma((8,)), dma((8,)), dma((8,)), dma((8,)),
            dma((4,)), dma((4,)),
        ],
        compiler_params=pltpu.CompilerParams(
            collective_id=2, has_side_effects=True, vmem_limit_bytes=66400000),
        cost_estimate=pl.CostEstimate(
            flops=2 * rows * feat * 3 * col_width, bytes_accessed=300 * 2**20, transcendentals=0),
    )(activity, wq, wk, wv, wm)


def per_device(activity, query_weight, key_weight, value_weight, merge_weight):
    G = lax.axis_size("tp")
    R = lax.axis_size("sp") // G
    r = lax.axis_index("sp") % R
    tok = activity.shape[0]
    if G == 4 and R == 2:
        return halves(activity, query_weight, key_weight, value_weight, merge_weight)
    merge_full = lax.all_gather(merge_weight, "sp", axis=1, tiled=True)
    block_start = (jnp.arange(G, dtype=jnp.int32) * R + r) * tok
    pos = (block_start[:, None] + jnp.arange(tok, dtype=jnp.int32)[None, :]).reshape(G * tok)
    half = HEAD // 2
    frequency = rope_base ** (-jnp.arange(0, half, dtype=jnp.float32) * 2.0 / HEAD)
    angles = pos.astype(jnp.float32)[:, None] * frequency[None, :]
    cosine = jnp.tile(jnp.cos(angles), (1, 4))
    sine = jnp.sin(angles)
    sine = jnp.tile(jnp.concatenate([-sine, sine], axis=1), (1, 2))
    merged = project(activity, query_weight, key_weight, value_weight, cosine, sine, G, R)
    return finish(merged, merge_full, 8)


def solution(mesh):
    placed = (P("sp", "tp"), P("sp", "tp"), P("sp", "tp"), P("sp", "tp"), P("tp", "sp"))
    return jax.shard_map(
        per_device, mesh=mesh, in_specs=placed, out_specs=P(("sp", "tp"), None), check_vma=False
    )
```

```python
import functools
import math

import jax
import jax.numpy as jnp
from jax import lax
from jax.experimental import pallas as pl
from jax.experimental.pallas import tpu as pltpu
from jax.sharding import PartitionSpec as P

HEAD = 64
HEAD_GROUPS = 3
SPAN = 128
DILATIONS = (1, 4, 8)
MESH = pl.DeviceIdType.MESH

rope_base = 500000.0


def project_kernel(
    G, R, act, wq, wk, wv, cos_ref, sin_ref, out,
    a_buf, w_buf, c_buf, r_buf, q_buf, kv_buf, o_buf, m_buf,
    local_sem, swap_send, swap_recv, fan_send, fan_recv,
    w_send, w_recv, c_send, c_recv, kv_send, kv_recv, m_send, m_recv,
):
    s = lax.axis_index("sp")
    t = lax.axis_index("tp")
    g = lax.div(s, R)
    r = lax.rem(s, R)
    tok = act.shape[0]
    krows = wq.shape[0]
    width = wq.shape[1] // G
    pairs = G // 2
    weights = (wq, wk, wv)

    swap_dev = (t * R + r, g)
    barrier = pltpu.get_barrier_semaphore()

    def greet(dev):
        pl.semaphore_signal(barrier, inc=1, device_id=dev, device_id_type=MESH)

    for i in range(1, G):
        greet((s, lax.rem(t + i, G)))
        greet((lax.rem(g + i, G) * R + r, t))
    for i in range(1, R):
        greet((g * R + lax.rem(r + i, R), t))

    @pl.when(g != t)
    def _():
        greet(swap_dev)

    pl.semaphore_wait(barrier, 2 * (G - 1) + (R - 1) + jnp.where(g != t, 1, 0))

    def swap_copy():
        return pltpu.make_async_remote_copy(
            src_ref=act, dst_ref=a_buf.at[g], send_sem=swap_send, recv_sem=swap_recv,
            device_id=swap_dev, device_id_type=MESH)

    def swap_local():
        return pltpu.make_async_copy(act, a_buf.at[t], local_sem)

    @pl.when(g != t)
    def _():
        swap_copy().start()

    @pl.when(g == t)
    def _():
        swap_local().start()

    def pair_at(stage):
        return lax.rem(lax.div(g, 2) + 1 + stage, pairs)

    def pair_cols(stage):
        return pl.ds(pl.multiple_of(pair_at(stage) * (2 * width), 128), 2 * width)

    def w_copy(stage, i, x):
        cols = pair_cols(stage)
        return pltpu.make_async_remote_copy(
            src_ref=weights[x].at[:, cols], dst_ref=w_buf.at[i - 1, x, :, cols],
            send_sem=w_send.at[stage, i - 1, x], recv_sem=w_recv.at[stage, i - 1, x],
            device_id=(g * R + lax.rem(r + R - i, R), t), device_id_type=MESH)

    for stage in range(pairs):
        for i in range(1, R):
            for x in range(3):
                w_copy(stage, i, x).start()

    @pl.when(g != t)
    def _():
        swap_copy().wait_recv()

    @pl.when(g == t)
    def _():
        swap_local().wait()

    def fan_copy(i):
        return pltpu.make_async_remote_copy(
            src_ref=a_buf.at[t], dst_ref=a_buf.at[t], send_sem=fan_send.at[i - 1],
            recv_sem=fan_recv.at[i - 1],
            device_id=(s, lax.rem(t + i, G)), device_id_type=MESH)

    def fan_arrival(i):
        slot = lax.rem(t + G - i, G)
        return pltpu.make_async_remote_copy(
            src_ref=a_buf.at[slot], dst_ref=a_buf.at[slot], send_sem=fan_send.at[i - 1],
            recv_sem=fan_recv.at[i - 1],
            device_id=(s, lax.rem(t + i, G)), device_id_type=MESH)

    for i in range(1, G):
        fan_copy(i).start()
    for i in range(1, G):
        fan_arrival(i).wait_recv()

    def c_copy(stage, j, b):
        dest = pair_at(stage) * 2 + j
        rows = pl.ds(pl.multiple_of(b * tok, tok), tok)
        return pltpu.make_async_remote_copy(
            src_ref=c_buf.at[stage, j, rows], dst_ref=r_buf.at[g, rows],
            send_sem=c_send.at[stage, j, b], recv_sem=c_recv.at[g, b],
            device_id=(dest * R + r, t), device_id_type=MESH)

    for stage in range(pairs):
        for i in range(1, R):
            for x in range(3):
                w_copy(stage, i, x).wait_recv()
        cols = pair_cols(stage)

        @pl.loop(0, G)
        def _(b):
            parts = []
            for x in range(3):
                total = jnp.dot(
                    a_buf[b, :, pl.ds(pl.multiple_of(r * krows, 128), krows)],
                    weights[x][:, cols], preferred_element_type=jnp.float32)
                for i in range(1, R):
                    start = pl.multiple_of(lax.rem(r + i, R) * krows, 128)
                    total = total + jnp.dot(
                        a_buf[b, :, pl.ds(start, krows)], w_buf[i - 1, x, :, cols],
                        preferred_element_type=jnp.float32)
                parts.append(total)
            rows = pl.ds(pl.multiple_of(b * tok, tok), tok)
            for j in range(2):
                c_buf[stage, j, rows, :] = jnp.concatenate(
                    [part[:, j * width:(j + 1) * width] for part in parts], axis=1
                ).astype(jnp.bfloat16)
            for j in range(2):
                @pl.when(pair_at(stage) * 2 + j != g)
                def _():
                    c_copy(stage, j, b).start()

    def c_arrival(source, b):
        rows = pl.ds(pl.multiple_of(b * tok, tok), tok)
        return pltpu.make_async_remote_copy(
            src_ref=r_buf.at[source, rows], dst_ref=r_buf.at[source, rows],
            send_sem=c_send.at[0, 0, b], recv_sem=c_recv.at[source, b],
            device_id=(s, t), device_id_type=MESH)

    mine = lax.rem(g, 2)
    most = SPAN * DILATIONS[-1]
    kv_buf[0:most, :] = jnp.zeros((most, 2 * width), jnp.bfloat16)

    def kv_rows(b, part):
        return pl.ds(pl.multiple_of(most + (b * R + part) * tok, 128), tok)

    def kv_copy(i, b):
        rows = kv_rows(b, r)
        return pltpu.make_async_remote_copy(
            src_ref=kv_buf.at[rows], dst_ref=kv_buf.at[rows],
            send_sem=kv_send.at[i - 1, b], recv_sem=kv_recv.at[i - 1, b],
            device_id=(g * R + lax.rem(r + R - i, R), t), device_id_type=MESH)

    def kv_arrival(i, b):
        rows = kv_rows(b, lax.rem(r + i, R))
        return pltpu.make_async_remote_copy(
            src_ref=kv_buf.at[rows], dst_ref=kv_buf.at[rows],
            send_sem=kv_send.at[i - 1, b], recv_sem=kv_recv.at[i - 1, b],
            device_id=(g * R + lax.rem(r + R - i, R), t), device_id_type=MESH)

    def gather_block(b):
        rows = pl.ds(pl.multiple_of(b * tok, tok), tok)
        total = c_buf[pairs - 1, mine, rows, :].astype(jnp.float32)
        for i in range(1, G):
            source = lax.rem(g + i, G)
            c_arrival(source, b).wait_recv()
            total = total + r_buf[source, rows, :].astype(jnp.float32)
        turn = total[:, :2 * width]
        half = HEAD // 2
        ahead = jnp.concatenate([turn[:, half:], turn[:, :half]], axis=1)
        behind = jnp.concatenate([turn[:, -half:], turn[:, :-half]], axis=1)
        lane = lax.broadcasted_iota(jnp.int32, turn.shape, 1)
        other = jnp.where((lane & (HEAD - 1)) < half, ahead, behind)
        reps = 2 * width // cos_ref.shape[1]
        cosine = jnp.concatenate([cos_ref[rows, :]] * reps, axis=1)
        sine = jnp.concatenate([sin_ref[rows, :]] * reps, axis=1)
        turned = turn * cosine + other * sine
        q_buf[rows, :] = turned[:, :width].astype(jnp.bfloat16)
        kv_buf[kv_rows(b, r), :] = jnp.concatenate(
            [turned[:, width:], total[:, 2 * width:]], axis=1).astype(jnp.bfloat16)
        for i in range(1, R):
            kv_copy(i, b).start()

    def m_copy(b):
        return pltpu.make_async_remote_copy(
            src_ref=o_buf.at[b], dst_ref=m_buf.at[g],
            send_sem=m_send.at[b], recv_sem=m_recv.at[g],
            device_id=(b * R + r, t), device_id_type=MESH)

    def m_arrival(source):
        return pltpu.make_async_remote_copy(
            src_ref=m_buf.at[source], dst_ref=m_buf.at[source],
            send_sem=m_send.at[source], recv_sem=m_recv.at[source],
            device_id=(source * R + r, t), device_id_type=MESH)

    def attend(b):
        for i in range(1, R):
            kv_arrival(i, b).wait_recv()
        rows = pl.ds(pl.multiple_of(b * tok, tok), tok)
        first = (b * R + r) * tok
        mixed_list = []
        total_list = []
        for index, dilation in enumerate(DILATIONS):
            reach = SPAN * dilation
            keys = reach + tok
            near = pl.ds(pl.multiple_of(most - reach + first, 128), keys)
            q = q_buf[rows, index * HEAD:(index + 1) * HEAD]
            k = kv_buf[near, index * HEAD:(index + 1) * HEAD]
            v = kv_buf[near, width + index * HEAD:width + (index + 1) * HEAD]
            scores = lax.dot_general(
                q, k, (((1,), (1,)), ((), ())), preferred_element_type=jnp.float32
            ) * HEAD ** (-0.5)
            col = lax.broadcasted_iota(jnp.int32, (tok, keys), 1)
            gap = reach + lax.broadcasted_iota(jnp.int32, (tok, keys), 0) - col
            allowed = (gap >= 0) & (gap <= reach) & (col >= reach - first)
            if dilation > 1:
                allowed = allowed & ((gap & (dilation - 1)) == 0)
            scores = jnp.where(allowed, scores, -jnp.inf)
            row_max = jnp.max(scores, axis=1, keepdims=True)
            expo = jnp.exp(scores - row_max)
            denominator = jnp.sum(expo, axis=1, keepdims=True)
            mixed = jnp.dot(expo.astype(jnp.bfloat16), v, preferred_element_type=jnp.float32)
            mixed_list.append(mixed / denominator)
            total_list.append(row_max + jnp.log(denominator))
        peak = jnp.maximum(jnp.maximum(total_list[0], total_list[1]), total_list[2])
        shifted = [jnp.exp(one - peak) for one in total_list]
        whole = shifted[0] + shifted[1] + shifted[2]
        merged = sum(a / whole * b_ for a, b_ in zip(shifted, mixed_list)).astype(jnp.bfloat16)

        @pl.when(b != g)
        def _():
            o_buf[b] = merged
            m_copy(b).start()

        @pl.when(b == g)
        def _():
            m_buf[b] = merged

    gather_block(0)

    @pl.loop(1, G)
    def _(b):
        gather_block(b)
        attend(b - 1)

    attend(G - 1)

    for i in range(1, G):
        m_arrival(lax.rem(g + i, G)).wait_recv()
    out[...] = jnp.concatenate(
        [m_buf[h].astype(jnp.float32) for h in range(G)], axis=1).astype(jnp.bfloat16)

    for i in range(1, G):
        m_copy(lax.rem(g + i, G)).wait_send()

    @pl.loop(0, G)
    def _(b):
        for i in range(1, R):
            kv_copy(i, b).wait_send()

    @pl.when(g != t)
    def _():
        swap_copy().wait_send()

    for i in range(1, G):
        fan_copy(i).wait_send()
    for stage in range(pairs):
        for i in range(1, R):
            for x in range(3):
                w_copy(stage, i, x).wait_send()
        for j in range(2):
            @pl.when(pair_at(stage) * 2 + j != g)
            def _():
                @pl.loop(0, G)
                def _(b):
                    c_copy(stage, j, b).wait_send()


def project(activity, wq, wk, wv, cosine, sine, G, R):
    tok, feat = activity.shape
    krows, col_width = wq.shape
    width = 3 * (col_width // G)
    pairs = G // 2
    rows = G * tok
    dma = pltpu.SemaphoreType.DMA
    return pl.pallas_call(
        functools.partial(project_kernel, G, R),
        out_shape=jax.ShapeDtypeStruct((tok, G * HEAD), jnp.bfloat16),
        in_specs=[pl.BlockSpec(memory_space=pltpu.VMEM)] * 6,
        out_specs=pl.BlockSpec(memory_space=pltpu.VMEM),
        scratch_shapes=[
            pltpu.VMEM((G, tok, feat), jnp.bfloat16),
            pltpu.VMEM((R - 1, 3, krows, col_width), jnp.bfloat16),
            pltpu.VMEM((pairs, 2, rows, width), jnp.bfloat16),
            pltpu.VMEM((G, rows, width), jnp.bfloat16),
            pltpu.VMEM((rows, width // 3), jnp.bfloat16),
            pltpu.VMEM((SPAN * DILATIONS[-1] + R * rows, 2 * (width // 3)), jnp.bfloat16),
            pltpu.VMEM((G, tok, HEAD), jnp.bfloat16),
            pltpu.VMEM((G, tok, HEAD), jnp.bfloat16),
            dma, dma, dma, dma((G - 1,)), dma((G - 1,)),
            dma((pairs, R - 1, 3)), dma((pairs, R - 1, 3)),
            dma((pairs, 2, G)), dma((G, G)),
            dma((R - 1, G)), dma((R - 1, G)), dma((G,)), dma((G,)),
        ],
        compiler_params=pltpu.CompilerParams(
            collective_id=0, has_side_effects=True, vmem_limit_bytes=58 * 2**20),
        cost_estimate=pl.CostEstimate(
            flops=2 * rows * feat * 3 * col_width, bytes_accessed=300 * 2**20, transcendentals=0),
    )(activity, wq, wk, wv, cosine, sine)


def finish_kernel(merged, weight, out, near_out, near_in, far_out, far_in, held,
                  near_send, near_recv, far_send, far_recv):
    s = lax.axis_index("sp")
    t = lax.axis_index("tp")
    chunks = near_out.shape[0]
    rows = out.shape[0]
    cols = weight.shape[1] // chunks
    low = lax.rem(t, 2)
    near = t + 1 - 2 * low
    far = lax.rem(t + 2, 4)
    across = lax.rem(near + 2, 4)

    barrier = pltpu.get_barrier_semaphore()
    for peer in (near, far):
        pl.semaphore_signal(barrier, inc=1, device_id=(s, peer), device_id_type=MESH)
    pl.semaphore_wait(barrier, 2)

    def near_copy(c):
        return pltpu.make_async_remote_copy(
            src_ref=near_out.at[c], dst_ref=near_in.at[c], send_sem=near_send.at[c],
            recv_sem=near_recv.at[c], device_id=(s, near), device_id_type=MESH)

    def far_copy(c):
        return pltpu.make_async_remote_copy(
            src_ref=far_out.at[c], dst_ref=far_in.at[c], send_sem=far_send.at[c],
            recv_sem=far_recv.at[c], device_id=(s, far), device_id_type=MESH)

    def part(owner, at):
        picked = merged[pl.ds(pl.multiple_of(owner * rows, rows), rows), :]
        return jnp.dot(picked, weight[:, at], preferred_element_type=jnp.float32)

    @pl.loop(0, chunks)
    def _(c):
        at = pl.ds(pl.multiple_of(c * cols, 128), cols)
        near_out[c, 0] = part(across, at).astype(jnp.bfloat16)
        near_out[c, 1] = part(near, at).astype(jnp.bfloat16)
        near_copy(c).start()
        held[c, 0] = part(far, at)
        held[c, 1] = part(t, at)

    @pl.loop(0, chunks)
    def _(c):
        near_copy(c).wait_recv()
        far_out[c] = (held[c, 0] + near_in[c, 0].astype(jnp.float32)).astype(jnp.bfloat16)
        far_copy(c).start()
        held[c, 1] = held[c, 1] + near_in[c, 1].astype(jnp.float32)

    @pl.loop(0, chunks)
    def _(c):
        at = pl.ds(pl.multiple_of(c * cols, 128), cols)
        far_copy(c).wait_recv()
        out[:, at] = (held[c, 1] + far_in[c].astype(jnp.float32)).astype(jnp.bfloat16)

    @pl.loop(0, chunks)
    def _(c):
        near_copy(c).wait_send()
        far_copy(c).wait_send()


def finish(merged, weight, chunks):
    rows = merged.shape[0] // 4
    cols = weight.shape[1] // chunks
    dma = pltpu.SemaphoreType.DMA
    return pl.pallas_call(
        finish_kernel,
        out_shape=jax.ShapeDtypeStruct((rows, weight.shape[1]), jnp.bfloat16),
        in_specs=[pl.BlockSpec(memory_space=pltpu.VMEM)] * 2,
        out_specs=pl.BlockSpec(memory_space=pltpu.VMEM),
        scratch_shapes=[
            pltpu.VMEM((chunks, 2, rows, cols), jnp.bfloat16),
            pltpu.VMEM((chunks, 2, rows, cols), jnp.bfloat16),
            pltpu.VMEM((chunks, rows, cols), jnp.bfloat16),
            pltpu.VMEM((chunks, rows, cols), jnp.bfloat16),
            pltpu.VMEM((chunks, 2, rows, cols), jnp.float32),
            dma((chunks,)), dma((chunks,)), dma((chunks,)), dma((chunks,)),
        ],
        compiler_params=pltpu.CompilerParams(
            collective_id=1, has_side_effects=True, vmem_limit_bytes=40 * 2**20),
    )(merged, weight)


def halves_kernel(
    act, wq, wk, wv, wm, out_hbm,
    x_buf, w_buf, own_buf, c_buf, r_buf, q_buf, kv_buf, ky_out, ky_in, o_buf, m_buf,
    cos_buf, sin_buf, wm_buf, merged_buf, near_out, near_in, far_out, far_in, held,
    done_out, prob_buf, gain_buf, out,
    local_sem, w_local, x_send, x_recv, w_send, w_recv, c_send, c_recv,
    ky_send, ky_recv, m_send, m_recv, wm_local, wm_send, wm_recv,
    near_send, near_recv, far_send, far_recv, done_send, done_recv, out_sem,
):
    s = lax.axis_index("sp")
    t = lax.axis_index("tp")
    z = lax.div(s, 2)
    y = lax.rem(s, 2)
    x = lax.div(t, 2)
    c = lax.rem(t, 2)
    zh = lax.div(z, 2)
    zl = lax.rem(z, 2)
    tok, feat = act.shape
    krows = wq.shape[0]
    pair = wq.shape[1] // 2
    width = pair // 2
    part = tok // 2
    weights = (wk, wv, wq)
    z_near = z + 1 - 2 * zl
    z_pair = lax.rem(z + 2, 4)
    y_far = 1 - y
    y_dev = (z * 2 + y_far, t)
    t_flip = 3 - t
    t_core = t + 1 - 2 * c
    hub = c == zh
    spoke = jnp.logical_not(hub)
    inner = zl != zh
    outer = jnp.logical_not(inner)
    straight = c == x
    bent = jnp.logical_not(straight)

    def at_z(other):
        return (other * 2 + y, t)

    barrier = pltpu.get_barrier_semaphore()

    def greet(dev):
        pl.semaphore_signal(barrier, inc=1, device_id=dev, device_id_type=MESH)

    for i in range(1, 4):
        greet(at_z(lax.rem(z + i, 4)))
        greet((s, lax.rem(t + i, 4)))
    greet(y_dev)
    cross_z = jnp.where(c == 0, 1, 2)
    cross_dev = (cross_z * 2 + y, t_core)

    for i in range(1, 4):
        greet((lax.rem(z + i, 4) * 2 + y, t_core))
    pl.semaphore_wait(barrier, 10)

    def remote(src, dst, send, recv, dev):
        return pltpu.make_async_remote_copy(
            src_ref=src, dst_ref=dst, send_sem=send, recv_sem=recv,
            device_id=dev, device_id_type=MESH)

    def own_rows(block):
        return pl.ds(pl.multiple_of(block * krows, 128), krows)

    def pair_cols(p):
        return pl.ds(pl.multiple_of(p * pair, 128), pair)

    mine_rows = own_rows(zl * 2 + y)

    def w_own(i):
        return pltpu.make_async_copy(
            weights[i].at[:, pair_cols(zl)], w_buf.at[i, mine_rows], w_local.at[i])

    small = krows // 2

    def piece_rows(block, p):
        return pl.ds(pl.multiple_of(block * krows + p * small, 128), small)

    def w_over_z(i, p):
        return remote(weights[i].at[p * small:(p + 1) * small, pair_cols(1 - zl)],
                      w_buf.at[i, piece_rows(zl * 2 + y, p)],
                      w_send.at[p, i], w_recv.at[p, i], at_z(z_near))

    def w_over_y(i):
        return remote(weights[i].at[:, pair_cols(zl)], w_buf.at[i, mine_rows],
                      w_send.at[4, i], w_recv.at[4, i], y_dev)

    def w_relay(i, p):
        rows = piece_rows((1 - zl) * 2 + y, p)
        return remote(w_buf.at[i, rows], w_buf.at[i, rows],
                      w_send.at[2 + p, i], w_recv.at[2 + p, i], y_dev)

    def w_push(i):
        for p in range(2):
            w_over_z(i, p).start()

    def w_hand_on(i):
        for p in range(2):
            w_over_z(i, p).wait_recv()
            w_relay(i, p).start()

    def w_wait(i):
        w_own(i).wait()
        w_over_y(i).wait_recv()
        w_relay(i, 0).wait_recv()
        w_relay(i, 1).wait_recv()

    wm_slot = zl * 2 + y
    wm_near_slot = (1 - zl) * 2 + y

    def wm_here():
        return pltpu.make_async_copy(wm, wm_buf.at[wm_slot], wm_local)

    def wm_over_z():
        return remote(wm, wm_buf.at[wm_slot], wm_send.at[0], wm_recv.at[wm_slot], at_z(z_near))

    def wm_over_y():
        return remote(wm, wm_buf.at[wm_slot], wm_send.at[1], wm_recv.at[wm_slot], y_dev)

    def wm_relay():
        return remote(wm_buf.at[wm_near_slot], wm_buf.at[wm_near_slot],
                      wm_send.at[2], wm_recv.at[wm_near_slot], y_dev)

    def wm_came(block):
        remote(wm_buf.at[block], wm_buf.at[block], wm_send.at[0], wm_recv.at[block], y_dev).wait_recv()

    hold = 8
    order = (z, z_near, jnp.where(inner, 3 - z, z_pair), jnp.where(inner, z_pair, 3 - z))

    def slot(quarter, block):
        return quarter * 4 + block

    def x_swap():
        there = jnp.where(1 - c == zh, slot(1 - x, z), hold)
        return remote(act, x_buf.at[there], x_send.at[0], x_recv.at[there], (s, t_flip))

    def x_here():
        return jnp.where(hub, slot(x, z), hold)

    def x_local():
        return pltpu.make_async_copy(act, x_buf.at[x_here()], local_sem)

    def x_move(index, block, dev):
        return remote(x_buf.at[block], x_buf.at[block], x_send.at[index], x_recv.at[block], dev)

    def x_arrived(block):
        remote(x_buf.at[block], x_buf.at[block], x_send.at[0], x_recv.at[block], (s, t)).wait_recv()

    def x_near():
        return x_move(1, slot(x, z), at_z(z_near))

    def x_cross():
        return remote(x_buf.at[hold], x_buf.at[slot(x, z)], x_send.at[1],
                      x_recv.at[slot(x, z)], cross_dev)

    def x_sideways(step):
        return x_move(2 + 2 * step, slot(x, order[step]), (s, t_flip))

    def x_inside(step):
        return x_move(3 + 2 * step, slot(x, order[step]), (s, t_core))

    def x_back(step):
        return x_move(3 + 2 * step, slot(1 - x, order[step]), (s, t_core))

    def x_outward(step):
        return x_move(8 + step, slot(x, order[step]), at_z(z_near))

    def lead(step):
        if step > 0:
            x_arrived(slot(x, order[step]))
        if step > 1:
            @pl.when(inner)
            def _():
                x_outward(step).start()
        if step > 0:
            x_sideways(step).start()
        x_inside(step).start()

    def follow(step):
        x_arrived(slot(1 - x, order[step]))
        x_back(step).start()

    def other_arrived(step):
        leads = hub if step < 2 else spoke
        x_arrived(slot(jnp.where(leads, 1 - x, x), order[step]))

    def packed(rows):
        return jnp.concatenate([rows[:part], rows[part:]], axis=1)

    def c_copy(i, b):
        return remote(c_buf.at[i, b], r_buf.at[i, b], c_send.at[i, b], c_recv.at[i, b], at_z(z_pair))

    def part_sum(i, b, held_back):
        total = jnp.dot(x_buf[b], w_buf[i, :feat, :], preferred_element_type=jnp.float32)
        total = total + jnp.dot(x_buf[4 + b], w_buf[i, feat:, :], preferred_element_type=jnp.float32)
        low = packed(total[:, :width])
        high = packed(total[:, width:])
        own_buf[i, b] = jnp.where(zh == 0, low, high)
        c_buf[i, b] = jnp.where(zh == 0, high, low).astype(jnp.bfloat16)
        if not held_back:
            c_copy(i, b).start()
        else:
            @pl.when(outer)
            def _():
                c_copy(i, b).start()

    w_push(0)
    w_over_y(0).start()

    @pl.when(bent)
    def _():
        x_swap().start()

    @pl.when(straight)
    def _():
        x_local().start()

    for i in range(3):
        w_own(i).start()
    wm_here().start()

    def x_first():
        @pl.when(hub)
        def _():
            x_near().start()
            lead(0)
            w_push(1)

        @pl.when(spoke)
        def _():
            x_cross().start()
            w_push(1)

    @pl.when(straight)
    def _():
        x_local().wait()
        x_first()

    @pl.loop(0, 4)
    def _(b):
        half = HEAD // 2
        shape = (part, pair)
        lane = lax.broadcasted_iota(jnp.int32, shape, 1)
        place = (b * 2 + y) * tok + lax.broadcasted_iota(jnp.int32, shape, 0)
        place = place + jnp.where(lane < width, 0, part)
        exponent = (lane & (half - 1)).astype(jnp.float32) * (2.0 / HEAD)
        angle = place.astype(jnp.float32) * jnp.exp(exponent * (-math.log(rope_base)))
        cos_buf[b] = jnp.cos(angle)
        sine = jnp.sin(angle)
        sin_buf[b] = jnp.where((lane & (HEAD - 1)) < half, -sine, sine)

    @pl.when(bent)
    def _():
        x_arrived(x_here())
        x_first()

    w_hand_on(0)
    w_over_y(1).start()

    @pl.when(hub)
    def _():
        x_sideways(0).start()

    @pl.when(spoke)
    def _():
        follow(0)

        @pl.when(inner)
        def _():
            lead(2)

    @pl.when(hub)
    def _():
        lead(1)

    w_wait(0)
    other_arrived(0)
    part_sum(0, order[0], False)

    @pl.when(spoke & inner)
    def _():
        lead(3)

    w_hand_on(1)
    w_over_y(2).start()
    w_push(2)

    @pl.when(spoke)
    def _():
        follow(1)

    @pl.when(hub & inner)
    def _():
        follow(2)

    other_arrived(1)
    part_sum(0, order[1], False)

    @pl.when(spoke & outer)
    def _():
        lead(2)

    @pl.when(hub & inner)
    def _():
        follow(3)

    w_wait(1)
    part_sum(1, order[0], True)
    part_sum(1, order[1], True)

    @pl.when(spoke & outer)
    def _():
        lead(3)

    @pl.when(hub & outer)
    def _():
        follow(2)

    w_hand_on(2)
    other_arrived(2)
    part_sum(0, order[2], False)
    part_sum(1, order[2], True)

    @pl.when(hub & outer)
    def _():
        follow(3)

    other_arrived(3)
    part_sum(0, order[3], False)
    part_sum(1, order[3], True)

    for p in range(2):
        w_over_z(2, p).wait_send()
    wm_over_z().start()

    @pl.when(inner)
    def _():
        for b in range(2):
            c_copy(1, b).start()

    most = SPAN * DILATIONS[-1]
    kv_buf[0:most, :] = jnp.zeros((most, 2 * width), jnp.bfloat16)

    w_wait(2)

    @pl.loop(0, 4)
    def _(n):
        @pl.when(inner & (n > 0) & (n < 3))
        def _():
            c_copy(1, n + 1).start()

        part_sum(2, jnp.where(n == 3, 3, lax.rem(2 * n, 3)), False)

    def kv_rows(b, which):
        return pl.ds(pl.multiple_of(most + (b * 2 + which) * tok, 128), tok)

    def ky_copy(i, b):
        return remote(ky_out.at[i, b], ky_in.at[i, b], ky_send.at[i, b], ky_recv.at[i, b], y_dev)

    def whole_sum(i, b):
        c_copy(i, b).wait_recv()
        return own_buf[i, b] + r_buf[i, b].astype(jnp.float32)

    def unpacked(both):
        return jnp.concatenate([both[:, :width], both[:, width:]], axis=0)

    def rotate(turn, b):
        half = HEAD // 2
        ahead = jnp.concatenate([turn[:, half:], turn[:, :half]], axis=1)
        behind = jnp.concatenate([turn[:, -half:], turn[:, :-half]], axis=1)
        lane = lax.broadcasted_iota(jnp.int32, turn.shape, 1)
        other = jnp.where((lane & (HEAD - 1)) < half, ahead, behind)
        return (turn * cos_buf[b] + other * sin_buf[b]).astype(jnp.bfloat16)

    theirs = (z_pair, lax.rem(z_near + 2, 4), jnp.where(outer, 3 - z_pair, z), jnp.where(outer, z, 3 - z_pair))

    for step in range(4):
        b = theirs[step]
        turned = rotate(whole_sum(0, b), b)
        ky_out[0, b] = turned
        ky_copy(0, b).start()
        kv_buf[kv_rows(b, y), :width] = unpacked(turned)


    def gather_values(b):
        value = whole_sum(1, b).astype(jnp.bfloat16)
        ky_out[1, b] = value
        ky_copy(1, b).start()
        kv_buf[kv_rows(b, y), width:] = unpacked(value)

    def gather_queries(b):
        rows = pl.ds(pl.multiple_of(b * tok, tok), tok)
        q_buf[rows, :] = unpacked(rotate(whole_sum(2, b), b))

    def keys_arrived(b):
        ky_copy(0, b).wait_recv()
        kv_buf[kv_rows(b, y_far), :width] = unpacked(ky_in[0, b])

    def values_arrived(b):
        ky_copy(1, b).wait_recv()
        kv_buf[kv_rows(b, y_far), width:] = unpacked(ky_in[1, b])

    head = 2 * zl + zh

    def m_copy(b, there):
        where = lax.rem(b + 2 * there, 4)
        return remote(o_buf.at[b], m_buf.at[there, head], m_send.at[there, b],
                      m_recv.at[there, head], at_z(where))

    def m_arrival(there, source):
        return remote(m_buf.at[there, source], m_buf.at[there, source], m_send.at[there, source],
                      m_recv.at[there, source], at_z(z))

    spans = [SPAN * dilation + tok for dilation in DILATIONS]
    places = [sum(spans[:index]) for index in range(HEAD_GROUPS)]

    def near_keys(index, b):
        first = (b * 2 + y) * tok
        return pl.ds(pl.multiple_of(most - SPAN * DILATIONS[index] + first, 128), spans[index])

    def weigh(b):
        rows = pl.ds(pl.multiple_of(b * tok, tok), tok)
        first = (b * 2 + y) * tok
        sum_list = []
        total_list = []
        for index, dilation in enumerate(DILATIONS):
            reach = SPAN * dilation
            keys = spans[index]
            q = q_buf[rows, index * HEAD:(index + 1) * HEAD]
            k = kv_buf[near_keys(index, b), index * HEAD:(index + 1) * HEAD]
            scores = lax.dot_general(
                q, k, (((1,), (1,)), ((), ())), preferred_element_type=jnp.float32
            ) * HEAD ** (-0.5)
            col = lax.broadcasted_iota(jnp.int32, (tok, keys), 1)
            gap = reach + lax.broadcasted_iota(jnp.int32, (tok, keys), 0) - col
            allowed = (gap >= 0) & (gap <= reach) & (col >= reach - first)
            if dilation > 1:
                allowed = allowed & ((gap & (dilation - 1)) == 0)
            scores = jnp.where(allowed, scores, -jnp.inf)
            row_max = jnp.max(scores, axis=1, keepdims=True)
            expo = jnp.exp(scores - row_max)
            denominator = jnp.sum(expo, axis=1, keepdims=True)
            prob_buf[b, :, places[index]:places[index] + keys] = expo.astype(jnp.bfloat16)
            sum_list.append(denominator)
            total_list.append(row_max + jnp.log(denominator))
        peak = jnp.maximum(jnp.maximum(total_list[0], total_list[1]), total_list[2])
        shifted = [jnp.exp(one - peak) for one in total_list]
        whole = shifted[0] + shifted[1] + shifted[2]
        for index in range(HEAD_GROUPS):
            gain_buf[b, index] = shifted[index] / whole / sum_list[index]

    def attend(b):
        merged = jnp.zeros((tok, HEAD), jnp.float32)
        for index in range(HEAD_GROUPS):
            v = kv_buf[near_keys(index, b), width + index * HEAD:width + (index + 1) * HEAD]
            prob = prob_buf[b, :, places[index]:places[index] + spans[index]]
            mixed = jnp.dot(prob, v, preferred_element_type=jnp.float32)
            merged = merged + gain_buf[b, index] * mixed
        merged = packed(merged).astype(jnp.bfloat16)
        o_buf[b] = merged
        for there in range(2):
            mine = lax.rem(b + 2 * there, 4) == z

            @pl.when(jnp.logical_not(mine))
            def _():
                m_copy(b, there).start()

            @pl.when(mine)
            def _():
                m_buf[there, head] = merged

    far = lax.rem(t + 2, 4)
    across = 3 - t
    piece = out.shape[0]
    cols = wm.shape[1]

    def near_copy(n):
        return remote(near_out.at[n], near_in.at[n], near_send.at[n], near_recv.at[n], (s, t_core))

    def far_copy(n):
        return remote(far_out.at[n], far_in.at[n], far_send.at[n], far_recv.at[n], (s, far))

    blocks = (wm_slot, wm_near_slot, zl * 2 + y_far, (1 - zl) * 2 + y_far)

    def product(n):
        there = 1 - n // 4
        block = blocks[n % 4]

        def rows_of(owner):
            picked = merged_buf[there, pl.ds(pl.multiple_of(owner * piece, piece), piece), :]
            return jnp.dot(picked, wm_buf[block], preferred_element_type=jnp.float32)
        near_out[n, 0] = rows_of(across).astype(jnp.bfloat16)
        near_out[n, 1] = rows_of(t_core).astype(jnp.bfloat16)
        near_copy(n).start()
        held[n, 0] = rows_of(far)
        held[n, 1] = rows_of(t)

    def pass_on(n):
        near_copy(n).wait_recv()
        far_out[n] = (held[n, 0] + near_in[n, 0].astype(jnp.float32)).astype(jnp.bfloat16)
        far_copy(n).start()
        held[n, 1] = held[n, 1] + near_in[n, 1].astype(jnp.float32)

    def total_of(n):
        far_copy(n).wait_recv()
        return (held[n, 1] + far_in[n].astype(jnp.float32)).astype(jnp.bfloat16)

    def block_at(half, n):
        return pl.ds(pl.multiple_of((half * 4 + blocks[n]) * cols, 128), cols)

    def out_copy(half, n):
        at = block_at(half, n)
        return pltpu.make_async_copy(out.at[:, at], out_hbm.at[:, at], out_sem.at[half, n])

    def done_copy(n):
        return remote(done_out.at[n], out.at[:, block_at(zh, n)], done_send.at[n],
                      done_recv.at[n], at_z(z_pair))

    def collect(group):
        there = 1 - group
        for i in range(1, 4):
            source = lax.rem(z + i, 4)
            m_arrival(there, 2 * lax.rem(source, 2) + lax.div(source, 2)).wait_recv()
        heads = [m_buf[there, h].astype(jnp.float32) for h in range(4)]
        for half in range(2):
            merged_buf[there, half * part:(half + 1) * part] = jnp.concatenate(
                [one[:, half * HEAD:(half + 1) * HEAD] for one in heads], axis=1).astype(jnp.bfloat16)

    def hand_over(n):
        total = total_of(n)
        if n < 4:
            done_out[n] = total
            done_copy(n).start()
        else:
            out[:, block_at(zh, n - 4)] = total
            out_copy(zh, n - 4).start()

    def finish_block(b, fresh):
        gather_queries(b)
        for one in fresh:
            keys_arrived(one)
            values_arrived(one)
        weigh(b)
        attend(b)

    wm_over_y().start()
    gather_values(0)
    gather_values(1)

    @pl.when(inner)
    def _():
        gather_values(2)
        gather_values(3)

    wm_here().wait()
    wm_came(wm_near_slot)
    wm_relay().start()

    finish_block(0, (0,))

    @pl.when(outer)
    def _():
        gather_values(2)

    finish_block(2, (1, 2))

    @pl.when(outer)
    def _():
        gather_values(3)

    finish_block(1, ())
    finish_block(3, (3,))
    collect(0)
    for n in range(4):
        if n == 2:
            wm_came(blocks[2])
        if n == 3:
            wm_came(blocks[3])
        product(n)
        if n > 0:
            pass_on(n - 1)
    pass_on(3)
    hand_over(0)
    collect(1)
    for n in range(4, 8):
        product(n)
        if n > 4:
            pass_on(n - 1)
            hand_over(n - 4)
    pass_on(7)
    for n in range(4, 8):
        hand_over(n)
    for n in range(4):
        done_copy(n).wait_recv()
        out_copy(1 - zh, n).start()
    for n in range(4):
        out_copy(zh, n).wait()
        out_copy(1 - zh, n).wait()

    for n in range(8):
        near_copy(n).wait_send()
        far_copy(n).wait_send()
    for n in range(4):
        done_copy(n).wait_send()
    wm_over_z().wait_send()
    wm_over_y().wait_send()
    wm_relay().wait_send()

    @pl.loop(0, 4)
    def _(b):
        for there in range(2):
            @pl.when(lax.rem(b + 2 * there, 4) != z)
            def _():
                m_copy(b, there).wait_send()
        for i in range(2):
            ky_copy(i, b).wait_send()
        for i in range(3):
            c_copy(i, b).wait_send()

    for i in range(3):
        for p in range(2):
            if i < 2:
                w_over_z(i, p).wait_send()
            w_relay(i, p).wait_send()
        w_over_y(i).wait_send()

    @pl.when(bent)
    def _():
        x_swap().wait_send()

    @pl.when(hub)
    def _():
        x_near().wait_send()

    @pl.when(spoke)
    def _():
        x_cross().wait_send()

    for step in range(4):
        leads = hub if step < 2 else spoke

        @pl.when(leads)
        def _():
            x_sideways(step).wait_send()
            x_inside(step).wait_send()
            if step > 1:
                @pl.when(inner)
                def _():
                    x_outward(step).wait_send()

        @pl.when(jnp.logical_not(leads))
        def _():
            x_back(step).wait_send()


def halves(activity, wq, wk, wv, wm):
    tok, feat = activity.shape
    krows, col_width = wq.shape
    width = col_width // 4
    rows = 4 * tok
    piece = tok // 4
    cols = wm.shape[1]
    dma = pltpu.SemaphoreType.DMA
    return pl.pallas_call(
        halves_kernel,
        out_shape=jax.ShapeDtypeStruct((piece, 8 * cols), jnp.bfloat16),
        in_specs=[pl.BlockSpec(memory_space=pltpu.HBM)] * 5,
        out_specs=pl.BlockSpec(memory_space=pltpu.HBM),
        scratch_shapes=[
            pltpu.VMEM((9, tok, feat), jnp.bfloat16),
            pltpu.VMEM((3, 4 * krows, 2 * width), jnp.bfloat16),
            pltpu.VMEM((3, 4, tok // 2, 2 * width), jnp.float32),
            pltpu.VMEM((3, 4, tok // 2, 2 * width), jnp.bfloat16),
            pltpu.VMEM((3, 4, tok // 2, 2 * width), jnp.bfloat16),
            pltpu.VMEM((rows, width), jnp.bfloat16),
            pltpu.VMEM((SPAN * DILATIONS[-1] + 2 * rows, 2 * width), jnp.bfloat16),
            pltpu.VMEM((2, 4, tok // 2, 2 * width), jnp.bfloat16),
            pltpu.VMEM((2, 4, tok // 2, 2 * width), jnp.bfloat16),
            pltpu.VMEM((4, tok // 2, 2 * HEAD), jnp.bfloat16),
            pltpu.VMEM((2, 4, tok // 2, 2 * HEAD), jnp.bfloat16),
            pltpu.VMEM((4, tok // 2, 2 * width), jnp.float32),
            pltpu.VMEM((4, tok // 2, 2 * width), jnp.float32),
            pltpu.VMEM((4, tok, cols), jnp.bfloat16),
            pltpu.VMEM((2, tok, 4 * HEAD), jnp.bfloat16),
            pltpu.VMEM((8, 2, piece, cols), jnp.bfloat16),
            pltpu.VMEM((8, 2, piece, cols), jnp.bfloat16),
            pltpu.VMEM((8, piece, cols), jnp.bfloat16),
            pltpu.VMEM((8, piece, cols), jnp.bfloat16),
            pltpu.VMEM((8, 2, piece, cols), jnp.float32),
            pltpu.VMEM((4, piece, cols), jnp.bfloat16),
            pltpu.VMEM((4, tok, sum(SPAN * one + tok for one in DILATIONS)), jnp.bfloat16),
            pltpu.VMEM((4, HEAD_GROUPS, tok, 1), jnp.float32),
            pltpu.VMEM((piece, 8 * cols), jnp.bfloat16),
            dma, dma((3,)), dma((12,)), dma((9,)), dma((5, 3)), dma((5, 3)),
            dma((3, 4)), dma((3, 4)), dma((2, 4)), dma((2, 4)), dma((2, 4)), dma((2, 4)),
            dma, dma((3,)), dma((4,)), dma((8,)), dma((8,)), dma((8,)), dma((8,)),
            dma((4,)), dma((4,)), dma((2, 4)),
        ],
        compiler_params=pltpu.CompilerParams(
            collective_id=2, has_side_effects=True, vmem_limit_bytes=66400000),
        cost_estimate=pl.CostEstimate(
            flops=2 * rows * feat * 3 * col_width, bytes_accessed=300 * 2**20, transcendentals=0),
    )(activity, wq, wk, wv, wm)


def per_device(activity, query_weight, key_weight, value_weight, merge_weight):
    G = lax.axis_size("tp")
    R = lax.axis_size("sp") // G
    r = lax.axis_index("sp") % R
    tok = activity.shape[0]
    if G == 4 and R == 2:
        return halves(activity, query_weight, key_weight, value_weight, merge_weight)
    merge_full = lax.all_gather(merge_weight, "sp", axis=1, tiled=True)
    block_start = (jnp.arange(G, dtype=jnp.int32) * R + r) * tok
    pos = (block_start[:, None] + jnp.arange(tok, dtype=jnp.int32)[None, :]).reshape(G * tok)
    half = HEAD // 2
    frequency = rope_base ** (-jnp.arange(0, half, dtype=jnp.float32) * 2.0 / HEAD)
    angles = pos.astype(jnp.float32)[:, None] * frequency[None, :]
    cosine = jnp.tile(jnp.cos(angles), (1, 4))
    sine = jnp.sin(angles)
    sine = jnp.tile(jnp.concatenate([-sine, sine], axis=1), (1, 2))
    merged = project(activity, query_weight, key_weight, value_weight, cosine, sine, G, R)
    return finish(merged, merge_full, 8)


def solution(mesh):
    placed = (P("sp", "tp"), P("sp", "tp"), P("sp", "tp"), P("sp", "tp"), P("tp", "sp"))
    return jax.shard_map(
        per_device, mesh=mesh, in_specs=placed, out_specs=P(("sp", "tp"), None), check_vma=False
    )
```

```python
import functools
import math

import jax
import jax.numpy as jnp
from jax import lax
from jax.experimental import pallas as pl
from jax.experimental.pallas import tpu as pltpu
from jax.sharding import PartitionSpec as P

HEAD = 64
HEAD_GROUPS = 3
SPAN = 128
DILATIONS = (1, 4, 8)
MESH = pl.DeviceIdType.MESH

rope_base = 500000.0


def project_kernel(
    G, R, act, wq, wk, wv, cos_ref, sin_ref, out,
    a_buf, w_buf, c_buf, r_buf, q_buf, kv_buf, o_buf, m_buf,
    local_sem, swap_send, swap_recv, fan_send, fan_recv,
    w_send, w_recv, c_send, c_recv, kv_send, kv_recv, m_send, m_recv,
):
    s = lax.axis_index("sp")
    t = lax.axis_index("tp")
    g = lax.div(s, R)
    r = lax.rem(s, R)
    tok = act.shape[0]
    krows = wq.shape[0]
    width = wq.shape[1] // G
    pairs = G // 2
    weights = (wq, wk, wv)

    swap_dev = (t * R + r, g)
    barrier = pltpu.get_barrier_semaphore()

    def greet(dev):
        pl.semaphore_signal(barrier, inc=1, device_id=dev, device_id_type=MESH)

    for i in range(1, G):
        greet((s, lax.rem(t + i, G)))
        greet((lax.rem(g + i, G) * R + r, t))
    for i in range(1, R):
        greet((g * R + lax.rem(r + i, R), t))

    @pl.when(g != t)
    def _():
        greet(swap_dev)

    pl.semaphore_wait(barrier, 2 * (G - 1) + (R - 1) + jnp.where(g != t, 1, 0))

    def swap_copy():
        return pltpu.make_async_remote_copy(
            src_ref=act, dst_ref=a_buf.at[g], send_sem=swap_send, recv_sem=swap_recv,
            device_id=swap_dev, device_id_type=MESH)

    def swap_local():
        return pltpu.make_async_copy(act, a_buf.at[t], local_sem)

    @pl.when(g != t)
    def _():
        swap_copy().start()

    @pl.when(g == t)
    def _():
        swap_local().start()

    def pair_at(stage):
        return lax.rem(lax.div(g, 2) + 1 + stage, pairs)

    def pair_cols(stage):
        return pl.ds(pl.multiple_of(pair_at(stage) * (2 * width), 128), 2 * width)

    def w_copy(stage, i, x):
        cols = pair_cols(stage)
        return pltpu.make_async_remote_copy(
            src_ref=weights[x].at[:, cols], dst_ref=w_buf.at[i - 1, x, :, cols],
            send_sem=w_send.at[stage, i - 1, x], recv_sem=w_recv.at[stage, i - 1, x],
            device_id=(g * R + lax.rem(r + R - i, R), t), device_id_type=MESH)

    for stage in range(pairs):
        for i in range(1, R):
            for x in range(3):
                w_copy(stage, i, x).start()

    @pl.when(g != t)
    def _():
        swap_copy().wait_recv()

    @pl.when(g == t)
    def _():
        swap_local().wait()

    def fan_copy(i):
        return pltpu.make_async_remote_copy(
            src_ref=a_buf.at[t], dst_ref=a_buf.at[t], send_sem=fan_send.at[i - 1],
            recv_sem=fan_recv.at[i - 1],
            device_id=(s, lax.rem(t + i, G)), device_id_type=MESH)

    def fan_arrival(i):
        slot = lax.rem(t + G - i, G)
        return pltpu.make_async_remote_copy(
            src_ref=a_buf.at[slot], dst_ref=a_buf.at[slot], send_sem=fan_send.at[i - 1],
            recv_sem=fan_recv.at[i - 1],
            device_id=(s, lax.rem(t + i, G)), device_id_type=MESH)

    for i in range(1, G):
        fan_copy(i).start()
    for i in range(1, G):
        fan_arrival(i).wait_recv()

    def c_copy(stage, j, b):
        dest = pair_at(stage) * 2 + j
        rows = pl.ds(pl.multiple_of(b * tok, tok), tok)
        return pltpu.make_async_remote_copy(
            src_ref=c_buf.at[stage, j, rows], dst_ref=r_buf.at[g, rows],
            send_sem=c_send.at[stage, j, b], recv_sem=c_recv.at[g, b],
            device_id=(dest * R + r, t), device_id_type=MESH)

    for stage in range(pairs):
        for i in range(1, R):
            for x in range(3):
                w_copy(stage, i, x).wait_recv()
        cols = pair_cols(stage)

        @pl.loop(0, G)
        def _(b):
            parts = []
            for x in range(3):
                total = jnp.dot(
                    a_buf[b, :, pl.ds(pl.multiple_of(r * krows, 128), krows)],
                    weights[x][:, cols], preferred_element_type=jnp.float32)
                for i in range(1, R):
                    start = pl.multiple_of(lax.rem(r + i, R) * krows, 128)
                    total = total + jnp.dot(
                        a_buf[b, :, pl.ds(start, krows)], w_buf[i - 1, x, :, cols],
                        preferred_element_type=jnp.float32)
                parts.append(total)
            rows = pl.ds(pl.multiple_of(b * tok, tok), tok)
            for j in range(2):
                c_buf[stage, j, rows, :] = jnp.concatenate(
                    [part[:, j * width:(j + 1) * width] for part in parts], axis=1
                ).astype(jnp.bfloat16)
            for j in range(2):
                @pl.when(pair_at(stage) * 2 + j != g)
                def _():
                    c_copy(stage, j, b).start()

    def c_arrival(source, b):
        rows = pl.ds(pl.multiple_of(b * tok, tok), tok)
        return pltpu.make_async_remote_copy(
            src_ref=r_buf.at[source, rows], dst_ref=r_buf.at[source, rows],
            send_sem=c_send.at[0, 0, b], recv_sem=c_recv.at[source, b],
            device_id=(s, t), device_id_type=MESH)

    mine = lax.rem(g, 2)
    most = SPAN * DILATIONS[-1]
    kv_buf[0:most, :] = jnp.zeros((most, 2 * width), jnp.bfloat16)

    def kv_rows(b, part):
        return pl.ds(pl.multiple_of(most + (b * R + part) * tok, 128), tok)

    def kv_copy(i, b):
        rows = kv_rows(b, r)
        return pltpu.make_async_remote_copy(
            src_ref=kv_buf.at[rows], dst_ref=kv_buf.at[rows],
            send_sem=kv_send.at[i - 1, b], recv_sem=kv_recv.at[i - 1, b],
            device_id=(g * R + lax.rem(r + R - i, R), t), device_id_type=MESH)

    def kv_arrival(i, b):
        rows = kv_rows(b, lax.rem(r + i, R))
        return pltpu.make_async_remote_copy(
            src_ref=kv_buf.at[rows], dst_ref=kv_buf.at[rows],
            send_sem=kv_send.at[i - 1, b], recv_sem=kv_recv.at[i - 1, b],
            device_id=(g * R + lax.rem(r + R - i, R), t), device_id_type=MESH)

    def gather_block(b):
        rows = pl.ds(pl.multiple_of(b * tok, tok), tok)
        total = c_buf[pairs - 1, mine, rows, :].astype(jnp.float32)
        for i in range(1, G):
            source = lax.rem(g + i, G)
            c_arrival(source, b).wait_recv()
            total = total + r_buf[source, rows, :].astype(jnp.float32)
        turn = total[:, :2 * width]
        half = HEAD // 2
        ahead = jnp.concatenate([turn[:, half:], turn[:, :half]], axis=1)
        behind = jnp.concatenate([turn[:, -half:], turn[:, :-half]], axis=1)
        lane = lax.broadcasted_iota(jnp.int32, turn.shape, 1)
        other = jnp.where((lane & (HEAD - 1)) < half, ahead, behind)
        reps = 2 * width // cos_ref.shape[1]
        cosine = jnp.concatenate([cos_ref[rows, :]] * reps, axis=1)
        sine = jnp.concatenate([sin_ref[rows, :]] * reps, axis=1)
        turned = turn * cosine + other * sine
        q_buf[rows, :] = turned[:, :width].astype(jnp.bfloat16)
        kv_buf[kv_rows(b, r), :] = jnp.concatenate(
            [turned[:, width:], total[:, 2 * width:]], axis=1).astype(jnp.bfloat16)
        for i in range(1, R):
            kv_copy(i, b).start()

    def m_copy(b):
        return pltpu.make_async_remote_copy(
            src_ref=o_buf.at[b], dst_ref=m_buf.at[g],
            send_sem=m_send.at[b], recv_sem=m_recv.at[g],
            device_id=(b * R + r, t), device_id_type=MESH)

    def m_arrival(source):
        return pltpu.make_async_remote_copy(
            src_ref=m_buf.at[source], dst_ref=m_buf.at[source],
            send_sem=m_send.at[source], recv_sem=m_recv.at[source],
            device_id=(source * R + r, t), device_id_type=MESH)

    def attend(b):
        for i in range(1, R):
            kv_arrival(i, b).wait_recv()
        rows = pl.ds(pl.multiple_of(b * tok, tok), tok)
        first = (b * R + r) * tok
        mixed_list = []
        total_list = []
        for index, dilation in enumerate(DILATIONS):
            reach = SPAN * dilation
            keys = reach + tok
            near = pl.ds(pl.multiple_of(most - reach + first, 128), keys)
            q = q_buf[rows, index * HEAD:(index + 1) * HEAD]
            k = kv_buf[near, index * HEAD:(index + 1) * HEAD]
            v = kv_buf[near, width + index * HEAD:width + (index + 1) * HEAD]
            scores = lax.dot_general(
                q, k, (((1,), (1,)), ((), ())), preferred_element_type=jnp.float32
            ) * HEAD ** (-0.5)
            col = lax.broadcasted_iota(jnp.int32, (tok, keys), 1)
            gap = reach + lax.broadcasted_iota(jnp.int32, (tok, keys), 0) - col
            allowed = (gap >= 0) & (gap <= reach) & (col >= reach - first)
            if dilation > 1:
                allowed = allowed & ((gap & (dilation - 1)) == 0)
            scores = jnp.where(allowed, scores, -jnp.inf)
            row_max = jnp.max(scores, axis=1, keepdims=True)
            expo = jnp.exp(scores - row_max)
            denominator = jnp.sum(expo, axis=1, keepdims=True)
            mixed = jnp.dot(expo.astype(jnp.bfloat16), v, preferred_element_type=jnp.float32)
            mixed_list.append(mixed / denominator)
            total_list.append(row_max + jnp.log(denominator))
        peak = jnp.maximum(jnp.maximum(total_list[0], total_list[1]), total_list[2])
        shifted = [jnp.exp(one - peak) for one in total_list]
        whole = shifted[0] + shifted[1] + shifted[2]
        merged = sum(a / whole * b_ for a, b_ in zip(shifted, mixed_list)).astype(jnp.bfloat16)

        @pl.when(b != g)
        def _():
            o_buf[b] = merged
            m_copy(b).start()

        @pl.when(b == g)
        def _():
            m_buf[b] = merged

    gather_block(0)

    @pl.loop(1, G)
    def _(b):
        gather_block(b)
        attend(b - 1)

    attend(G - 1)

    for i in range(1, G):
        m_arrival(lax.rem(g + i, G)).wait_recv()
    out[...] = jnp.concatenate(
        [m_buf[h].astype(jnp.float32) for h in range(G)], axis=1).astype(jnp.bfloat16)

    for i in range(1, G):
        m_copy(lax.rem(g + i, G)).wait_send()

    @pl.loop(0, G)
    def _(b):
        for i in range(1, R):
            kv_copy(i, b).wait_send()

    @pl.when(g != t)
    def _():
        swap_copy().wait_send()

    for i in range(1, G):
        fan_copy(i).wait_send()
    for stage in range(pairs):
        for i in range(1, R):
            for x in range(3):
                w_copy(stage, i, x).wait_send()
        for j in range(2):
            @pl.when(pair_at(stage) * 2 + j != g)
            def _():
                @pl.loop(0, G)
                def _(b):
                    c_copy(stage, j, b).wait_send()


def project(activity, wq, wk, wv, cosine, sine, G, R):
    tok, feat = activity.shape
    krows, col_width = wq.shape
    width = 3 * (col_width // G)
    pairs = G // 2
    rows = G * tok
    dma = pltpu.SemaphoreType.DMA
    return pl.pallas_call(
        functools.partial(project_kernel, G, R),
        out_shape=jax.ShapeDtypeStruct((tok, G * HEAD), jnp.bfloat16),
        in_specs=[pl.BlockSpec(memory_space=pltpu.VMEM)] * 6,
        out_specs=pl.BlockSpec(memory_space=pltpu.VMEM),
        scratch_shapes=[
            pltpu.VMEM((G, tok, feat), jnp.bfloat16),
            pltpu.VMEM((R - 1, 3, krows, col_width), jnp.bfloat16),
            pltpu.VMEM((pairs, 2, rows, width), jnp.bfloat16),
            pltpu.VMEM((G, rows, width), jnp.bfloat16),
            pltpu.VMEM((rows, width // 3), jnp.bfloat16),
            pltpu.VMEM((SPAN * DILATIONS[-1] + R * rows, 2 * (width // 3)), jnp.bfloat16),
            pltpu.VMEM((G, tok, HEAD), jnp.bfloat16),
            pltpu.VMEM((G, tok, HEAD), jnp.bfloat16),
            dma, dma, dma, dma((G - 1,)), dma((G - 1,)),
            dma((pairs, R - 1, 3)), dma((pairs, R - 1, 3)),
            dma((pairs, 2, G)), dma((G, G)),
            dma((R - 1, G)), dma((R - 1, G)), dma((G,)), dma((G,)),
        ],
        compiler_params=pltpu.CompilerParams(
            collective_id=0, has_side_effects=True, vmem_limit_bytes=58 * 2**20),
        cost_estimate=pl.CostEstimate(
            flops=2 * rows * feat * 3 * col_width, bytes_accessed=300 * 2**20, transcendentals=0),
    )(activity, wq, wk, wv, cosine, sine)


def finish_kernel(merged, weight, out, near_out, near_in, far_out, far_in, held,
                  near_send, near_recv, far_send, far_recv):
    s = lax.axis_index("sp")
    t = lax.axis_index("tp")
    chunks = near_out.shape[0]
    rows = out.shape[0]
    cols = weight.shape[1] // chunks
    low = lax.rem(t, 2)
    near = t + 1 - 2 * low
    far = lax.rem(t + 2, 4)
    across = lax.rem(near + 2, 4)

    barrier = pltpu.get_barrier_semaphore()
    for peer in (near, far):
        pl.semaphore_signal(barrier, inc=1, device_id=(s, peer), device_id_type=MESH)
    pl.semaphore_wait(barrier, 2)

    def near_copy(c):
        return pltpu.make_async_remote_copy(
            src_ref=near_out.at[c], dst_ref=near_in.at[c], send_sem=near_send.at[c],
            recv_sem=near_recv.at[c], device_id=(s, near), device_id_type=MESH)

    def far_copy(c):
        return pltpu.make_async_remote_copy(
            src_ref=far_out.at[c], dst_ref=far_in.at[c], send_sem=far_send.at[c],
            recv_sem=far_recv.at[c], device_id=(s, far), device_id_type=MESH)

    def part(owner, at):
        picked = merged[pl.ds(pl.multiple_of(owner * rows, rows), rows), :]
        return jnp.dot(picked, weight[:, at], preferred_element_type=jnp.float32)

    @pl.loop(0, chunks)
    def _(c):
        at = pl.ds(pl.multiple_of(c * cols, 128), cols)
        near_out[c, 0] = part(across, at).astype(jnp.bfloat16)
        near_out[c, 1] = part(near, at).astype(jnp.bfloat16)
        near_copy(c).start()
        held[c, 0] = part(far, at)
        held[c, 1] = part(t, at)

    @pl.loop(0, chunks)
    def _(c):
        near_copy(c).wait_recv()
        far_out[c] = (held[c, 0] + near_in[c, 0].astype(jnp.float32)).astype(jnp.bfloat16)
        far_copy(c).start()
        held[c, 1] = held[c, 1] + near_in[c, 1].astype(jnp.float32)

    @pl.loop(0, chunks)
    def _(c):
        at = pl.ds(pl.multiple_of(c * cols, 128), cols)
        far_copy(c).wait_recv()
        out[:, at] = (held[c, 1] + far_in[c].astype(jnp.float32)).astype(jnp.bfloat16)

    @pl.loop(0, chunks)
    def _(c):
        near_copy(c).wait_send()
        far_copy(c).wait_send()


def finish(merged, weight, chunks):
    rows = merged.shape[0] // 4
    cols = weight.shape[1] // chunks
    dma = pltpu.SemaphoreType.DMA
    return pl.pallas_call(
        finish_kernel,
        out_shape=jax.ShapeDtypeStruct((rows, weight.shape[1]), jnp.bfloat16),
        in_specs=[pl.BlockSpec(memory_space=pltpu.VMEM)] * 2,
        out_specs=pl.BlockSpec(memory_space=pltpu.VMEM),
        scratch_shapes=[
            pltpu.VMEM((chunks, 2, rows, cols), jnp.bfloat16),
            pltpu.VMEM((chunks, 2, rows, cols), jnp.bfloat16),
            pltpu.VMEM((chunks, rows, cols), jnp.bfloat16),
            pltpu.VMEM((chunks, rows, cols), jnp.bfloat16),
            pltpu.VMEM((chunks, 2, rows, cols), jnp.float32),
            dma((chunks,)), dma((chunks,)), dma((chunks,)), dma((chunks,)),
        ],
        compiler_params=pltpu.CompilerParams(
            collective_id=1, has_side_effects=True, vmem_limit_bytes=40 * 2**20),
    )(merged, weight)


def halves_kernel(
    act, wq, wk, wv, wm, out_hbm,
    x_buf, w_buf, own_buf, c_buf, r_buf, q_buf, kv_buf, ky_out, ky_in, o_buf, m_buf,
    cos_buf, sin_buf, wm_buf, merged_buf, near_out, near_in, far_out, far_in, held,
    done_out, prob_buf, gain_buf, out,
    local_sem, w_local, x_send, x_recv, w_send, w_recv, c_send, c_recv,
    ky_send, ky_recv, m_send, m_recv, wm_local, wm_send, wm_recv,
    near_send, near_recv, far_send, far_recv, done_send, done_recv, out_sem,
):
    s = lax.axis_index("sp")
    t = lax.axis_index("tp")
    z = lax.div(s, 2)
    y = lax.rem(s, 2)
    x = lax.div(t, 2)
    c = lax.rem(t, 2)
    zh = lax.div(z, 2)
    zl = lax.rem(z, 2)
    tok, feat = act.shape
    krows = wq.shape[0]
    pair = wq.shape[1] // 2
    width = pair // 2
    part = tok // 2
    weights = (wk, wv, wq)
    z_near = z + 1 - 2 * zl
    z_pair = lax.rem(z + 2, 4)
    y_far = 1 - y
    y_dev = (z * 2 + y_far, t)
    t_flip = 3 - t
    t_core = t + 1 - 2 * c
    hub = c == zh
    spoke = jnp.logical_not(hub)
    inner = zl != zh
    outer = jnp.logical_not(inner)
    straight = c == x
    bent = jnp.logical_not(straight)

    def at_z(other):
        return (other * 2 + y, t)

    barrier = pltpu.get_barrier_semaphore()

    def greet(dev):
        pl.semaphore_signal(barrier, inc=1, device_id=dev, device_id_type=MESH)

    for i in range(1, 4):
        greet(at_z(lax.rem(z + i, 4)))
        greet((s, lax.rem(t + i, 4)))
    greet(y_dev)
    cross_z = jnp.where(c == 0, 1, 2)
    cross_dev = (cross_z * 2 + y, t_core)

    for i in range(1, 4):
        greet((lax.rem(z + i, 4) * 2 + y, t_core))
    pl.semaphore_wait(barrier, 10)

    def remote(src, dst, send, recv, dev):
        return pltpu.make_async_remote_copy(
            src_ref=src, dst_ref=dst, send_sem=send, recv_sem=recv,
            device_id=dev, device_id_type=MESH)

    def own_rows(block):
        return pl.ds(pl.multiple_of(block * krows, 128), krows)

    def pair_cols(p):
        return pl.ds(pl.multiple_of(p * pair, 128), pair)

    mine_rows = own_rows(zl * 2 + y)

    def w_own(i):
        return pltpu.make_async_copy(
            weights[i].at[:, pair_cols(zl)], w_buf.at[i, mine_rows], w_local.at[i])

    small = krows // 2

    def piece_rows(block, p):
        return pl.ds(pl.multiple_of(block * krows + p * small, 128), small)

    def w_over_z(i, p):
        return remote(weights[i].at[p * small:(p + 1) * small, pair_cols(1 - zl)],
                      w_buf.at[i, piece_rows(zl * 2 + y, p)],
                      w_send.at[p, i], w_recv.at[p, i], at_z(z_near))

    def w_over_y(i):
        return remote(weights[i].at[:, pair_cols(zl)], w_buf.at[i, mine_rows],
                      w_send.at[4, i], w_recv.at[4, i], y_dev)

    def w_relay(i, p):
        rows = piece_rows((1 - zl) * 2 + y, p)
        return remote(w_buf.at[i, rows], w_buf.at[i, rows],
                      w_send.at[2 + p, i], w_recv.at[2 + p, i], y_dev)

    def w_push(i):
        for p in range(2):
            w_over_z(i, p).start()

    def w_hand_on(i):
        for p in range(2):
            w_over_z(i, p).wait_recv()
            w_relay(i, p).start()

    def w_wait(i):
        w_own(i).wait()
        w_over_y(i).wait_recv()
        w_relay(i, 0).wait_recv()
        w_relay(i, 1).wait_recv()

    wm_slot = zl * 2 + y
    wm_near_slot = (1 - zl) * 2 + y

    def wm_here():
        return pltpu.make_async_copy(wm, wm_buf.at[wm_slot], wm_local)

    def wm_over_z():
        return remote(wm, wm_buf.at[wm_slot], wm_send.at[0], wm_recv.at[wm_slot], at_z(z_near))

    def wm_over_y():
        return remote(wm, wm_buf.at[wm_slot], wm_send.at[1], wm_recv.at[wm_slot], y_dev)

    def wm_relay():
        return remote(wm_buf.at[wm_near_slot], wm_buf.at[wm_near_slot],
                      wm_send.at[2], wm_recv.at[wm_near_slot], y_dev)

    def wm_came(block):
        remote(wm_buf.at[block], wm_buf.at[block], wm_send.at[0], wm_recv.at[block], y_dev).wait_recv()

    hold = 8
    order = (z, z_near, jnp.where(inner, 3 - z, z_pair), jnp.where(inner, z_pair, 3 - z))

    def slot(quarter, block):
        return quarter * 4 + block

    def x_swap():
        there = jnp.where(1 - c == zh, slot(1 - x, z), hold)
        return remote(act, x_buf.at[there], x_send.at[0], x_recv.at[there], (s, t_flip))

    def x_here():
        return jnp.where(hub, slot(x, z), hold)

    def x_local():
        return pltpu.make_async_copy(act, x_buf.at[x_here()], local_sem)

    def x_move(index, block, dev):
        return remote(x_buf.at[block], x_buf.at[block], x_send.at[index], x_recv.at[block], dev)

    def x_arrived(block):
        remote(x_buf.at[block], x_buf.at[block], x_send.at[0], x_recv.at[block], (s, t)).wait_recv()

    def x_near():
        return x_move(1, slot(x, z), at_z(z_near))

    def x_cross():
        return remote(x_buf.at[hold], x_buf.at[slot(x, z)], x_send.at[1],
                      x_recv.at[slot(x, z)], cross_dev)

    def x_sideways(step):
        return x_move(2 + 2 * step, slot(x, order[step]), (s, t_flip))

    def x_inside(step):
        return x_move(3 + 2 * step, slot(x, order[step]), (s, t_core))

    def x_back(step):
        return x_move(3 + 2 * step, slot(1 - x, order[step]), (s, t_core))

    def x_outward(step):
        return x_move(8 + step, slot(x, order[step]), at_z(z_near))

    def lead(step):
        if step > 0:
            x_arrived(slot(x, order[step]))
        if step > 1:
            @pl.when(inner)
            def _():
                x_outward(step).start()
        if step > 0:
            x_sideways(step).start()
        x_inside(step).start()

    def follow(step):
        x_arrived(slot(1 - x, order[step]))
        x_back(step).start()

    def other_arrived(step):
        leads = hub if step < 2 else spoke
        x_arrived(slot(jnp.where(leads, 1 - x, x), order[step]))

    def packed(rows):
        return jnp.concatenate([rows[:part], rows[part:]], axis=1)

    def c_copy(i, b):
        return remote(c_buf.at[i, b], r_buf.at[i, b], c_send.at[i, b], c_recv.at[i, b], at_z(z_pair))

    def part_sum(i, b, held_back):
        total = jnp.dot(x_buf[b], w_buf[i, :feat, :], preferred_element_type=jnp.float32)
        total = total + jnp.dot(x_buf[4 + b], w_buf[i, feat:, :], preferred_element_type=jnp.float32)
        low = packed(total[:, :width])
        high = packed(total[:, width:])
        own_buf[i, b] = jnp.where(zh == 0, low, high)
        c_buf[i, b] = jnp.where(zh == 0, high, low).astype(jnp.bfloat16)
        if not held_back:
            c_copy(i, b).start()
        else:
            @pl.when(outer)
            def _():
                c_copy(i, b).start()

    w_push(0)
    w_over_y(0).start()

    @pl.when(bent)
    def _():
        x_swap().start()

    @pl.when(straight)
    def _():
        x_local().start()

    for i in range(3):
        w_own(i).start()
    wm_here().start()

    def x_first():
        @pl.when(hub)
        def _():
            x_near().start()
            lead(0)
            w_push(1)

        @pl.when(spoke)
        def _():
            x_cross().start()
            w_push(1)

    @pl.when(straight)
    def _():
        x_local().wait()
        x_first()

    @pl.loop(0, 4)
    def _(b):
        half = HEAD // 2
        shape = (part, pair)
        lane = lax.broadcasted_iota(jnp.int32, shape, 1)
        place = (b * 2 + y) * tok + lax.broadcasted_iota(jnp.int32, shape, 0)
        place = place + jnp.where(lane < width, 0, part)
        exponent = (lane & (half - 1)).astype(jnp.float32) * (2.0 / HEAD)
        angle = place.astype(jnp.float32) * jnp.exp(exponent * (-math.log(rope_base)))
        cos_buf[b] = jnp.cos(angle)
        sine = jnp.sin(angle)
        sin_buf[b] = jnp.where((lane & (HEAD - 1)) < half, -sine, sine)

    @pl.when(bent)
    def _():
        x_arrived(x_here())
        x_first()

    w_hand_on(0)
    w_over_y(1).start()

    @pl.when(hub)
    def _():
        x_sideways(0).start()

    @pl.when(spoke)
    def _():
        follow(0)

        @pl.when(inner)
        def _():
            lead(2)

    @pl.when(hub)
    def _():
        lead(1)

    w_wait(0)
    other_arrived(0)
    part_sum(0, order[0], False)

    @pl.when(spoke & inner)
    def _():
        lead(3)

    w_hand_on(1)
    w_over_y(2).start()
    w_push(2)

    @pl.when(spoke)
    def _():
        follow(1)

    @pl.when(hub & inner)
    def _():
        follow(2)

    other_arrived(1)
    part_sum(0, order[1], False)

    @pl.when(spoke & outer)
    def _():
        lead(2)

    @pl.when(hub & inner)
    def _():
        follow(3)

    w_wait(1)
    part_sum(1, order[0], True)
    part_sum(1, order[1], True)

    @pl.when(spoke & outer)
    def _():
        lead(3)

    @pl.when(hub & outer)
    def _():
        follow(2)

    w_hand_on(2)
    other_arrived(2)
    part_sum(0, order[2], False)
    part_sum(1, order[2], True)

    @pl.when(hub & outer)
    def _():
        follow(3)

    other_arrived(3)
    part_sum(0, order[3], False)
    part_sum(1, order[3], True)

    for p in range(2):
        w_over_z(2, p).wait_send()
    wm_over_z().start()
    wm_over_y().start()

    @pl.when(inner)
    def _():
        for b in range(2):
            c_copy(1, b).start()

    most = SPAN * DILATIONS[-1]
    kv_buf[0:most, :] = jnp.zeros((most, 2 * width), jnp.bfloat16)

    w_wait(2)

    @pl.loop(0, 4)
    def _(n):
        @pl.when(inner & (n > 0) & (n < 3))
        def _():
            c_copy(1, n + 1).start()

        part_sum(2, jnp.where(n == 3, 3, lax.rem(2 * n, 3)), False)

    def kv_rows(b, which):
        return pl.ds(pl.multiple_of(most + (b * 2 + which) * tok, 128), tok)

    def ky_copy(i, b):
        return remote(ky_out.at[i, b], ky_in.at[i, b], ky_send.at[i, b], ky_recv.at[i, b], y_dev)

    def whole_sum(i, b):
        c_copy(i, b).wait_recv()
        return own_buf[i, b] + r_buf[i, b].astype(jnp.float32)

    def unpacked(both):
        return jnp.concatenate([both[:, :width], both[:, width:]], axis=0)

    def rotate(turn, b):
        half = HEAD // 2
        ahead = jnp.concatenate([turn[:, half:], turn[:, :half]], axis=1)
        behind = jnp.concatenate([turn[:, -half:], turn[:, :-half]], axis=1)
        lane = lax.broadcasted_iota(jnp.int32, turn.shape, 1)
        other = jnp.where((lane & (HEAD - 1)) < half, ahead, behind)
        return (turn * cos_buf[b] + other * sin_buf[b]).astype(jnp.bfloat16)

    theirs = (z_pair, lax.rem(z_near + 2, 4), jnp.where(outer, 3 - z_pair, z), jnp.where(outer, z, 3 - z_pair))

    for step in range(4):
        b = theirs[step]
        turned = rotate(whole_sum(0, b), b)
        ky_out[0, b] = turned
        ky_copy(0, b).start()
        kv_buf[kv_rows(b, y), :width] = unpacked(turned)


    def gather_values(b):
        value = whole_sum(1, b).astype(jnp.bfloat16)
        ky_out[1, b] = value
        ky_copy(1, b).start()
        kv_buf[kv_rows(b, y), width:] = unpacked(value)

    def gather_queries(b):
        rows = pl.ds(pl.multiple_of(b * tok, tok), tok)
        q_buf[rows, :] = unpacked(rotate(whole_sum(2, b), b))

    def keys_arrived(b):
        ky_copy(0, b).wait_recv()
        kv_buf[kv_rows(b, y_far), :width] = unpacked(ky_in[0, b])

    def values_arrived(b):
        ky_copy(1, b).wait_recv()
        kv_buf[kv_rows(b, y_far), width:] = unpacked(ky_in[1, b])

    head = 2 * zl + zh

    def m_copy(b, there):
        where = lax.rem(b + 2 * there, 4)
        return remote(o_buf.at[b], m_buf.at[there, head], m_send.at[there, b],
                      m_recv.at[there, head], at_z(where))

    def m_arrival(there, source):
        return remote(m_buf.at[there, source], m_buf.at[there, source], m_send.at[there, source],
                      m_recv.at[there, source], at_z(z))

    spans = [SPAN * dilation + tok for dilation in DILATIONS]
    places = [sum(spans[:index]) for index in range(HEAD_GROUPS)]

    def near_keys(index, b):
        first = (b * 2 + y) * tok
        return pl.ds(pl.multiple_of(most - SPAN * DILATIONS[index] + first, 128), spans[index])

    def weigh(b):
        rows = pl.ds(pl.multiple_of(b * tok, tok), tok)
        first = (b * 2 + y) * tok
        sum_list = []
        total_list = []
        for index, dilation in enumerate(DILATIONS):
            reach = SPAN * dilation
            keys = spans[index]
            q = q_buf[rows, index * HEAD:(index + 1) * HEAD]
            k = kv_buf[near_keys(index, b), index * HEAD:(index + 1) * HEAD]
            scores = lax.dot_general(
                q, k, (((1,), (1,)), ((), ())), preferred_element_type=jnp.float32
            ) * HEAD ** (-0.5)
            col = lax.broadcasted_iota(jnp.int32, (tok, keys), 1)
            gap = reach + lax.broadcasted_iota(jnp.int32, (tok, keys), 0) - col
            allowed = (gap >= 0) & (gap <= reach) & (col >= reach - first)
            if dilation > 1:
                allowed = allowed & ((gap & (dilation - 1)) == 0)
            scores = jnp.where(allowed, scores, -jnp.inf)
            row_max = jnp.max(scores, axis=1, keepdims=True)
            expo = jnp.exp(scores - row_max)
            denominator = jnp.sum(expo, axis=1, keepdims=True)
            prob_buf[b, :, places[index]:places[index] + keys] = expo.astype(jnp.bfloat16)
            sum_list.append(denominator)
            total_list.append(row_max + jnp.log(denominator))
        peak = jnp.maximum(jnp.maximum(total_list[0], total_list[1]), total_list[2])
        shifted = [jnp.exp(one - peak) for one in total_list]
        whole = shifted[0] + shifted[1] + shifted[2]
        for index in range(HEAD_GROUPS):
            gain_buf[b, index] = shifted[index] / whole / sum_list[index]

    def attend(b):
        merged = jnp.zeros((tok, HEAD), jnp.float32)
        for index in range(HEAD_GROUPS):
            v = kv_buf[near_keys(index, b), width + index * HEAD:width + (index + 1) * HEAD]
            prob = prob_buf[b, :, places[index]:places[index] + spans[index]]
            mixed = jnp.dot(prob, v, preferred_element_type=jnp.float32)
            merged = merged + gain_buf[b, index] * mixed
        merged = packed(merged).astype(jnp.bfloat16)
        o_buf[b] = merged
        for there in range(2):
            mine = lax.rem(b + 2 * there, 4) == z

            @pl.when(jnp.logical_not(mine))
            def _():
                m_copy(b, there).start()

            @pl.when(mine)
            def _():
                m_buf[there, head] = merged

    far = lax.rem(t + 2, 4)
    across = 3 - t
    piece = out.shape[0]
    cols = wm.shape[1]

    def near_copy(n):
        return remote(near_out.at[n], near_in.at[n], near_send.at[n], near_recv.at[n], (s, t_core))

    def far_copy(n):
        return remote(far_out.at[n], far_in.at[n], far_send.at[n], far_recv.at[n], (s, far))

    blocks = (wm_slot, wm_near_slot, zl * 2 + y_far, (1 - zl) * 2 + y_far)

    def product(n):
        there = 1 - n // 4
        block = blocks[n % 4]

        def rows_of(owner):
            picked = merged_buf[there, pl.ds(pl.multiple_of(owner * piece, piece), piece), :]
            return jnp.dot(picked, wm_buf[block], preferred_element_type=jnp.float32)
        near_out[n, 0] = rows_of(across).astype(jnp.bfloat16)
        near_out[n, 1] = rows_of(t_core).astype(jnp.bfloat16)
        near_copy(n).start()
        held[n, 0] = rows_of(far)
        held[n, 1] = rows_of(t)

    def pass_on(n):
        near_copy(n).wait_recv()
        far_out[n] = (held[n, 0] + near_in[n, 0].astype(jnp.float32)).astype(jnp.bfloat16)
        far_copy(n).start()
        held[n, 1] = held[n, 1] + near_in[n, 1].astype(jnp.float32)

    def total_of(n):
        far_copy(n).wait_recv()
        return (held[n, 1] + far_in[n].astype(jnp.float32)).astype(jnp.bfloat16)

    def block_at(half, n):
        return pl.ds(pl.multiple_of((half * 4 + blocks[n]) * cols, 128), cols)

    def out_copy(half, n):
        at = block_at(half, n)
        return pltpu.make_async_copy(out.at[:, at], out_hbm.at[:, at], out_sem.at[half, n])

    def done_copy(n):
        return remote(done_out.at[n], out.at[:, block_at(zh, n)], done_send.at[n],
                      done_recv.at[n], at_z(z_pair))

    def collect(group):
        there = 1 - group
        for i in range(1, 4):
            source = lax.rem(z + i, 4)
            m_arrival(there, 2 * lax.rem(source, 2) + lax.div(source, 2)).wait_recv()
        heads = [m_buf[there, h].astype(jnp.float32) for h in range(4)]
        for half in range(2):
            merged_buf[there, half * part:(half + 1) * part] = jnp.concatenate(
                [one[:, half * HEAD:(half + 1) * HEAD] for one in heads], axis=1).astype(jnp.bfloat16)

    def hand_over(n):
        total = total_of(n)
        if n < 4:
            done_out[n] = total
            done_copy(n).start()
        else:
            out[:, block_at(zh, n - 4)] = total
            out_copy(zh, n - 4).start()

    def finish_block(b, fresh):
        gather_queries(b)
        for one in fresh:
            keys_arrived(one)
            values_arrived(one)
        weigh(b)
        attend(b)

    gather_values(0)
    gather_values(1)

    @pl.when(inner)
    def _():
        gather_values(2)
        gather_values(3)

    wm_here().wait()
    wm_came(wm_near_slot)
    wm_relay().start()

    finish_block(0, (0,))

    @pl.when(outer)
    def _():
        gather_values(2)

    finish_block(2, (1, 2))

    @pl.when(outer)
    def _():
        gather_values(3)

    finish_block(1, ())
    finish_block(3, (3,))
    collect(0)
    for n in range(4):
        if n == 2:
            wm_came(blocks[2])
        if n == 3:
            wm_came(blocks[3])
        product(n)
        if n > 0:
            pass_on(n - 1)
    pass_on(3)
    hand_over(0)
    collect(1)
    for n in range(4, 8):
        product(n)
        if n > 4:
            pass_on(n - 1)
            hand_over(n - 4)
    pass_on(7)
    for n in range(4, 8):
        hand_over(n)
    for n in range(4):
        done_copy(n).wait_recv()
        out_copy(1 - zh, n).start()
    for n in range(4):
        out_copy(zh, n).wait()
        out_copy(1 - zh, n).wait()

    for n in range(8):
        near_copy(n).wait_send()
        far_copy(n).wait_send()
    for n in range(4):
        done_copy(n).wait_send()
    wm_over_z().wait_send()
    wm_over_y().wait_send()
    wm_relay().wait_send()

    @pl.loop(0, 4)
    def _(b):
        for there in range(2):
            @pl.when(lax.rem(b + 2 * there, 4) != z)
            def _():
                m_copy(b, there).wait_send()
        for i in range(2):
            ky_copy(i, b).wait_send()
        for i in range(3):
            c_copy(i, b).wait_send()

    for i in range(3):
        for p in range(2):
            if i < 2:
                w_over_z(i, p).wait_send()
            w_relay(i, p).wait_send()
        w_over_y(i).wait_send()

    @pl.when(bent)
    def _():
        x_swap().wait_send()

    @pl.when(hub)
    def _():
        x_near().wait_send()

    @pl.when(spoke)
    def _():
        x_cross().wait_send()

    for step in range(4):
        leads = hub if step < 2 else spoke

        @pl.when(leads)
        def _():
            x_sideways(step).wait_send()
            x_inside(step).wait_send()
            if step > 1:
                @pl.when(inner)
                def _():
                    x_outward(step).wait_send()

        @pl.when(jnp.logical_not(leads))
        def _():
            x_back(step).wait_send()


def halves(activity, wq, wk, wv, wm):
    tok, feat = activity.shape
    krows, col_width = wq.shape
    width = col_width // 4
    rows = 4 * tok
    piece = tok // 4
    cols = wm.shape[1]
    dma = pltpu.SemaphoreType.DMA
    return pl.pallas_call(
        halves_kernel,
        out_shape=jax.ShapeDtypeStruct((piece, 8 * cols), jnp.bfloat16),
        in_specs=[pl.BlockSpec(memory_space=pltpu.HBM)] * 5,
        out_specs=pl.BlockSpec(memory_space=pltpu.HBM),
        scratch_shapes=[
            pltpu.VMEM((9, tok, feat), jnp.bfloat16),
            pltpu.VMEM((3, 4 * krows, 2 * width), jnp.bfloat16),
            pltpu.VMEM((3, 4, tok // 2, 2 * width), jnp.float32),
            pltpu.VMEM((3, 4, tok // 2, 2 * width), jnp.bfloat16),
            pltpu.VMEM((3, 4, tok // 2, 2 * width), jnp.bfloat16),
            pltpu.VMEM((rows, width), jnp.bfloat16),
            pltpu.VMEM((SPAN * DILATIONS[-1] + 2 * rows, 2 * width), jnp.bfloat16),
            pltpu.VMEM((2, 4, tok // 2, 2 * width), jnp.bfloat16),
            pltpu.VMEM((2, 4, tok // 2, 2 * width), jnp.bfloat16),
            pltpu.VMEM((4, tok // 2, 2 * HEAD), jnp.bfloat16),
            pltpu.VMEM((2, 4, tok // 2, 2 * HEAD), jnp.bfloat16),
            pltpu.VMEM((4, tok // 2, 2 * width), jnp.float32),
            pltpu.VMEM((4, tok // 2, 2 * width), jnp.float32),
            pltpu.VMEM((4, tok, cols), jnp.bfloat16),
            pltpu.VMEM((2, tok, 4 * HEAD), jnp.bfloat16),
            pltpu.VMEM((8, 2, piece, cols), jnp.bfloat16),
            pltpu.VMEM((8, 2, piece, cols), jnp.bfloat16),
            pltpu.VMEM((8, piece, cols), jnp.bfloat16),
            pltpu.VMEM((8, piece, cols), jnp.bfloat16),
            pltpu.VMEM((8, 2, piece, cols), jnp.float32),
            pltpu.VMEM((4, piece, cols), jnp.bfloat16),
            pltpu.VMEM((4, tok, sum(SPAN * one + tok for one in DILATIONS)), jnp.bfloat16),
            pltpu.VMEM((4, HEAD_GROUPS, tok, 1), jnp.float32),
            pltpu.VMEM((piece, 8 * cols), jnp.bfloat16),
            dma, dma((3,)), dma((12,)), dma((9,)), dma((5, 3)), dma((5, 3)),
            dma((3, 4)), dma((3, 4)), dma((2, 4)), dma((2, 4)), dma((2, 4)), dma((2, 4)),
            dma, dma((3,)), dma((4,)), dma((8,)), dma((8,)), dma((8,)), dma((8,)),
            dma((4,)), dma((4,)), dma((2, 4)),
        ],
        compiler_params=pltpu.CompilerParams(
            collective_id=2, has_side_effects=True, vmem_limit_bytes=66400000),
        cost_estimate=pl.CostEstimate(
            flops=2 * rows * feat * 3 * col_width, bytes_accessed=300 * 2**20, transcendentals=0),
    )(activity, wq, wk, wv, wm)


def per_device(activity, query_weight, key_weight, value_weight, merge_weight):
    G = lax.axis_size("tp")
    R = lax.axis_size("sp") // G
    r = lax.axis_index("sp") % R
    tok = activity.shape[0]
    if G == 4 and R == 2:
        return halves(activity, query_weight, key_weight, value_weight, merge_weight)
    merge_full = lax.all_gather(merge_weight, "sp", axis=1, tiled=True)
    block_start = (jnp.arange(G, dtype=jnp.int32) * R + r) * tok
    pos = (block_start[:, None] + jnp.arange(tok, dtype=jnp.int32)[None, :]).reshape(G * tok)
    half = HEAD // 2
    frequency = rope_base ** (-jnp.arange(0, half, dtype=jnp.float32) * 2.0 / HEAD)
    angles = pos.astype(jnp.float32)[:, None] * frequency[None, :]
    cosine = jnp.tile(jnp.cos(angles), (1, 4))
    sine = jnp.sin(angles)
    sine = jnp.tile(jnp.concatenate([-sine, sine], axis=1), (1, 2))
    merged = project(activity, query_weight, key_weight, value_weight, cosine, sine, G, R)
    return finish(merged, merge_full, 8)


def solution(mesh):
    placed = (P("sp", "tp"), P("sp", "tp"), P("sp", "tp"), P("sp", "tp"), P("tp", "sp"))
    return jax.shard_map(
        per_device, mesh=mesh, in_specs=placed, out_specs=P(("sp", "tp"), None), check_vma=False
    )
```
